32 devices in a mesh: sp: 4 (over y, core), dp: 8 (over z, x).
Axes of the slice: x: 2, y: 2, z: 4, core: 2. Of those that a mesh axis runs over, the one named last changes fastest.
Arguments:
- q_latent: bfloat16 [8, 512, 512], P('dp', 'sp'), may hold values from -70 to 70
- kv_latent: bfloat16 [8, 512, 512], P('dp', 'sp'), may hold values from -70 to 70
- rope_key: bfloat16 [8, 512, 64], P('dp', 'sp'), may hold values from -370 to 370
- w_query: bfloat16 [512, 3072], P(None, 'dp'), may hold values from -0.25 to 0.25
- w_keyval: bfloat16 [512, 4096], P(None, 'sp'), may hold values from -0.25 to 0.25
- w_out: bfloat16 [2048, 2048], replicated, may hold values from -0.125 to 0.125
- query_gain: bfloat16 [512], replicated, may hold values from 0.099609375 to 1.8984375
- latent_gain: bfloat16 [512], replicated, may hold values from 0.099609375 to 1.8984375
- out_gain: bfloat16 [2048], replicated, may hold values from 0.099609375 to 1.8984375
Outputs:
- output: bfloat16 [8, 512, 2048], P('dp', 'sp')
The draws below stay inside these ranges and needn't reach their ends.
All inputs are finite; a program needn't handle non-finite values.
Results may differ from the reference program's by a relative error of at most 0.03.
The reference program's roundings to bfloat16 on the way (of `query_norm`, `queries`, `latent_norm`, `keyval`, `rope_turned`, `weights`, `attended` and `mixed_norm`) count: a program that leaves them out, or rounds other values in their place, can miss the bound.
Values may be sent and summed in bfloat16 or wider, within the bound.
A program may use at most 64 MiB of HBM per device.

```python
import math
import jax
import jax.numpy as jnp
from jax import lax

D = 2048
H = 16
QR = 512
KR = 512
NOPE = 128
ROPE = 64
VDIM = 128
SEQ_LEN = 512
SEQS = 8


def scaled_latent_draw(key, width):
    base_key, channel_key, row_key = jax.random.split(key, 3)
    array_shape = (SEQS, SEQ_LEN, width)
    base_draw = jnp.clip(jax.random.normal(base_key, array_shape, jnp.float32), -5.0, 5.0)
    channel = jnp.exp(jax.random.uniform(channel_key, (width,), jnp.float32, math.log(0.3), math.log(3.0)))
    row_scale = jnp.exp(jax.random.uniform(row_key, (SEQS, SEQ_LEN, 1), jnp.float32, math.log(0.3), math.log(3.0)))
    return base_draw * channel * row_scale


def draw_q_latent(key, part):
    return scaled_latent_draw(jax.random.fold_in(key, 11), QR).astype(jnp.bfloat16)


def draw_kv_latent(key, part):
    return scaled_latent_draw(jax.random.fold_in(key, 12), KR).astype(jnp.bfloat16)


def draw_rope_key(key, part):
    base_key = jax.random.fold_in(jax.random.fold_in(key, 13), 0)
    array_shape = (SEQS, SEQ_LEN, ROPE)
    result_draw = jnp.clip(jax.random.normal(base_key, array_shape, jnp.float32), -5.0, 5.0)
    return result_draw.astype(jnp.bfloat16)


def steps_of(own_key, extent, cuts, least, largest):
    gain = 1.0
    for dim, parts in cuts:
        draws = jax.random.uniform(jax.random.fold_in(jax.random.fold_in(own_key, 6), dim), (parts,), jnp.float32, least / len(cuts), largest / len(cuts))
        gain = gain * jnp.repeat(jnp.exp(draws), extent[dim] // parts).reshape((-1,) + (1,) * (len(extent) - 1 - dim))
    return gain


def noise(own_key, shape, scale, limit, cuts=(), kind=jnp.bfloat16):
    values = scale * jax.random.normal(own_key, shape, jnp.float32)
    if cuts:
        values = values * steps_of(own_key, shape, cuts, -0.22, 0.18)
    return jnp.clip(values, -limit, limit).astype(kind)


def setup_inputs(seed: int = 0) -> dict:
    keys = jax.random.split(jax.random.key(seed), 10)
    return {
        "q_latent": draw_q_latent(jax.random.fold_in(keys[9], 71), 0),
        "kv_latent": draw_kv_latent(jax.random.fold_in(keys[9], 71), 0),
        "rope_key": draw_rope_key(jax.random.fold_in(keys[9], 71), 0),
        "w_query": noise(keys[3], (QR, H * (NOPE + ROPE)), QR ** -0.5, 0.25, ((1, 8),)),
        "w_keyval": noise(keys[4], (KR, H * (NOPE + VDIM)), KR ** -0.5, 0.25, ((1, 4),)),
        "w_out": noise(keys[5], (H * VDIM, D), (H * VDIM) ** -0.5, 0.125),
        "query_gain": jnp.clip(1.0 + 0.18 * jax.random.normal(keys[6], (QR,), jnp.float32), 0.099609375, 1.8984375).astype(jnp.bfloat16),
        "latent_gain": jnp.clip(1.0 + 0.18 * jax.random.normal(keys[7], (KR,), jnp.float32), 0.099609375, 1.8984375).astype(jnp.bfloat16),
        "out_gain": jnp.clip(1.0 + 0.18 * jax.random.normal(keys[8], (H * VDIM,), jnp.float32), 0.099609375, 1.8984375).astype(jnp.bfloat16),
    }


def normalize(row_values, gain_vector):
    widened = row_values.astype(jnp.float32)
    return widened * lax.rsqrt(lax.optimization_barrier(jnp.mean(widened * widened, axis=-1, keepdims=True)) + 1e-05) * gain_vector.astype(jnp.float32)

def angles_for(positions, rope_width):
    half_width = rope_width // 2
    inverse = 10000.0 ** (-jnp.arange(half_width, dtype=jnp.float32) / half_width)
    return positions.astype(jnp.float32)[:, None] * inverse[None, :]

def turn(vectors, angles):
    half_width = vectors.shape[-1] // 2
    cosine = jnp.cos(angles)
    sine_value = jnp.sin(angles)
    low_half = vectors[..., :half_width]
    high_half = vectors[..., half_width:]
    return jnp.concatenate([low_half * cosine - high_half * sine_value, high_half * cosine + low_half * sine_value], axis=-1)

def one_sequence(query_latent, kv_rows, rope_rows, w_query, w_keyval, w_out, query_gain, latent_gain, out_gain):
    length = query_latent.shape[0]
    positions = jnp.arange(length, dtype=jnp.int32)
    angles = angles_for(positions, ROPE)
    query_norm = normalize(query_latent, query_gain).astype(jnp.bfloat16)
    query_raw = jnp.dot(query_norm, w_query, preferred_element_type=jnp.float32).reshape(length, H, NOPE + ROPE)
    queries = jnp.concatenate([query_raw[..., :NOPE], turn(query_raw[..., NOPE:], angles[:, None, :])], axis=-1).astype(jnp.bfloat16)
    queries = lax.optimization_barrier(queries)
    latent_norm = normalize(kv_rows, latent_gain).astype(jnp.bfloat16)
    keyval = jnp.dot(latent_norm, w_keyval, preferred_element_type=jnp.float32).astype(jnp.bfloat16)
    keyval = lax.optimization_barrier(keyval).reshape(length, H, NOPE + VDIM)
    rope_turned = turn(rope_rows.astype(jnp.float32), angles).astype(jnp.bfloat16)
    rope_turned = lax.optimization_barrier(rope_turned)
    key_rows = jnp.concatenate([keyval[..., :NOPE], jnp.broadcast_to(rope_turned[:, None, :], (length, H, ROPE))], axis=-1)
    value_rows = keyval[..., NOPE:]
    block_rows = min(512, length)
    score_scale = (NOPE + ROPE) ** (-0.5)
    pieces = []
    for block_index in range(length // block_rows):
        block_start = block_index * block_rows
        block_stop = block_start + block_rows
        scores = jnp.einsum('qhd,khd->hqk', queries[block_start:block_stop].astype(jnp.float32), key_rows[:block_stop].astype(jnp.float32)) * score_scale
        allowed = jnp.arange(block_stop)[None, :] <= (block_start + jnp.arange(block_rows))[:, None]
        scores = jnp.where(allowed[None], scores, -jnp.inf)
        row_top = lax.optimization_barrier(jnp.max(scores, axis=-1, keepdims=True))
        exponent = jnp.exp(scores - row_top)
        row_total = lax.optimization_barrier(jnp.sum(exponent, axis=-1))
        weights = lax.optimization_barrier(exponent.astype(jnp.bfloat16))
        summed = jnp.einsum('hqk,khd->qhd', weights.astype(jnp.float32), value_rows[:block_stop].astype(jnp.float32))
        pieces.append((summed / jnp.transpose(row_total)[:, :, None]).astype(jnp.bfloat16))
    attended = lax.optimization_barrier(jnp.concatenate(pieces, axis=0)).reshape(length, H * VDIM)
    mixed_norm = normalize(attended, out_gain).astype(jnp.bfloat16)
    return jnp.dot(mixed_norm, w_out, preferred_element_type=jnp.float32).astype(jnp.bfloat16)

def reference(q_latent, kv_latent, rope_key, w_query, w_keyval, w_out, query_gain, latent_gain, out_gain):

    def per_sequence(inputs):
        return one_sequence(inputs[0], inputs[1], inputs[2], w_query, w_keyval, w_out, query_gain, latent_gain, out_gain)
    return lax.map(per_sequence, (q_latent, kv_latent, rope_key))
```

```python
import functools

import jax
import jax.numpy as jnp
import numpy as np
from jax import lax
from jax.experimental import pallas as pl
from jax.experimental.pallas import tpu as pltpu
from jax.sharding import PartitionSpec as P

H = 16
NOPE = 128
ROPE = 64
VDIM = 128
HEAD = NOPE + ROPE
MESH = pl.DeviceIdType.MESH
F32 = jnp.float32
BF16 = jnp.bfloat16


def turn_table(length):
    half = ROPE // 2
    inverse = np.float32(10000.0) ** (-np.arange(half, dtype=np.float32) / np.float32(half))
    angles = np.arange(length, dtype=np.float32)[:, None] * inverse[None, :].astype(np.float32)
    angles = angles.astype(np.float64)
    cosine, sine = np.cos(angles), np.sin(angles)
    return np.concatenate([cosine, cosine, sine, sine], axis=1).astype(np.float32)


def spread_matrix(rows, row_start, head):
    g = lax.broadcasted_iota(jnp.int32, (rows, 256), 0) + row_start
    f = lax.broadcasted_iota(jnp.int32, (rows, 256), 1)
    source = jnp.where(f < HEAD, f, jnp.where(f < HEAD + 32, f - 32, f - 96)) + head * HEAD
    sign = jnp.where((f >= HEAD) & (f < HEAD + 32), -1.0, 1.0)
    return jnp.where(g == source, sign, 0.0).astype(BF16)


def rope_matrix():
    r = lax.broadcasted_iota(jnp.int32, (ROPE, 128), 0)
    f = lax.broadcasted_iota(jnp.int32, (ROPE, 128), 1)
    source = jnp.where(f < 64, f, jnp.where(f < 96, f - 32, f - 96))
    sign = jnp.where((f >= 64) & (f < 96), -1.0, 1.0)
    return jnp.where(r == source, sign, 0.0).astype(BF16)


def scaled_rows(values, gain):
    wide = values.astype(F32)
    mean = jnp.mean(wide * wide, axis=-1, keepdims=True)
    return (wide * lax.rsqrt(mean + 1e-05) * gain).astype(BF16)


def kernel(
    geometry,
    q_ref, kv_ref, rope_ref, wq_ref, wkv_ref, wout_ref, table_ref, qg_ref, lg_ref, og_ref,
    out_ref,
    qall, kvall, ropeall, wqall, wkv, wout, table, spread, qn, qs, ks, vs, att_out, att_in, acc,
    out_gain,
    local_sem, gat_send, gat_recv, fwd_send, w_send, w_recv, att_send, att_recv,
):
    n, m, X, k, chunks, local_heads, groups = geometry
    per_group = local_heads // groups
    width = wqall.shape[2]
    Z = m // X
    rows = q_ref.shape[1]
    n_chips = n // 2
    i = lax.axis_index("sp")
    j = lax.axis_index("dp")
    core = lax.rem(i, 2)
    chip = lax.div(i, 2)
    partner = i + 1 - 2 * core
    z = lax.div(j, X)
    x = lax.rem(j, X)
    first = i * k
    owns = (j >= first) & (j < first + k)

    gathered = ((kv_ref.at[0], kvall), (rope_ref.at[0], ropeall), (q_ref.at[0], qall))
    own_copies = [
        pltpu.make_async_copy(src, dst.at[i], local_sem.at[a]) for a, (src, dst) in enumerate(gathered)
    ]
    wq_copy = pltpu.make_async_copy(wq_ref, wqall.at[lax.rem(j, k)], local_sem.at[3])
    wkv_copy = pltpu.make_async_copy(wkv_ref, wkv, local_sem.at[4])
    table_copy = pltpu.make_async_copy(table_ref, table, local_sem.at[5])
    wout_copy = pltpu.make_async_copy(wout_ref, wout, local_sem.at[6])

    @pl.when(owns)
    def _():
        wq_copy.start()

    for copy in own_copies:
        copy.start()
    wkv_copy.start()
    table_copy.start()
    wout_copy.start()

    turner = rope_matrix()
    latent_gain = lg_ref[...].astype(F32).reshape(1, -1)
    query_gain = qg_ref[...].astype(F32).reshape(1, -1)
    group = local_heads * VDIM
    every_gain = og_ref[...].astype(F32).reshape(1, -1)
    for s in range(n):
        out_gain[s] = every_gain[:, s * group:(s + 1) * group]
    if groups > 1:
        for h in range(per_group):
            spread[h] = spread_matrix(width, 0, h)

    barrier = pltpu.get_barrier_semaphore()
    for d in range(1, n):
        pl.semaphore_signal(
            barrier, inc=1, device_id={"sp": lax.rem(i + d, n)}, device_id_type=MESH
        )
    sides = ((z < Z - 1, j + X), (z > 0, j - X), (x < X - 1, j + 1), (x > 0, j - 1))
    count = n - 1
    for present, target in sides:
        @pl.when(present)
        def _(target=target):
            pl.semaphore_signal(barrier, inc=1, device_id={"dp": target}, device_id_type=MESH)
        count = count + jnp.where(present, 1, 0)
    pl.semaphore_wait(barrier, count)

    step_rows = wqall.shape[1] // chunks

    def relay_parts(slot, c):
        owner = first + slot
        zo, xo = lax.div(owner, X), lax.rem(owner, X)
        part = wqall.at[slot, pl.ds(c * step_rows, step_rows)]
        in_column = x == xo
        conditions = (
            in_column & (z >= zo) & (z < Z - 1),
            in_column & (z <= zo) & (z > 0),
            (x >= xo) & (x < X - 1),
            (x <= xo) & (x > 0),
        )
        copies = [
            pltpu.make_async_remote_copy(
                src_ref=part, dst_ref=part,
                send_sem=w_send.at[side, slot, c], recv_sem=w_recv.at[slot, c],
                device_id={"dp": sides[side][1]}, device_id_type=MESH,
            )
            for side in range(4)
        ]
        return owner, conditions, copies

    def relay(slot, c):
        owner, conditions, copies = relay_parts(slot, c)

        @pl.when(owner != j)
        def _():
            copies[0].wait_recv()

        for condition, copy in zip(conditions, copies):
            @pl.when(condition)
            def _(copy=copy):
                copy.start()

    def relay_finish(slot, c):
        _, conditions, copies = relay_parts(slot, c)
        for condition, copy in zip(conditions, copies):
            @pl.when(condition)
            def _(copy=copy):
                copy.wait_send()

    if groups > 1:
        columns = [lax.rem(x + t, k) for t in range(k)]
        events = [[(column, c) for c in range(chunks)] for column in columns]
    else:
        columns = [0]
        events = [[(slot, c) for c in range(chunks) for slot in range(k)]]
    events_left = list(events[0])

    def relay_some(number):
        for _ in range(min(number, len(events_left))):
            relay(*events_left.pop(0))

    def gather_copy(a, slot, sem, target):
        dst = gathered[a][1]
        return pltpu.make_async_remote_copy(
            src_ref=dst.at[slot], dst_ref=dst.at[slot],
            send_sem=sem, recv_sem=gat_recv.at[a, slot],
            device_id={"sp": target}, device_id_type=MESH,
        )

    sends = []

    @pl.when(owns)
    def _():
        wq_copy.wait()

    for a in range(3):
        own_copies[a].wait()
        for d in range(1, n_chips):
            target = 2 * lax.rem(chip + d, n_chips) + core
            sends.append(gather_copy(a, i, gat_send.at[a, d], target))
            sends[-1].start()
    for a in range(3):
        sends.append(gather_copy(a, i, gat_send.at[a, 0], partner))
        sends[-1].start()

    def far_slot(d):
        return 2 * lax.rem(chip + n_chips - d, n_chips) + core

    def forward(a, d):
        slot = far_slot(d)
        copy = gather_copy(a, slot, fwd_send.at[a, d - 1], partner)
        copy.wait_recv()
        copy.start()
        sends.append(copy)

    def arrive(a, slot):
        gather_copy(a, slot, gat_send.at[a, 0], partner).wait_recv()

    lane = lax.broadcasted_iota(jnp.int32, (rows, 128), 1)

    def keyval(slot):
        at = pl.ds(pl.multiple_of(slot * rows, rows), rows)
        both = jnp.dot(
            scaled_rows(kvall[slot], latent_gain), wkv[...], preferred_element_type=F32
        ).astype(BF16)
        pair = lax.dot_general(
            ropeall[slot], turner, (((0,), (0,)), ((), ())), preferred_element_type=F32
        ) * table[at, :]
        pair = pair + pltpu.roll(pair, 64, 1)
        turned = jnp.where(lane < 64, pair, 0.0).astype(BF16)
        for h in range(local_heads):
            base = h * (NOPE + VDIM)
            ks[h, at, 0:NOPE] = both[:, base:base + NOPE]
            ks[h, at, NOPE:256] = turned
            vs[h, at, :] = both[:, base + NOPE:base + NOPE + VDIM]

    def query_rows(slot):
        at = pl.ds(pl.multiple_of(slot * rows, rows), rows)
        qn[at, :] = scaled_rows(qall[slot], query_gain)

    relay_some(k + 1)
    wkv_copy.wait()
    table_copy.wait()
    keyval(i)
    relay_some(1)
    query_rows(i)
    relay_some(1)
    arrive(0, partner)
    arrive(1, partner)
    keyval(partner)
    relay_some(1)
    for d in range(1, n_chips):
        forward(0, d)
        forward(1, d)
        keyval(far_slot(d))
        relay_some(1)
    arrive(2, partner)
    query_rows(partner)
    relay_some(2)
    for d in range(1, n_chips):
        other = far_slot(d) + 1 - 2 * core
        arrive(0, other)
        arrive(1, other)
        keyval(other)
        relay_some(2)
    for d in range(1, n_chips):
        forward(2, d)
        query_rows(far_slot(d))
        relay_some(2)
    for d in range(1, n_chips):
        other = far_slot(d) + 1 - 2 * core
        arrive(2, other)
        query_rows(other)
    relay_some(len(events_left))

    def raw_queries(slot, hh):
        if groups > 1:
            total = jnp.dot(wqall[slot], spread[hh], preferred_element_type=F32)
        else:
            total = None
            for s in range(k):
                if (s + 1) * width <= hh * HEAD or s * width >= (hh + 1) * HEAD:
                    continue
                term = jnp.dot(
                    wqall[s], spread_matrix(width, s * width, hh), preferred_element_type=F32
                )
                total = term if total is None else total + term
        return jnp.dot(qn[...], total.astype(BF16), preferred_element_type=F32)

    def queries(slot):
        for hh in range(per_group):
            h = slot * per_group + hh
            raw = raw_queries(slot, hh)
            qs[h, :, 0:NOPE] = raw[:, 0:NOPE].astype(BF16)
            pair = raw[:, NOPE:256] * table[...]
            qs[h, :, NOPE:256] = (pair + pltpu.roll(pair, 64, 1)).astype(BF16)

    power = HEAD ** (-0.5) * float(np.log2(np.e))
    causal = lax.broadcasted_iota(jnp.int32, (rows, rows), 1) <= lax.broadcasted_iota(
        jnp.int32, (rows, rows), 0
    )

    def attend(b, slot):
        stop = (b + 1) * rows
        for hh in range(per_group):
            h = slot * per_group + hh
            scores = lax.dot_general(
                qs[h, b * rows:stop, :], ks[h, 0:stop, :], (((1,), (1,)), ((), ())),
                preferred_element_type=F32,
            )
            last = jnp.where(causal, scores[:, b * rows:], -jnp.inf)
            if b:
                scores = jnp.concatenate([scores[:, :b * rows], last], axis=1)
            else:
                scores = last
            top = jnp.max(scores, axis=-1, keepdims=True)
            weights = jnp.exp2((scores - top) * power)
            row_total = jnp.sum(weights, axis=-1, keepdims=True)
            summed = jnp.dot(weights.astype(BF16), vs[h, 0:stop, :], preferred_element_type=F32)
            att_out[b, slot, :, hh * VDIM:(hh + 1) * VDIM] = (summed / row_total).astype(BF16)

    def att_copy(b, slot):
        return pltpu.make_async_remote_copy(
            src_ref=att_out.at[b, slot], dst_ref=att_in.at[i, slot],
            send_sem=att_send.at[b, slot], recv_sem=att_recv.at[i, slot],
            device_id={"sp": b}, device_id_type=MESH,
        )

    for t, slot in enumerate(columns):
        if t:
            for event in events[t]:
                relay(*event)
        queries(slot)
        for c in range(n_chips):
            @pl.when(chip != c)
            def _(c=c):
                for b in (2 * c, 2 * c + 1):
                    attend(b, slot)
                    att_copy(b, slot).start()
    for c in range(n_chips):
        @pl.when(chip == c)
        def _(c=c):
            for slot in columns:
                for b in (2 * c, 2 * c + 1):
                    attend(b, slot)
    for slot in columns:
        att_copy(partner, slot).start()

    wout_copy.wait()
    squares = None
    order = [partner]
    for d in range(1, n_chips):
        order += [far_slot(d), far_slot(d) + 1 - 2 * core]
    for t, s in enumerate([i] + order):
        source = att_out
        if t:
            source = att_in
            for slot in range(groups):
                pltpu.make_async_remote_copy(
                    src_ref=att_in.at[s, slot], dst_ref=att_in.at[s, slot],
                    send_sem=att_send.at[0, slot], recv_sem=att_recv.at[s, slot],
                    device_id={"sp": partner}, device_id_type=MESH,
                ).wait_recv()
        values = jnp.concatenate([source[s, slot] for slot in range(groups)], axis=1).astype(F32)
        at = pl.ds(pl.multiple_of(s * group, group), group)
        square = jnp.sum(values * values, axis=-1, keepdims=True)
        squares = square if squares is None else squares + square
        scaled = (values * out_gain[s]).astype(BF16)
        term = jnp.dot(scaled, wout[at, :], preferred_element_type=F32)
        if t == 0:
            acc[...] = term
        elif t < n - 1:
            acc[...] += term
        else:
            factor = lax.rsqrt(squares / (n * group) + 1e-05)
            out_ref[0] = ((acc[...] + term) * factor).astype(BF16)

    for copy in sends:
        copy.wait_send()
    for event in sum(events, []):
        relay_finish(*event)
    for b in range(n):
        @pl.when(i != b)
        def _(b=b):
            for slot in range(groups):
                att_copy(b, slot).wait_send()


def x_size(mesh):
    row = mesh.devices[0]
    places = [getattr(device, "coords", None) for device in row]
    if any(place is None for place in places):
        return 1
    return len({place[0] for place in places})


def per_device(
    mesh, q_latent, kv_latent, rope_key, w_query, w_keyval, w_out, query_gain, latent_gain, out_gain
):
    n, m = mesh.shape["sp"], mesh.shape["dp"]
    rows = q_latent.shape[1]
    length = n * rows
    rank = q_latent.shape[2]
    width = w_query.shape[1]
    local_heads = H // n
    k = local_heads * HEAD // width
    chunks = 16
    columns = x_size(mesh)
    groups = k if k == columns == 2 and width % HEAD == 0 else 1
    dim = w_out.shape[1]
    group = local_heads * VDIM
    table = jnp.asarray(turn_table(length))
    geometry = (n, m, columns, k, chunks, local_heads, groups)
    any_spec = pl.BlockSpec(memory_space=pl.ANY)
    vmem_spec = pl.BlockSpec(memory_space=pltpu.VMEM)
    dma = pltpu.SemaphoreType.DMA
    return pl.pallas_call(
        functools.partial(kernel, geometry),
        out_shape=pltpu.VMEM((1, rows, dim), BF16),
        in_specs=[any_spec] * 7 + [vmem_spec] * 3,
        out_specs=vmem_spec,
        scratch_shapes=[
            pltpu.VMEM((n, rows, rank), BF16),
            pltpu.VMEM((n, rows, kv_latent.shape[2]), BF16),
            pltpu.VMEM((n, ROPE, rows), BF16),
            pltpu.VMEM((k, rank, width), BF16),
            pltpu.VMEM(w_keyval.shape, BF16),
            pltpu.VMEM(w_out.shape, BF16),
            pltpu.VMEM((length, 128), F32),
            pltpu.VMEM((local_heads // groups, width, 256), BF16),
            pltpu.VMEM((length, rank), BF16),
            pltpu.VMEM((local_heads, length, 256), BF16),
            pltpu.VMEM((local_heads, length, 256), BF16),
            pltpu.VMEM((local_heads, length, VDIM), BF16),
            pltpu.VMEM((n, groups, rows, group // groups), BF16),
            pltpu.VMEM((n, groups, rows, group // groups), BF16),
            pltpu.VMEM((rows, dim), F32),
            pltpu.VMEM((n, 1, group), F32),
            dma((7,)),
            dma((3, n // 2)),
            dma((3, n)),
            dma((3, n // 2)),
            dma((4, k, chunks)),
            dma((k, chunks)),
            dma((n, groups)),
            dma((n, groups)),
        ],
        compiler_params=pltpu.CompilerParams(
            collective_id=0, has_side_effects=True, vmem_limit_bytes=56 * 1024 * 1024
        ),
    )(
        q_latent, kv_latent, jnp.swapaxes(rope_key, 1, 2), w_query, w_keyval, w_out, table,
        query_gain, latent_gain, out_gain,
    )


def solution(mesh):
    in_specs = (
        P("dp", "sp", None),
        P("dp", "sp", None),
        P("dp", "sp", None),
        P(None, "dp"),
        P(None, "sp"),
        P(),
        P(),
        P(),
        P(),
    )
    return jax.shard_map(
        functools.partial(per_device, mesh), mesh=mesh, in_specs=in_specs,
        out_specs=P("dp", "sp", None), check_vma=False,
    )
```

```python
import functools

import jax
import jax.numpy as jnp
import numpy as np
from jax import lax
from jax.experimental import pallas as pl
from jax.experimental.pallas import tpu as pltpu
from jax.sharding import PartitionSpec as P

H = 16
NOPE = 128
ROPE = 64
VDIM = 128
HEAD = NOPE + ROPE
MESH = pl.DeviceIdType.MESH
F32 = jnp.float32
BF16 = jnp.bfloat16


def turn_table(length):
    half = ROPE // 2
    inverse = np.float32(10000.0) ** (-np.arange(half, dtype=np.float32) / np.float32(half))
    angles = np.arange(length, dtype=np.float32)[:, None] * inverse[None, :].astype(np.float32)
    angles = angles.astype(np.float64)
    cosine, sine = np.cos(angles), np.sin(angles)
    return np.concatenate([cosine, cosine, sine, sine], axis=1).astype(np.float32)


def spread_matrix(rows, row_start, head):
    g = lax.broadcasted_iota(jnp.int32, (rows, 256), 0) + row_start
    f = lax.broadcasted_iota(jnp.int32, (rows, 256), 1)
    source = jnp.where(f < HEAD, f, jnp.where(f < HEAD + 32, f - 32, f - 96)) + head * HEAD
    sign = jnp.where((f >= HEAD) & (f < HEAD + 32), -1.0, 1.0)
    return jnp.where(g == source, sign, 0.0).astype(BF16)


def rope_matrix():
    r = lax.broadcasted_iota(jnp.int32, (ROPE, 128), 0)
    f = lax.broadcasted_iota(jnp.int32, (ROPE, 128), 1)
    source = jnp.where(f < 64, f, jnp.where(f < 96, f - 32, f - 96))
    sign = jnp.where((f >= 64) & (f < 96), -1.0, 1.0)
    return jnp.where(r == source, sign, 0.0).astype(BF16)


def scaled_rows(values, gain):
    wide = values.astype(F32)
    mean = jnp.mean(wide * wide, axis=-1, keepdims=True)
    return (wide * lax.rsqrt(mean + 1e-05) * gain).astype(BF16)


def kernel(
    geometry,
    q_ref, kv_ref, rope_ref, wq_ref, wkv_ref, wout_ref, table_ref, qg_ref, lg_ref, og_ref,
    out_ref,
    qall, kvall, ropeall, wqall, wkv, wout, table, spread, qn, qs, ks, vs, att_out, att_in, acc,
    out_gain,
    local_sem, gat_send, gat_recv, fwd_send, w_send, w_recv, att_send, att_recv,
):
    n, m, X, k, chunks, local_heads, groups = geometry
    per_group = local_heads // groups
    width = wqall.shape[2]
    Z = m // X
    rows = q_ref.shape[1]
    n_chips = n // 2
    i = lax.axis_index("sp")
    j = lax.axis_index("dp")
    core = lax.rem(i, 2)
    chip = lax.div(i, 2)
    partner = i + 1 - 2 * core
    z = lax.div(j, X)
    x = lax.rem(j, X)
    first = i * k
    owns = (j >= first) & (j < first + k)

    gathered = ((kv_ref.at[0], kvall), (rope_ref.at[0], ropeall), (q_ref.at[0], qall))
    own_copies = [
        pltpu.make_async_copy(src, dst.at[i], local_sem.at[a]) for a, (src, dst) in enumerate(gathered)
    ]
    wq_copy = pltpu.make_async_copy(wq_ref, wqall.at[lax.rem(j, k)], local_sem.at[3])
    wkv_copy = pltpu.make_async_copy(wkv_ref, wkv, local_sem.at[4])
    table_copy = pltpu.make_async_copy(table_ref, table, local_sem.at[5])
    wout_copy = pltpu.make_async_copy(wout_ref, wout, local_sem.at[6])

    @pl.when(owns)
    def _():
        wq_copy.start()

    for copy in own_copies:
        copy.start()
    wkv_copy.start()
    table_copy.start()
    wout_copy.start()

    turner = rope_matrix()
    latent_gain = lg_ref[...].astype(F32).reshape(1, -1)
    query_gain = qg_ref[...].astype(F32).reshape(1, -1)
    group = local_heads * VDIM
    every_gain = og_ref[...].astype(F32).reshape(1, -1)
    for s in range(n):
        out_gain[s] = every_gain[:, s * group:(s + 1) * group]
    if groups > 1:
        for h in range(per_group):
            spread[h] = spread_matrix(width, 0, h)

    barrier = pltpu.get_barrier_semaphore()
    for d in range(1, n):
        pl.semaphore_signal(
            barrier, inc=1, device_id={"sp": lax.rem(i + d, n)}, device_id_type=MESH
        )
    sides = ((z < Z - 1, j + X), (z > 0, j - X), (x < X - 1, j + 1), (x > 0, j - 1))
    count = n - 1
    for present, target in sides:
        @pl.when(present)
        def _(target=target):
            pl.semaphore_signal(barrier, inc=1, device_id={"dp": target}, device_id_type=MESH)
        count = count + jnp.where(present, 1, 0)
    pl.semaphore_wait(barrier, count)

    step_rows = wqall.shape[1] // chunks

    def relay_parts(slot, c):
        owner = first + slot
        zo, xo = lax.div(owner, X), lax.rem(owner, X)
        part = wqall.at[slot, pl.ds(c * step_rows, step_rows)]
        in_column = x == xo
        conditions = (
            in_column & (z >= zo) & (z < Z - 1),
            in_column & (z <= zo) & (z > 0),
            (x >= xo) & (x < X - 1),
            (x <= xo) & (x > 0),
        )
        copies = [
            pltpu.make_async_remote_copy(
                src_ref=part, dst_ref=part,
                send_sem=w_send.at[side, slot, c], recv_sem=w_recv.at[slot, c],
                device_id={"dp": sides[side][1]}, device_id_type=MESH,
            )
            for side in range(4)
        ]
        return owner, conditions, copies

    def relay(slot, c):
        owner, conditions, copies = relay_parts(slot, c)

        @pl.when(owner != j)
        def _():
            copies[0].wait_recv()

        for condition, copy in zip(conditions, copies):
            @pl.when(condition)
            def _(copy=copy):
                copy.start()

    def relay_finish(slot, c):
        _, conditions, copies = relay_parts(slot, c)
        for condition, copy in zip(conditions, copies):
            @pl.when(condition)
            def _(copy=copy):
                copy.wait_send()

    if groups > 1:
        columns = [lax.rem(x + t, k) for t in range(k)]
        events = [[(column, c) for c in range(chunks)] for column in columns]
    else:
        columns = [0]
        events = [[(slot, c) for c in range(chunks) for slot in range(k)]]
    events_left = list(events[0])

    def relay_some(number):
        for _ in range(min(number, len(events_left))):
            relay(*events_left.pop(0))

    def gather_copy(a, slot, sem, target):
        dst = gathered[a][1]
        return pltpu.make_async_remote_copy(
            src_ref=dst.at[slot], dst_ref=dst.at[slot],
            send_sem=sem, recv_sem=gat_recv.at[a, slot],
            device_id={"sp": target}, device_id_type=MESH,
        )

    sends = []

    @pl.when(owns)
    def _():
        wq_copy.wait()

    for a in range(3):
        own_copies[a].wait()
        for d in range(1, n_chips):
            target = 2 * lax.rem(chip + d, n_chips) + core
            sends.append(gather_copy(a, i, gat_send.at[a, d], target))
            sends[-1].start()
    for a in range(3):
        sends.append(gather_copy(a, i, gat_send.at[a, 0], partner))
        sends[-1].start()

    def far_slot(d):
        return 2 * lax.rem(chip + n_chips - d, n_chips) + core

    def forward(a, d):
        slot = far_slot(d)
        copy = gather_copy(a, slot, fwd_send.at[a, d - 1], partner)
        copy.wait_recv()
        copy.start()
        sends.append(copy)

    def arrive(a, slot):
        gather_copy(a, slot, gat_send.at[a, 0], partner).wait_recv()

    lane = lax.broadcasted_iota(jnp.int32, (rows, 128), 1)

    def keyval(slot):
        at = pl.ds(pl.multiple_of(slot * rows, rows), rows)
        both = jnp.dot(
            scaled_rows(kvall[slot], latent_gain), wkv[...], preferred_element_type=F32
        ).astype(BF16)
        pair = lax.dot_general(
            ropeall[slot], turner, (((0,), (0,)), ((), ())), preferred_element_type=F32
        ) * table[at, :]
        pair = pair + pltpu.roll(pair, 64, 1)
        turned = jnp.where(lane < 64, pair, 0.0).astype(BF16)
        for h in range(local_heads):
            base = h * (NOPE + VDIM)
            ks[h, at, 0:NOPE] = both[:, base:base + NOPE]
            ks[h, at, NOPE:256] = turned
            vs[h, at, :] = both[:, base + NOPE:base + NOPE + VDIM]

    def query_rows(slot):
        at = pl.ds(pl.multiple_of(slot * rows, rows), rows)
        qn[at, :] = scaled_rows(qall[slot], query_gain)

    relay_some(k + 1)
    wkv_copy.wait()
    table_copy.wait()
    keyval(i)
    relay_some(1)
    query_rows(i)
    relay_some(1)
    arrive(0, partner)
    arrive(1, partner)
    keyval(partner)
    relay_some(1)
    for d in range(1, n_chips):
        forward(0, d)
        forward(1, d)
        keyval(far_slot(d))
        relay_some(1)
    arrive(2, partner)
    query_rows(partner)
    relay_some(2)
    for d in range(1, n_chips):
        other = far_slot(d) + 1 - 2 * core
        arrive(0, other)
        arrive(1, other)
        keyval(other)
        relay_some(2)
    for d in range(1, n_chips):
        forward(2, d)
        query_rows(far_slot(d))
        relay_some(2)
    for d in range(1, n_chips):
        other = far_slot(d) + 1 - 2 * core
        arrive(2, other)
        query_rows(other)
    relay_some(len(events_left))

    def raw_queries(slot, hh):
        if groups > 1:
            total = jnp.dot(wqall[slot], spread[hh], preferred_element_type=F32)
        else:
            total = None
            for s in range(k):
                if (s + 1) * width <= hh * HEAD or s * width >= (hh + 1) * HEAD:
                    continue
                term = jnp.dot(
                    wqall[s], spread_matrix(width, s * width, hh), preferred_element_type=F32
                )
                total = term if total is None else total + term
        return jnp.dot(qn[...], total.astype(BF16), preferred_element_type=F32)

    def queries(slot):
        for hh in range(per_group):
            h = slot * per_group + hh
            raw = raw_queries(slot, hh)
            qs[h, :, 0:NOPE] = raw[:, 0:NOPE].astype(BF16)
            pair = raw[:, NOPE:256] * table[...]
            qs[h, :, NOPE:256] = (pair + pltpu.roll(pair, 64, 1)).astype(BF16)

    power = HEAD ** (-0.5) * float(np.log2(np.e))
    causal = lax.broadcasted_iota(jnp.int32, (rows, rows), 1) <= lax.broadcasted_iota(
        jnp.int32, (rows, rows), 0
    )

    def attend(b, slot):
        stop = (b + 1) * rows
        for hh in range(per_group):
            h = slot * per_group + hh
            scores = lax.dot_general(
                qs[h, b * rows:stop, :], ks[h, 0:stop, :], (((1,), (1,)), ((), ())),
                preferred_element_type=F32,
            )
            last = jnp.where(causal, scores[:, b * rows:], -jnp.inf)
            if b:
                scores = jnp.concatenate([scores[:, :b * rows], last], axis=1)
            else:
                scores = last
            top = jnp.max(scores, axis=-1, keepdims=True)
            weights = jnp.exp2((scores - top) * power)
            row_total = jnp.sum(weights, axis=-1, keepdims=True)
            summed = jnp.dot(weights.astype(BF16), vs[h, 0:stop, :], preferred_element_type=F32)
            att_out[b, slot, :, hh * VDIM:(hh + 1) * VDIM] = (summed / row_total).astype(BF16)

    def att_copy(b, slot):
        return pltpu.make_async_remote_copy(
            src_ref=att_out.at[b, slot], dst_ref=att_in.at[i, slot],
            send_sem=att_send.at[b, slot], recv_sem=att_recv.at[i, slot],
            device_id={"sp": b}, device_id_type=MESH,
        )

    for t, slot in enumerate(columns):
        if t:
            for event in events[t]:
                relay(*event)
        queries(slot)
        for c in range(n_chips):
            @pl.when(chip != c)
            def _(c=c):
                for b in (2 * c, 2 * c + 1):
                    attend(b, slot)
                    att_copy(b, slot).start()
    for c in range(n_chips):
        @pl.when(chip == c)
        def _(c=c):
            for slot in columns:
                for b in (2 * c, 2 * c + 1):
                    attend(b, slot)
    for slot in columns:
        att_copy(partner, slot).start()

    wout_copy.wait()
    squares = None
    order = [partner]
    for d in range(1, n_chips):
        order += [far_slot(d), far_slot(d) + 1 - 2 * core]
    for t, s in enumerate([i] + order):
        source = att_out
        if t:
            source = att_in
            for slot in range(groups):
                pltpu.make_async_remote_copy(
                    src_ref=att_in.at[s, slot], dst_ref=att_in.at[s, slot],
                    send_sem=att_send.at[0, slot], recv_sem=att_recv.at[s, slot],
                    device_id={"sp": partner}, device_id_type=MESH,
                ).wait_recv()
        values = jnp.concatenate([source[s, slot] for slot in range(groups)], axis=1).astype(F32)
        at = pl.ds(pl.multiple_of(s * group, group), group)
        square = jnp.sum(values * values, axis=-1, keepdims=True)
        squares = square if squares is None else squares + square
        scaled = (values * out_gain[s]).astype(BF16)
        term = jnp.dot(scaled, wout[at, :], preferred_element_type=F32)
        if t == 0:
            acc[...] = term
        elif t < n - 1:
            acc[...] += term
        else:
            factor = lax.rsqrt(squares / (n * group) + 1e-05)
            out_ref[0] = ((acc[...] + term) * factor).astype(BF16)

    for copy in sends:
        copy.wait_send()
    for event in sum(events, []):
        relay_finish(*event)
    for b in range(n):
        @pl.when(i != b)
        def _(b=b):
            for slot in range(groups):
                att_copy(b, slot).wait_send()


def paired_table(length):
    half = ROPE // 2
    inverse = np.float32(10000.0) ** (-np.arange(half, dtype=np.float32) / np.float32(half))
    angles = np.arange(length, dtype=np.float32)[:, None] * inverse[None, :].astype(np.float32)
    angles = angles.astype(np.float64)
    cosine, sine = np.cos(angles), np.sin(angles)
    parts = [cosine] * 4 + [-sine, sine, -sine, sine]
    return np.concatenate(parts, axis=1).astype(np.float32)


def paired_kernel(
    geometry,
    q_ref, kv_ref, rope_ref, wq_ref, wkv_ref, wout_ref, table_ref, qg_ref, lg_ref, og_ref,
    out_ref,
    qall, kvall, ropeall, wqall, wkv, wout, table, qgain, lgain, ogain, qn, qs, ks, vs,
    att_out, att_in, acc,
    local_sem, gat_send, gat_recv, w_send, w_recv, x_recv, att_send, att_recv,
):
    n, X, Z, chunks, local_heads = geometry
    width = wqall.shape[2]
    rows = q_ref.shape[1]
    n_chips = n // 2
    i = lax.axis_index("sp")
    j = lax.axis_index("dp")
    core = lax.rem(i, 2)
    chip = lax.div(i, 2)
    partner = i + 1 - 2 * core
    z = lax.div(j, X)
    x = lax.rem(j, X)
    across = 1 - x
    zo = i
    owns = z == zo
    pair_dim = 2 * VDIM

    gathered = ((kv_ref.at[0], kvall), (rope_ref.at[0], ropeall), (q_ref.at[0], qall))
    own_copies = [
        pltpu.make_async_copy(src, dst.at[i], local_sem.at[a]) for a, (src, dst) in enumerate(gathered)
    ]
    wq_copy = pltpu.make_async_copy(wq_ref, wqall.at[x], local_sem.at[3])
    wkv_copy = pltpu.make_async_copy(wkv_ref, wkv, local_sem.at[4])
    table_copy = pltpu.make_async_copy(table_ref, table, local_sem.at[5])
    wout_copy = pltpu.make_async_copy(wout_ref, wout, local_sem.at[6])
    gain_copies = [
        pltpu.make_async_copy(src, dst, local_sem.at[7 + a])
        for a, (src, dst) in enumerate(((qg_ref, qgain), (lg_ref, lgain), (og_ref, ogain)))
    ]

    barrier = pltpu.get_barrier_semaphore()
    for d in range(1, n):
        pl.semaphore_signal(
            barrier, inc=1, device_id={"sp": lax.rem(i + d, n)}, device_id_type=MESH
        )
    low_end = zo == 0
    high_end = zo == Z - 1
    greet = (
        (z < Z - 1, j + X), (z > 0, j - X), (x >= 0, j + 1 - 2 * x),
        (low_end & (z == 0), j + 2 * X), (low_end & (z == 2), j - 2 * X),
        (high_end & (z == Z - 1), j - 2 * X), (high_end & (z == Z - 3), j + 2 * X),
    )
    count = n - 1
    for present, target in greet:
        @pl.when(present)
        def _(target=target):
            pl.semaphore_signal(barrier, inc=1, device_id={"dp": target}, device_id_type=MESH)
        count = count + jnp.where(present, 1, 0)

    @pl.when(owns)
    def _():
        wq_copy.start()

    for copy in own_copies:
        copy.start()
    for copy in gain_copies:
        copy.start()
    wkv_copy.start()
    table_copy.start()
    wout_copy.start()

    for h in range(local_heads):
        vs[h, :, VDIM:2 * VDIM] = jnp.ones((vs.shape[1], VDIM), BF16)
    r = lax.broadcasted_iota(jnp.int32, (ROPE, 128), 0)
    f = lax.broadcasted_iota(jnp.int32, (ROPE, 128), 1)
    turner = jnp.where(r == lax.rem(f, ROPE), 1.0, 0.0).astype(BF16)

    step_rows = wqall.shape[1] // chunks

    def w_part(c):
        return wqall.at[x, pl.ds(c * step_rows, step_rows)]

    sides = (
        ((z >= zo) & (z < Z - 1) & jnp.logical_not(low_end & (z == 1)), j + X),
        ((z <= zo) & (z > 0) & jnp.logical_not(high_end & (z == Z - 2)), j - X),
        (low_end & (z == 0), j + 2 * X),
        (high_end & (z == Z - 1), j - 2 * X),
    )

    def w_copy(side, c):
        part = w_part(c)
        return pltpu.make_async_remote_copy(
            src_ref=part, dst_ref=part, send_sem=w_send.at[side], recv_sem=w_recv.at[c],
            device_id={"dp": sides[side][1]}, device_id_type=MESH,
        )

    def x_copy(part):
        return pltpu.make_async_remote_copy(
            src_ref=part, dst_ref=part, send_sem=w_send.at[4], recv_sem=x_recv.at[0],
            device_id={"dp": j + 1 - 2 * x}, device_id_type=MESH,
        )

    chunks_left = list(range(chunks))

    def relay(number):
        number = min(number, len(chunks_left))
        if not number:
            return
        todo = [chunks_left.pop(0) for _ in range(number)]

        @pl.when(jnp.logical_not(owns))
        def _():
            for c in todo:
                w_copy(0, c).wait_recv()
                for side in (0, 1):
                    @pl.when(sides[side][0])
                    def _(side=side, c=c):
                        w_copy(side, c).start()
                x_copy(w_part(c)).start()

    def gather_copy(a, slot, target):
        dst = gathered[a][1]
        return pltpu.make_async_remote_copy(
            src_ref=dst.at[slot], dst_ref=dst.at[slot],
            send_sem=gat_send.at[a], recv_sem=gat_recv.at[a, slot],
            device_id={"sp": target}, device_id_type=MESH,
        )

    def far_slot(d):
        return 2 * lax.rem(chip + n_chips - d, n_chips) + core

    def forward(a, d):
        slot = far_slot(d)
        copy = gather_copy(a, slot, partner)
        copy.wait_recv()
        copy.start()

    def arrive(a, slot):
        gather_copy(a, slot, partner).wait_recv()

    lane = lax.broadcasted_iota(jnp.int32, (rows, 128), 1)
    left = lane < 64

    def turned_pair(both_halves, at):
        swap_low = lax.rem(lax.broadcasted_iota(jnp.int32, both_halves.shape, 1), 64) < 32
        swapped = jnp.where(
            swap_low, pltpu.roll(both_halves, 96, 1), pltpu.roll(both_halves, 32, 1)
        )
        return both_halves * table[at, 0:128] + swapped * table[at, 128:256]

    def keyval(slot):
        at = pl.ds(pl.multiple_of(slot * rows, rows), rows)
        both = jnp.dot(
            scaled_rows(kvall[slot], lgain[...].astype(F32).reshape(1, -1)), wkv[...],
            preferred_element_type=F32,
        )
        twice = lax.dot_general(
            ropeall[slot], turner, (((0,), (0,)), ((), ())), preferred_element_type=F32
        )
        turned = turned_pair(twice, at)
        for h in range(local_heads):
            base = h * (NOPE + VDIM)
            key = both[:, base:base + NOPE]
            if h % 2 == 0:
                ks[h, at, 0:NOPE] = key.astype(BF16)
                ks[h, at, NOPE:256] = jnp.where(left, turned, 0.0).astype(BF16)
            else:
                key = pltpu.roll(key, 64, 1)
                ks[h, at, 0:NOPE] = jnp.where(left, 0.0, key).astype(BF16)
                ks[h, at, NOPE:256] = jnp.where(left, key, turned).astype(BF16)
            vs[h, at, 0:VDIM] = both[:, base + NOPE:base + NOPE + VDIM].astype(BF16)

    def query_rows(slot):
        at = pl.ds(pl.multiple_of(slot * rows, rows), rows)
        qn[at, :] = scaled_rows(qall[slot], qgain[...].astype(F32).reshape(1, -1))

    for copy in own_copies:
        copy.wait()
    for copy in gain_copies:
        copy.wait()
    query_rows(i)

    @pl.when(owns)
    def _():
        wq_copy.wait()

    pl.semaphore_wait(barrier, count)

    for a in range(3):
        for d in range(1, n_chips):
            gather_copy(a, i, 2 * lax.rem(chip + d, n_chips) + core).start()

    @pl.when(owns)
    def _():
        x_copy(wqall.at[x]).start()
        for c in range(chunks):
            for side in range(4):
                @pl.when(sides[side][0])
                def _(side=side, c=c):
                    w_copy(side, c).start()

    for a in range(3):
        gather_copy(a, i, partner).start()

    wkv_copy.wait()
    table_copy.wait()
    keyval(i)
    arrive(0, partner)
    arrive(1, partner)
    keyval(partner)
    arrive(2, partner)
    query_rows(partner)
    relay(chunks * 3 // 8)
    for d in range(1, n_chips):
        forward(0, d)
        forward(1, d)
        relay(chunks // 16)
        keyval(far_slot(d))
        relay(chunks // 16)
    for d in range(1, n_chips):
        other = far_slot(d) + 1 - 2 * core
        arrive(0, other)
        arrive(1, other)
        keyval(other)
        relay(chunks // 8)
    for d in range(1, n_chips):
        forward(2, d)
        query_rows(far_slot(d))
        relay(chunks // 8)
    for d in range(1, n_chips):
        other = far_slot(d) + 1 - 2 * core
        arrive(2, other)
        query_rows(other)
    relay(len(chunks_left))

    wide = (qn.shape[0], 128)
    wide_left = lax.broadcasted_iota(jnp.int32, wide, 1) < 64

    def queries(slot):
        raw = jnp.dot(qn[...], wqall[slot], preferred_element_type=F32)
        mid, last = raw[:, 128:256], raw[:, 256:384]
        turned = turned_pair(jnp.where(wide_left, mid, last), pl.ds(0, qn.shape[0]))
        qs[slot, :, 0:128] = raw[:, 0:128].astype(BF16)
        qs[slot, :, 128:256] = jnp.where(wide_left, turned, mid).astype(BF16)
        qs[slot, :, 256:384] = jnp.where(wide_left, last, turned).astype(BF16)

    power = HEAD ** (-0.5) * float(np.log2(np.e))
    block = 2 * rows
    causal = lax.broadcasted_iota(jnp.int32, (block, block), 1) <= lax.broadcasted_iota(
        jnp.int32, (block, block), 0
    )

    def attend(c, slot):
        start, stop = c * block, (c + 1) * block
        scores = []
        for hh in range(2):
            score = lax.dot_general(
                qs[slot, start:stop, hh * 128:hh * 128 + 256], ks[2 * slot + hh, 0:stop, :],
                (((1,), (1,)), ((), ())), preferred_element_type=F32,
            )
            last = jnp.where(causal, score[:, start:], -jnp.inf)
            scores.append(jnp.concatenate([score[:, :start], last], axis=1) if c else last)
        tops = [jnp.max(score, axis=-1, keepdims=True) for score in scores]
        weights = [
            jnp.exp2((score - top) * power).astype(BF16) for score, top in zip(scores, tops)
        ]
        for hh in range(2):
            summed = jnp.dot(
                weights[hh], vs[2 * slot + hh, 0:stop, :], preferred_element_type=F32
            )
            result = (summed[:, 0:VDIM] / summed[:, VDIM:2 * VDIM]).astype(BF16)
            for e in range(2):
                att_out[2 * c + e, slot, :, hh * VDIM:(hh + 1) * VDIM] = result[
                    e * rows:(e + 1) * rows
                ]

    def att_copy(b, slot):
        return pltpu.make_async_remote_copy(
            src_ref=att_out.at[b, slot], dst_ref=att_in.at[i, slot],
            send_sem=att_send.at[0], recv_sem=att_recv.at[i, slot],
            device_id={"sp": b}, device_id_type=MESH,
        )

    for t, slot in enumerate((x, across)):
        if t:
            x_copy(wqall.at[across]).wait_recv()
        queries(slot)
        for c in range(n_chips):
            @pl.when(chip != c)
            def _(c=c):
                attend(c, slot)
                for b in (2 * c, 2 * c + 1):
                    att_copy(b, slot).start()
    for slot in (x, across):
        for c in range(n_chips):
            @pl.when(chip == c)
            def _(c=c):
                attend(c, slot)
        att_copy(partner, slot).start()

    wout_copy.wait()
    squares = []
    group = 2 * pair_dim

    def piece(s, slot, local):
        if not local:
            pltpu.make_async_remote_copy(
                src_ref=att_in.at[s, slot], dst_ref=att_in.at[s, slot],
                send_sem=att_send.at[0], recv_sem=att_recv.at[s, slot],
                device_id={"sp": partner}, device_id_type=MESH,
            ).wait_recv()
        values = (att_out if local else att_in)[s, slot].astype(F32)
        squares.append(jnp.sum(values * values, axis=-1, keepdims=True))
        at = pl.multiple_of(s * group + slot * pair_dim, pair_dim)
        gain = ogain[pl.ds(at, pair_dim)].astype(F32).reshape(1, -1)
        return jnp.dot(
            (values * gain).astype(BF16), wout[pl.ds(at, pair_dim), :],
            preferred_element_type=F32,
        )

    acc[...] = piece(i, x, True) + piece(i, across, True)
    acc[...] += piece(partner, x, False) + piece(partner, across, False)
    far = []
    for d in range(1, n_chips):
        far += [far_slot(d), far_slot(d) + 1 - 2 * core]
    steps = [(s, slot) for slot in (x, across) for s in far]
    for s, slot in steps[:-1]:
        acc[...] += piece(s, slot, False)
    term = piece(*steps[-1], False)
    factor = lax.rsqrt(sum(squares[1:], squares[0]) / (n * group) + 1e-05)
    out_ref[0] = ((acc[...] + term) * factor).astype(BF16)

    for a in range(3):
        every = gathered[a][1].at[pl.ds(0, n - 1)]
        pltpu.make_async_remote_copy(
            src_ref=every, dst_ref=every, send_sem=gat_send.at[a], recv_sem=gat_recv.at[a, 0],
            device_id={"sp": partner}, device_id_type=MESH,
        ).wait_send()
    for side in range(4):
        @pl.when(sides[side][0])
        def _(side=side):
            pltpu.make_async_remote_copy(
                src_ref=wqall.at[x], dst_ref=wqall.at[x],
                send_sem=w_send.at[side], recv_sem=w_recv.at[0],
                device_id={"dp": sides[side][1]}, device_id_type=MESH,
            ).wait_send()
    x_copy(wqall.at[x]).wait_send()
    every = att_out.at[pl.ds(0, n - 1)]
    pltpu.make_async_remote_copy(
        src_ref=every, dst_ref=every, send_sem=att_send.at[0], recv_sem=att_recv.at[0, 0],
        device_id={"sp": partner}, device_id_type=MESH,
    ).wait_send()


def paired(
    mesh, columns, q_latent, kv_latent, rope_key, w_query, w_keyval, w_out, query_gain, latent_gain,
    out_gain,
):
    n, m = mesh.shape["sp"], mesh.shape["dp"]
    rows = q_latent.shape[1]
    length = n * rows
    rank = q_latent.shape[2]
    width = w_query.shape[1]
    local_heads = H // n
    chunks = 16
    dim = w_out.shape[1]
    geometry = (n, columns, m // columns, chunks, local_heads)
    any_spec = pl.BlockSpec(memory_space=pl.ANY)
    vmem_spec = pl.BlockSpec(memory_space=pltpu.VMEM)
    dma = pltpu.SemaphoreType.DMA
    return pl.pallas_call(
        functools.partial(paired_kernel, geometry),
        out_shape=pltpu.VMEM((1, rows, dim), BF16),
        in_specs=[any_spec] * 10,
        out_specs=vmem_spec,
        scratch_shapes=[
            pltpu.VMEM((n, rows, rank), BF16),
            pltpu.VMEM((n, rows, kv_latent.shape[2]), BF16),
            pltpu.VMEM((n, ROPE, rows), BF16),
            pltpu.VMEM((columns, rank, width), BF16),
            pltpu.VMEM(w_keyval.shape, BF16),
            pltpu.VMEM(w_out.shape, BF16),
            pltpu.VMEM((length, 256), F32),
            pltpu.VMEM(query_gain.shape, BF16),
            pltpu.VMEM(latent_gain.shape, BF16),
            pltpu.VMEM(out_gain.shape, BF16),
            pltpu.VMEM((length, rank), BF16),
            pltpu.VMEM((columns, length, width), BF16),
            pltpu.VMEM((local_heads, length, 256), BF16),
            pltpu.VMEM((local_heads, length, 2 * VDIM), BF16),
            pltpu.VMEM((n, columns, rows, 2 * VDIM), BF16),
            pltpu.VMEM((n, columns, rows, 2 * VDIM), BF16),
            pltpu.VMEM((rows, dim), F32),
            dma((10,)),
            dma((3,)),
            dma((3, n)),
            dma((5,)),
            dma((chunks,)),
            dma((1,)),
            dma((1,)),
            dma((n, columns)),
        ],
        compiler_params=pltpu.CompilerParams(
            collective_id=0, has_side_effects=True, vmem_limit_bytes=56 * 1024 * 1024
        ),
    )(
        q_latent, kv_latent, jnp.swapaxes(rope_key, 1, 2), w_query, w_keyval, w_out,
        jnp.asarray(paired_table(length)), query_gain, latent_gain, out_gain,
    )


def x_size(mesh):
    row = mesh.devices[0]
    places = [getattr(device, "coords", None) for device in row]
    if any(place is None for place in places):
        return 1
    return len({place[0] for place in places})


def per_device(
    mesh, q_latent, kv_latent, rope_key, w_query, w_keyval, w_out, query_gain, latent_gain, out_gain
):
    n, m = mesh.shape["sp"], mesh.shape["dp"]
    rows = q_latent.shape[1]
    length = n * rows
    rank = q_latent.shape[2]
    width = w_query.shape[1]
    local_heads = H // n
    k = local_heads * HEAD // width
    chunks = 16
    columns = x_size(mesh)
    groups = k if k == columns == 2 and width % HEAD == 0 else 1
    dim = w_out.shape[1]
    group = local_heads * VDIM
    if groups == columns and width == 2 * HEAD and H % m == 0 and m == n * columns:
        return paired(
            mesh, columns, q_latent, kv_latent, rope_key, w_query, w_keyval, w_out, query_gain,
            latent_gain, out_gain,
        )
    table = jnp.asarray(turn_table(length))
    geometry = (n, m, columns, k, chunks, local_heads, groups)
    any_spec = pl.BlockSpec(memory_space=pl.ANY)
    vmem_spec = pl.BlockSpec(memory_space=pltpu.VMEM)
    dma = pltpu.SemaphoreType.DMA
    return pl.pallas_call(
        functools.partial(kernel, geometry),
        out_shape=pltpu.VMEM((1, rows, dim), BF16),
        in_specs=[any_spec] * 7 + [vmem_spec] * 3,
        out_specs=vmem_spec,
        scratch_shapes=[
            pltpu.VMEM((n, rows, rank), BF16),
            pltpu.VMEM((n, rows, kv_latent.shape[2]), BF16),
            pltpu.VMEM((n, ROPE, rows), BF16),
            pltpu.VMEM((k, rank, width), BF16),
            pltpu.VMEM(w_keyval.shape, BF16),
            pltpu.VMEM(w_out.shape, BF16),
            pltpu.VMEM((length, 128), F32),
            pltpu.VMEM((local_heads // groups, width, 256), BF16),
            pltpu.VMEM((length, rank), BF16),
            pltpu.VMEM((local_heads, length, 256), BF16),
            pltpu.VMEM((local_heads, length, 256), BF16),
            pltpu.VMEM((local_heads, length, VDIM), BF16),
            pltpu.VMEM((n, groups, rows, group // groups), BF16),
            pltpu.VMEM((n, groups, rows, group // groups), BF16),
            pltpu.VMEM((rows, dim), F32),
            pltpu.VMEM((n, 1, group), F32),
            dma((7,)),
            dma((3, n // 2)),
            dma((3, n)),
            dma((3, n // 2)),
            dma((4, k, chunks)),
            dma((k, chunks)),
            dma((n, groups)),
            dma((n, groups)),
        ],
        compiler_params=pltpu.CompilerParams(
            collective_id=0, has_side_effects=True, vmem_limit_bytes=56 * 1024 * 1024
        ),
    )(
        q_latent, kv_latent, jnp.swapaxes(rope_key, 1, 2), w_query, w_keyval, w_out, table,
        query_gain, latent_gain, out_gain,
    )


def solution(mesh):
    in_specs = (
        P("dp", "sp", None),
        P("dp", "sp", None),
        P("dp", "sp", None),
        P(None, "dp"),
        P(None, "sp"),
        P(),
        P(),
        P(),
        P(),
    )
    return jax.shard_map(
        functools.partial(per_device, mesh), mesh=mesh, in_specs=in_specs,
        out_specs=P("dp", "sp", None), check_vma=False,
    )
```

```python
import functools

import jax
import jax.numpy as jnp
import numpy as np
from jax import lax
from jax.experimental import pallas as pl
from jax.experimental.pallas import tpu as pltpu
from jax.sharding import PartitionSpec as P

H = 16
NOPE = 128
ROPE = 64
VDIM = 128
HEAD = NOPE + ROPE
MESH = pl.DeviceIdType.MESH
F32 = jnp.float32
BF16 = jnp.bfloat16


def turn_table(length):
    half = ROPE // 2
    inverse = np.float32(10000.0) ** (-np.arange(half, dtype=np.float32) / np.float32(half))
    angles = np.arange(length, dtype=np.float32)[:, None] * inverse[None, :].astype(np.float32)
    angles = angles.astype(np.float64)
    cosine, sine = np.cos(angles), np.sin(angles)
    return np.concatenate([cosine, cosine, sine, sine], axis=1).astype(np.float32)


def spread_matrix(rows, row_start, head):
    g = lax.broadcasted_iota(jnp.int32, (rows, 256), 0) + row_start
    f = lax.broadcasted_iota(jnp.int32, (rows, 256), 1)
    source = jnp.where(f < HEAD, f, jnp.where(f < HEAD + 32, f - 32, f - 96)) + head * HEAD
    sign = jnp.where((f >= HEAD) & (f < HEAD + 32), -1.0, 1.0)
    return jnp.where(g == source, sign, 0.0).astype(BF16)


def rope_matrix():
    r = lax.broadcasted_iota(jnp.int32, (ROPE, 128), 0)
    f = lax.broadcasted_iota(jnp.int32, (ROPE, 128), 1)
    source = jnp.where(f < 64, f, jnp.where(f < 96, f - 32, f - 96))
    sign = jnp.where((f >= 64) & (f < 96), -1.0, 1.0)
    return jnp.where(r == source, sign, 0.0).astype(BF16)


def scaled_rows(values, gain):
    wide = values.astype(F32)
    mean = jnp.mean(wide * wide, axis=-1, keepdims=True)
    return (wide * lax.rsqrt(mean + 1e-05) * gain).astype(BF16)


def kernel(
    geometry,
    q_ref, kv_ref, rope_ref, wq_ref, wkv_ref, wout_ref, table_ref, qg_ref, lg_ref, og_ref,
    out_ref,
    qall, kvall, ropeall, wqall, wkv, wout, table, spread, qn, qs, ks, vs, att_out, att_in, acc,
    out_gain,
    local_sem, gat_send, gat_recv, fwd_send, w_send, w_recv, att_send, att_recv,
):
    n, m, X, k, chunks, local_heads, groups = geometry
    per_group = local_heads // groups
    width = wqall.shape[2]
    Z = m // X
    rows = q_ref.shape[1]
    n_chips = n // 2
    i = lax.axis_index("sp")
    j = lax.axis_index("dp")
    core = lax.rem(i, 2)
    chip = lax.div(i, 2)
    partner = i + 1 - 2 * core
    z = lax.div(j, X)
    x = lax.rem(j, X)
    first = i * k
    owns = (j >= first) & (j < first + k)

    gathered = ((kv_ref.at[0], kvall), (rope_ref.at[0], ropeall), (q_ref.at[0], qall))
    own_copies = [
        pltpu.make_async_copy(src, dst.at[i], local_sem.at[a]) for a, (src, dst) in enumerate(gathered)
    ]
    wq_copy = pltpu.make_async_copy(wq_ref, wqall.at[lax.rem(j, k)], local_sem.at[3])
    wkv_copy = pltpu.make_async_copy(wkv_ref, wkv, local_sem.at[4])
    table_copy = pltpu.make_async_copy(table_ref, table, local_sem.at[5])
    wout_copy = pltpu.make_async_copy(wout_ref, wout, local_sem.at[6])

    @pl.when(owns)
    def _():
        wq_copy.start()

    for copy in own_copies:
        copy.start()
    wkv_copy.start()
    table_copy.start()
    wout_copy.start()

    turner = rope_matrix()
    latent_gain = lg_ref[...].astype(F32).reshape(1, -1)
    query_gain = qg_ref[...].astype(F32).reshape(1, -1)
    group = local_heads * VDIM
    every_gain = og_ref[...].astype(F32).reshape(1, -1)
    for s in range(n):
        out_gain[s] = every_gain[:, s * group:(s + 1) * group]
    if groups > 1:
        for h in range(per_group):
            spread[h] = spread_matrix(width, 0, h)

    barrier = pltpu.get_barrier_semaphore()
    for d in range(1, n):
        pl.semaphore_signal(
            barrier, inc=1, device_id={"sp": lax.rem(i + d, n)}, device_id_type=MESH
        )
    sides = ((z < Z - 1, j + X), (z > 0, j - X), (x < X - 1, j + 1), (x > 0, j - 1))
    count = n - 1
    for present, target in sides:
        @pl.when(present)
        def _(target=target):
            pl.semaphore_signal(barrier, inc=1, device_id={"dp": target}, device_id_type=MESH)
        count = count + jnp.where(present, 1, 0)
    pl.semaphore_wait(barrier, count)

    step_rows = wqall.shape[1] // chunks

    def relay_parts(slot, c):
        owner = first + slot
        zo, xo = lax.div(owner, X), lax.rem(owner, X)
        part = wqall.at[slot, pl.ds(c * step_rows, step_rows)]
        in_column = x == xo
        conditions = (
            in_column & (z >= zo) & (z < Z - 1),
            in_column & (z <= zo) & (z > 0),
            (x >= xo) & (x < X - 1),
            (x <= xo) & (x > 0),
        )
        copies = [
            pltpu.make_async_remote_copy(
                src_ref=part, dst_ref=part,
                send_sem=w_send.at[side, slot, c], recv_sem=w_recv.at[slot, c],
                device_id={"dp": sides[side][1]}, device_id_type=MESH,
            )
            for side in range(4)
        ]
        return owner, conditions, copies

    def relay(slot, c):
        owner, conditions, copies = relay_parts(slot, c)

        @pl.when(owner != j)
        def _():
            copies[0].wait_recv()

        for condition, copy in zip(conditions, copies):
            @pl.when(condition)
            def _(copy=copy):
                copy.start()

    def relay_finish(slot, c):
        _, conditions, copies = relay_parts(slot, c)
        for condition, copy in zip(conditions, copies):
            @pl.when(condition)
            def _(copy=copy):
                copy.wait_send()

    if groups > 1:
        columns = [lax.rem(x + t, k) for t in range(k)]
        events = [[(column, c) for c in range(chunks)] for column in columns]
    else:
        columns = [0]
        events = [[(slot, c) for c in range(chunks) for slot in range(k)]]
    events_left = list(events[0])

    def relay_some(number):
        for _ in range(min(number, len(events_left))):
            relay(*events_left.pop(0))

    def gather_copy(a, slot, sem, target):
        dst = gathered[a][1]
        return pltpu.make_async_remote_copy(
            src_ref=dst.at[slot], dst_ref=dst.at[slot],
            send_sem=sem, recv_sem=gat_recv.at[a, slot],
            device_id={"sp": target}, device_id_type=MESH,
        )

    sends = []

    @pl.when(owns)
    def _():
        wq_copy.wait()

    for a in range(3):
        own_copies[a].wait()
        for d in range(1, n_chips):
            target = 2 * lax.rem(chip + d, n_chips) + core
            sends.append(gather_copy(a, i, gat_send.at[a, d], target))
            sends[-1].start()
    for a in range(3):
        sends.append(gather_copy(a, i, gat_send.at[a, 0], partner))
        sends[-1].start()

    def far_slot(d):
        return 2 * lax.rem(chip + n_chips - d, n_chips) + core

    def forward(a, d):
        slot = far_slot(d)
        copy = gather_copy(a, slot, fwd_send.at[a, d - 1], partner)
        copy.wait_recv()
        copy.start()
        sends.append(copy)

    def arrive(a, slot):
        gather_copy(a, slot, gat_send.at[a, 0], partner).wait_recv()

    lane = lax.broadcasted_iota(jnp.int32, (rows, 128), 1)

    def keyval(slot):
        at = pl.ds(pl.multiple_of(slot * rows, rows), rows)
        both = jnp.dot(
            scaled_rows(kvall[slot], latent_gain), wkv[...], preferred_element_type=F32
        ).astype(BF16)
        pair = lax.dot_general(
            ropeall[slot], turner, (((0,), (0,)), ((), ())), preferred_element_type=F32
        ) * table[at, :]
        pair = pair + pltpu.roll(pair, 64, 1)
        turned = jnp.where(lane < 64, pair, 0.0).astype(BF16)
        for h in range(local_heads):
            base = h * (NOPE + VDIM)
            ks[h, at, 0:NOPE] = both[:, base:base + NOPE]
            ks[h, at, NOPE:256] = turned
            vs[h, at, :] = both[:, base + NOPE:base + NOPE + VDIM]

    def query_rows(slot):
        at = pl.ds(pl.multiple_of(slot * rows, rows), rows)
        qn[at, :] = scaled_rows(qall[slot], query_gain)

    relay_some(k + 1)
    wkv_copy.wait()
    table_copy.wait()
    keyval(i)
    relay_some(1)
    query_rows(i)
    relay_some(1)
    arrive(0, partner)
    arrive(1, partner)
    keyval(partner)
    relay_some(1)
    for d in range(1, n_chips):
        forward(0, d)
        forward(1, d)
        keyval(far_slot(d))
        relay_some(1)
    arrive(2, partner)
    query_rows(partner)
    relay_some(2)
    for d in range(1, n_chips):
        other = far_slot(d) + 1 - 2 * core
        arrive(0, other)
        arrive(1, other)
        keyval(other)
        relay_some(2)
    for d in range(1, n_chips):
        forward(2, d)
        query_rows(far_slot(d))
        relay_some(2)
    for d in range(1, n_chips):
        other = far_slot(d) + 1 - 2 * core
        arrive(2, other)
        query_rows(other)
    relay_some(len(events_left))

    def raw_queries(slot, hh):
        if groups > 1:
            total = jnp.dot(wqall[slot], spread[hh], preferred_element_type=F32)
        else:
            total = None
            for s in range(k):
                if (s + 1) * width <= hh * HEAD or s * width >= (hh + 1) * HEAD:
                    continue
                term = jnp.dot(
                    wqall[s], spread_matrix(width, s * width, hh), preferred_element_type=F32
                )
                total = term if total is None else total + term
        return jnp.dot(qn[...], total.astype(BF16), preferred_element_type=F32)

    def queries(slot):
        for hh in range(per_group):
            h = slot * per_group + hh
            raw = raw_queries(slot, hh)
            qs[h, :, 0:NOPE] = raw[:, 0:NOPE].astype(BF16)
            pair = raw[:, NOPE:256] * table[...]
            qs[h, :, NOPE:256] = (pair + pltpu.roll(pair, 64, 1)).astype(BF16)

    power = HEAD ** (-0.5) * float(np.log2(np.e))
    causal = lax.broadcasted_iota(jnp.int32, (rows, rows), 1) <= lax.broadcasted_iota(
        jnp.int32, (rows, rows), 0
    )

    def attend(b, slot):
        stop = (b + 1) * rows
        for hh in range(per_group):
            h = slot * per_group + hh
            scores = lax.dot_general(
                qs[h, b * rows:stop, :], ks[h, 0:stop, :], (((1,), (1,)), ((), ())),
                preferred_element_type=F32,
            )
            last = jnp.where(causal, scores[:, b * rows:], -jnp.inf)
            if b:
                scores = jnp.concatenate([scores[:, :b * rows], last], axis=1)
            else:
                scores = last
            top = jnp.max(scores, axis=-1, keepdims=True)
            weights = jnp.exp2((scores - top) * power)
            row_total = jnp.sum(weights, axis=-1, keepdims=True)
            summed = jnp.dot(weights.astype(BF16), vs[h, 0:stop, :], preferred_element_type=F32)
            att_out[b, slot, :, hh * VDIM:(hh + 1) * VDIM] = (summed / row_total).astype(BF16)

    def att_copy(b, slot):
        return pltpu.make_async_remote_copy(
            src_ref=att_out.at[b, slot], dst_ref=att_in.at[i, slot],
            send_sem=att_send.at[b, slot], recv_sem=att_recv.at[i, slot],
            device_id={"sp": b}, device_id_type=MESH,
        )

    for t, slot in enumerate(columns):
        if t:
            for event in events[t]:
                relay(*event)
        queries(slot)
        for c in range(n_chips):
            @pl.when(chip != c)
            def _(c=c):
                for b in (2 * c, 2 * c + 1):
                    attend(b, slot)
                    att_copy(b, slot).start()
    for c in range(n_chips):
        @pl.when(chip == c)
        def _(c=c):
            for slot in columns:
                for b in (2 * c, 2 * c + 1):
                    attend(b, slot)
    for slot in columns:
        att_copy(partner, slot).start()

    wout_copy.wait()
    squares = None
    order = [partner]
    for d in range(1, n_chips):
        order += [far_slot(d), far_slot(d) + 1 - 2 * core]
    for t, s in enumerate([i] + order):
        source = att_out
        if t:
            source = att_in
            for slot in range(groups):
                pltpu.make_async_remote_copy(
                    src_ref=att_in.at[s, slot], dst_ref=att_in.at[s, slot],
                    send_sem=att_send.at[0, slot], recv_sem=att_recv.at[s, slot],
                    device_id={"sp": partner}, device_id_type=MESH,
                ).wait_recv()
        values = jnp.concatenate([source[s, slot] for slot in range(groups)], axis=1).astype(F32)
        at = pl.ds(pl.multiple_of(s * group, group), group)
        square = jnp.sum(values * values, axis=-1, keepdims=True)
        squares = square if squares is None else squares + square
        scaled = (values * out_gain[s]).astype(BF16)
        term = jnp.dot(scaled, wout[at, :], preferred_element_type=F32)
        if t == 0:
            acc[...] = term
        elif t < n - 1:
            acc[...] += term
        else:
            factor = lax.rsqrt(squares / (n * group) + 1e-05)
            out_ref[0] = ((acc[...] + term) * factor).astype(BF16)

    for copy in sends:
        copy.wait_send()
    for event in sum(events, []):
        relay_finish(*event)
    for b in range(n):
        @pl.when(i != b)
        def _(b=b):
            for slot in range(groups):
                att_copy(b, slot).wait_send()


def paired_table(length):
    half = ROPE // 2
    inverse = np.float32(10000.0) ** (-np.arange(half, dtype=np.float32) / np.float32(half))
    angles = np.arange(length, dtype=np.float32)[:, None] * inverse[None, :].astype(np.float32)
    angles = angles.astype(np.float64)
    cosine, sine = np.cos(angles), np.sin(angles)
    parts = [cosine] * 4 + [-sine, sine, -sine, sine]
    return np.concatenate(parts, axis=1).astype(np.float32)


def paired_kernel(
    geometry,
    q_ref, kv_ref, rope_ref, wq_ref, wkv_ref, wout_ref, table_ref, qg_ref, lg_ref, og_ref,
    out_ref,
    qall, kvall, ropeall, wqa, wqb, assist, wkv, wout, table, qgain, lgain, ogain, head_gain, qn, qs, ks, vs,
    att_out, att_in, acc,
    local_sem, gat_send, gat_recv, w_send, w_recv, x_recv, att_send, att_recv,
):
    n, X, Z, chunks, local_heads = geometry
    whead = (wqa, wqb)
    first_width = wqa.shape[2]
    rows = q_ref.shape[1]
    n_chips = n // 2
    i = lax.axis_index("sp")
    j = lax.axis_index("dp")
    core = lax.rem(i, 2)
    chip = lax.div(i, 2)
    partner = i + 1 - 2 * core
    z = lax.div(j, X)
    x = lax.rem(j, X)
    across = 1 - x
    zo = i
    owns = z == zo

    gathered = ((kv_ref.at[0], kvall), (rope_ref.at[0], ropeall), (q_ref.at[0], qall))
    own_copies = [
        pltpu.make_async_copy(src, dst.at[i], local_sem.at[a]) for a, (src, dst) in enumerate(gathered)
    ]
    wq_copies = [
        pltpu.make_async_copy(wq_ref.at[:, 0:first_width], wqa.at[x], local_sem.at[3]),
        pltpu.make_async_copy(
            wq_ref.at[:, first_width:first_width + wqb.shape[2]], wqb.at[x], local_sem.at[10]
        ),
    ]
    wkv_copy = pltpu.make_async_copy(wkv_ref, wkv, local_sem.at[4])
    table_copy = pltpu.make_async_copy(table_ref, table, local_sem.at[5])
    wout_copy = pltpu.make_async_copy(wout_ref, wout, local_sem.at[6])
    gain_copies = [
        pltpu.make_async_copy(src, dst, local_sem.at[7 + a])
        for a, (src, dst) in enumerate(((qg_ref, qgain), (lg_ref, lgain), (og_ref, ogain)))
    ]

    assist_copy = pltpu.make_async_copy(
        wq_ref.at[:, first_width:first_width + wqb.shape[2]], assist, local_sem.at[11]
    )

    barrier = pltpu.get_barrier_semaphore()
    for d in range(1, n):
        pl.semaphore_signal(
            barrier, inc=1, device_id={"sp": lax.rem(i + d, n)}, device_id_type=MESH
        )
    def places(owner):
        low = owner * 2 < Z
        inner = owner == jnp.where(low, 1, Z - 2)
        last = jnp.where(low, Z - 1, 0)
        relayer = jnp.where(low, Z - 2, 1)
        return last, relayer, jnp.where(low, jnp.where(inner, 0, 1), jnp.where(inner, Z - 1, Z - 2))

    end, mid, other = places(zo)
    at_mid, at_end, at_other = z == mid, z == end, z == other
    twin = lax.rem(i + n // 2, n)
    twin_end = places(twin)[0]
    assists = z == twin

    def row(target, column=x):
        return target * X + column

    greet = (
        (at_other | at_mid, {"dp": row(zo)}), (at_end, {"dp": row(mid)}),
        (at_end, {"sp": twin, "dp": row(zo)}), (at_end, {"sp": twin, "dp": row(zo, across)}),
    )
    pl.semaphore_signal(barrier, inc=1, device_id={"dp": row(z, across)}, device_id_type=MESH)
    count = n + jnp.where(owns, 2, 0) + jnp.where(at_mid, 1, 0) + jnp.where(assists, 2, 0)
    for present, target in greet:
        @pl.when(present)
        def _(target=target):
            pl.semaphore_signal(barrier, inc=1, device_id=target, device_id_type=MESH)

    @pl.when(assists)
    def _():
        assist_copy.start()

    @pl.when(owns)
    def _():
        for copy in wq_copies:
            copy.start()

    for copy in own_copies:
        copy.start()
    for copy in gain_copies:
        copy.start()
    wkv_copy.start()
    table_copy.start()
    wout_copy.start()

    for h in range(local_heads):
        vs[h, :, VDIM:2 * VDIM] = jnp.ones((vs.shape[1], VDIM), BF16)
    r = lax.broadcasted_iota(jnp.int32, (ROPE, 128), 0)
    f = lax.broadcasted_iota(jnp.int32, (ROPE, 128), 1)
    turner = jnp.where(r == lax.rem(f, ROPE), 1.0, 0.0).astype(BF16)

    parts = [(part, c) for part in range(2) for c in range(chunks[part])]

    def w_part(index):
        part, c = parts[index]
        step = whead[part].shape[1] // chunks[part]
        return whead[part].at[x, pl.ds(c * step, step)]

    targets = (row(other), row(mid), row(end))

    def assist_send(column, sem):
        return pltpu.make_async_remote_copy(
            src_ref=assist, dst_ref=wqb.at[x], send_sem=w_send.at[10 + sem],
            recv_sem=x_recv.at[1 + sem],
            device_id={"sp": twin, "dp": row(twin_end, column)}, device_id_type=MESH,
        )

    def w_copy(side, c):
        part = w_part(c)
        return pltpu.make_async_remote_copy(
            src_ref=part, dst_ref=part, send_sem=w_send.at[4 * parts[c][0] + side], recv_sem=w_recv.at[c],
            device_id={"dp": targets[side]}, device_id_type=MESH,
        )

    def x_copy(source, part):
        return pltpu.make_async_remote_copy(
            src_ref=source, dst_ref=source, send_sem=w_send.at[8 + part], recv_sem=x_recv.at[part],
            device_id={"dp": j + 1 - 2 * x}, device_id_type=MESH,
        )

    late = at_end
    soon = at_mid | at_other
    chunks_left = {True: list(range(len(parts))), False: list(range(len(parts)))}

    def relay_one(index):
        w_copy(0, index).wait_recv()
        if parts[index][0] == 0:
            @pl.when(at_mid)
            def _():
                w_copy(2, index).start()
        x_copy(w_part(index), parts[index][0]).start()

    chunks_left[True] = chunks_left[True][:chunks[0]]

    def relay(early, after):
        for is_late, number in ((False, early), (True, after)):
            left = chunks_left[is_late]
            todo = [left.pop(0) for _ in range(min(number, len(left)))]
            if todo:
                @pl.when(late if is_late else soon)
                def _(todo=todo):
                    for index in todo:
                        relay_one(index)

    def gather_copy(a, slot, target):
        dst = gathered[a][1]
        return pltpu.make_async_remote_copy(
            src_ref=dst.at[slot], dst_ref=dst.at[slot],
            send_sem=gat_send.at[a], recv_sem=gat_recv.at[a, slot],
            device_id={"sp": target}, device_id_type=MESH,
        )

    def far_slot(d):
        return 2 * lax.rem(chip + n_chips - d, n_chips) + core

    def forward(a, d):
        slot = far_slot(d)
        copy = gather_copy(a, slot, partner)
        copy.wait_recv()
        copy.start()

    def arrive(a, slot):
        gather_copy(a, slot, partner).wait_recv()

    lane = lax.broadcasted_iota(jnp.int32, (rows, 128), 1)
    left = lane < 64

    def turned_pair(both_halves, at):
        swap_low = lax.rem(lax.broadcasted_iota(jnp.int32, both_halves.shape, 1), 64) < 32
        swapped = jnp.where(
            swap_low, pltpu.roll(both_halves, 96, 1), pltpu.roll(both_halves, 32, 1)
        )
        return both_halves * table[at, 0:128] + swapped * table[at, 128:256]

    def keyval(slot):
        at = pl.ds(pl.multiple_of(slot * rows, rows), rows)
        both = jnp.dot(
            scaled_rows(kvall[slot], lgain[...].astype(F32).reshape(1, -1)), wkv[...],
            preferred_element_type=F32,
        )
        twice = lax.dot_general(
            ropeall[slot], turner, (((0,), (0,)), ((), ())), preferred_element_type=F32
        )
        turned = turned_pair(twice, at)
        for h in range(local_heads):
            base = h * (NOPE + VDIM)
            key = both[:, base:base + NOPE]
            if h % 2 == 0:
                ks[h, at, 0:NOPE] = key.astype(BF16)
                ks[h, at, NOPE:256] = jnp.where(left, turned, 0.0).astype(BF16)
            else:
                key = pltpu.roll(key, 64, 1)
                ks[h, at, 0:NOPE] = jnp.where(left, 0.0, key).astype(BF16)
                ks[h, at, NOPE:256] = jnp.where(left, key, turned).astype(BF16)
            vs[h, at, 0:VDIM] = both[:, base + NOPE:base + NOPE + VDIM].astype(BF16)

    def query_rows(slot):
        at = pl.ds(pl.multiple_of(slot * rows, rows), rows)
        qn[at, :] = scaled_rows(qall[slot], qgain[...].astype(F32).reshape(1, -1))

    for copy in own_copies:
        copy.wait()
    for copy in gain_copies:
        copy.wait()
    query_rows(i)
    every_gain = ogain[...].astype(F32).reshape(1, -1)
    for h in range(n * local_heads):
        head_gain[h] = every_gain[:, h * VDIM:(h + 1) * VDIM]

    @pl.when(owns)
    def _():
        for copy in wq_copies:
            copy.wait()

    pl.semaphore_wait(barrier, count)

    for a in range(3):
        for d in range(1, n_chips):
            gather_copy(a, i, 2 * lax.rem(chip + d, n_chips) + core).start()

    @pl.when(owns)
    def _():
        for part in range(2):
            x_copy(whead[part].at[x], part).start()
        for index in range(len(parts)):
            w_copy(1, index).start()
            w_copy(0, index).start()

    for a in range(3):
        gather_copy(a, i, partner).start()

    wkv_copy.wait()
    table_copy.wait()
    keyval(i)
    arrive(0, partner)
    arrive(1, partner)
    keyval(partner)
    arrive(2, partner)
    query_rows(partner)
    relay(4, 0)
    for d in range(1, n_chips):
        forward(0, d)
        forward(1, d)
        relay(1, 0)
        keyval(far_slot(d))
    @pl.when(assists)
    def _():
        assist_copy.wait()
        assist_send(x, 1).start()

    relay(1, 1)
    for d in range(1, n_chips):
        other = far_slot(d) + 1 - 2 * core
        arrive(0, other)
        arrive(1, other)
        keyval(other)
    @pl.when(assists)
    def _():
        assist_send(across, 0).start()

    relay(1, 2)
    for d in range(1, n_chips):
        forward(2, d)
        query_rows(far_slot(d))
    relay(1, 1)
    for d in range(1, n_chips):
        other = far_slot(d) + 1 - 2 * core
        arrive(2, other)
        query_rows(other)
    relay(1, 5)

    wide = (qn.shape[0], 128)
    wide_left = lax.broadcasted_iota(jnp.int32, wide, 1) < 64

    def queries(slot, part):
        raw = jnp.dot(qn[...], whead[part][slot], preferred_element_type=F32)
        last = raw[:, raw.shape[1] - 128:]
        turned = turned_pair(last, pl.ds(0, qn.shape[0]))
        if part == 0:
            qs[slot, :, 0:128] = raw[:, 0:128].astype(BF16)
            qs[slot, :, 128:256] = jnp.where(wide_left, turned, last).astype(BF16)
        else:
            qs[slot, :, 256:384] = jnp.where(wide_left, last, turned).astype(BF16)

    power = HEAD ** (-0.5) * float(np.log2(np.e))
    block = 2 * rows
    causal = lax.broadcasted_iota(jnp.int32, (block, block), 1) <= lax.broadcasted_iota(
        jnp.int32, (block, block), 0
    )

    def attend(c, slot, heads):
        start, stop = c * block, (c + 1) * block
        scores = []
        for hh in heads:
            score = lax.dot_general(
                qs[slot, start:stop, hh * 128:hh * 128 + 256], ks[2 * slot + hh, 0:stop, :],
                (((1,), (1,)), ((), ())), preferred_element_type=F32,
            )
            last = jnp.where(causal, score[:, start:], -jnp.inf)
            scores.append(jnp.concatenate([score[:, :start], last], axis=1) if c else last)
        tops = [jnp.max(score, axis=-1, keepdims=True) for score in scores]
        weights = [
            jnp.exp2((score - top) * power).astype(BF16) for score, top in zip(scores, tops)
        ]
        for hh, weight in zip(heads, weights):
            summed = jnp.dot(weight, vs[2 * slot + hh, 0:stop, :], preferred_element_type=F32)
            result = (summed[:, 0:VDIM] / summed[:, VDIM:2 * VDIM]).astype(BF16)
            for e in range(2):
                att_out[2 * c + e, 2 * slot + hh] = result[e * rows:(e + 1) * rows]

    def att_copy(b, head):
        return pltpu.make_async_remote_copy(
            src_ref=att_out.at[b, head], dst_ref=att_in.at[i, head],
            send_sem=att_send.at[0], recv_sem=att_recv.at[i, head],
            device_id={"sp": b}, device_id_type=MESH,
        )

    def attend_far(slot, hh):
        for c in range(n_chips):
            @pl.when(chip != c)
            def _(c=c):
                attend(c, slot, (hh,))
                for b in (2 * c, 2 * c + 1):
                    att_copy(b, 2 * slot + hh).start()

    def attend_own(slot):
        for c in range(n_chips):
            @pl.when(chip == c)
            def _(c=c):
                attend(c, slot, (0, 1))
        for hh in range(2):
            att_copy(partner, 2 * slot + hh).start()

    queries(x, 0)
    relay(1, 0)
    attend_far(x, 0)
    relay(len(parts), 0)

    @pl.when(at_end)
    def _():
        assist_send(x, 1).wait_recv()

    queries(x, 1)
    attend_far(x, 1)
    attend_own(x)
    for part in range(2):
        x_copy(whead[part].at[across], part).wait_recv()
        queries(across, part)
        attend_far(across, part)
    attend_own(across)

    wout_copy.wait()
    squares = []
    group = local_heads * VDIM

    def piece(s, first, count, local):
        chosen = []
        for hh in range(count):
            if not local:
                pltpu.make_async_remote_copy(
                    src_ref=att_in.at[s, first + hh], dst_ref=att_in.at[s, first + hh],
                    send_sem=att_send.at[0], recv_sem=att_recv.at[s, first + hh],
                    device_id={"sp": partner}, device_id_type=MESH,
                ).wait_recv()
            chosen.append((att_out if local else att_in)[s, first + hh])
        values = jnp.concatenate(chosen, axis=1).astype(F32)
        squares.append(jnp.sum(values * values, axis=-1, keepdims=True))
        at = pl.multiple_of(s * group + first * VDIM, VDIM)
        gain = jnp.concatenate(
            [head_gain[s * local_heads + first + hh] for hh in range(count)], axis=1
        )
        return jnp.dot(
            (values * gain).astype(BF16), wout[pl.ds(at, count * VDIM), :],
            preferred_element_type=F32,
        )

    acc[...] = piece(i, 0, local_heads, True)
    acc[...] += piece(partner, 0, local_heads, False)
    far = []
    for d in range(1, n_chips):
        far += [far_slot(d), far_slot(d) + 1 - 2 * core]
    steps = [(s, 2 * x, 2) for s in far]
    steps += [(s, 2 * across + hh, 1) for hh in range(2) for s in far]
    for step in steps[:-1]:
        acc[...] += piece(*step, False)
    term = piece(*steps[-1], False)
    factor = lax.rsqrt(sum(squares[1:], squares[0]) / (n * group) + 1e-05)
    out_ref[0] = ((acc[...] + term) * factor).astype(BF16)

    for a in range(3):
        every = gathered[a][1].at[pl.ds(0, n - 1)]
        pltpu.make_async_remote_copy(
            src_ref=every, dst_ref=every, send_sem=gat_send.at[a], recv_sem=gat_recv.at[a, 0],
            device_id={"sp": partner}, device_id_type=MESH,
        ).wait_send()
    for part in range(2):
        for side, sender in ((0, owns), (1, owns), (2, at_mid)):
            if part == 0 or side < 2:
                @pl.when(sender)
                def _(side=side, part=part):
                    pltpu.make_async_remote_copy(
                        src_ref=whead[part].at[x], dst_ref=whead[part].at[x],
                        send_sem=w_send.at[4 * part + side], recv_sem=w_recv.at[0],
                        device_id={"dp": targets[side]}, device_id_type=MESH,
                    ).wait_send()

    @pl.when(assists)
    def _():
        assist_send(x, 1).wait_send()
        assist_send(across, 0).wait_send()

    x_copy(wqa.at[x], 0).wait_send()

    @pl.when(jnp.logical_not(at_end))
    def _():
        x_copy(wqb.at[x], 1).wait_send()

    every = att_out.at[pl.ds(0, n - 1)]
    pltpu.make_async_remote_copy(
        src_ref=every, dst_ref=every, send_sem=att_send.at[0], recv_sem=att_recv.at[0, 0],
        device_id={"sp": partner}, device_id_type=MESH,
    ).wait_send()


def paired(
    mesh, columns, q_latent, kv_latent, rope_key, w_query, w_keyval, w_out, query_gain, latent_gain,
    out_gain,
):
    n, m = mesh.shape["sp"], mesh.shape["dp"]
    rows = q_latent.shape[1]
    length = n * rows
    rank = q_latent.shape[2]
    width = w_query.shape[1]
    local_heads = H // n
    chunks = (8, 4)
    dim = w_out.shape[1]
    geometry = (n, columns, m // columns, chunks, local_heads)
    any_spec = pl.BlockSpec(memory_space=pl.ANY)
    vmem_spec = pl.BlockSpec(memory_space=pltpu.VMEM)
    dma = pltpu.SemaphoreType.DMA
    return pl.pallas_call(
        functools.partial(paired_kernel, geometry),
        out_shape=pltpu.VMEM((1, rows, dim), BF16),
        in_specs=[any_spec] * 10,
        out_specs=vmem_spec,
        scratch_shapes=[
            pltpu.VMEM((n, rows, rank), BF16),
            pltpu.VMEM((n, rows, kv_latent.shape[2]), BF16),
            pltpu.VMEM((n, ROPE, rows), BF16),
            pltpu.VMEM((columns, rank, 2 * NOPE), BF16),
            pltpu.VMEM((columns, rank, width - 2 * NOPE), BF16),
            pltpu.VMEM((rank, width - 2 * NOPE), BF16),
            pltpu.VMEM(w_keyval.shape, BF16),
            pltpu.VMEM(w_out.shape, BF16),
            pltpu.VMEM((length, 256), F32),
            pltpu.VMEM(query_gain.shape, BF16),
            pltpu.VMEM(latent_gain.shape, BF16),
            pltpu.VMEM(out_gain.shape, BF16),
            pltpu.VMEM((n * local_heads, 1, VDIM), F32),
            pltpu.VMEM((length, rank), BF16),
            pltpu.VMEM((columns, length, width), BF16),
            pltpu.VMEM((local_heads, length, 256), BF16),
            pltpu.VMEM((local_heads, length, 2 * VDIM), BF16),
            pltpu.VMEM((n, local_heads, rows, VDIM), BF16),
            pltpu.VMEM((n, local_heads, rows, VDIM), BF16),
            pltpu.VMEM((rows, dim), F32),
            dma((12,)),
            dma((3,)),
            dma((3, n)),
            dma((12,)),
            dma((sum(chunks),)),
            dma((3,)),
            dma((1,)),
            dma((n, local_heads)),
        ],
        compiler_params=pltpu.CompilerParams(
            collective_id=0, has_side_effects=True, vmem_limit_bytes=56 * 1024 * 1024
        ),
    )(
        q_latent, kv_latent, jnp.swapaxes(rope_key, 1, 2), w_query, w_keyval, w_out,
        jnp.asarray(paired_table(length)), query_gain, latent_gain, out_gain,
    )


def x_size(mesh):
    row = mesh.devices[0]
    places = [getattr(device, "coords", None) for device in row]
    if any(place is None for place in places):
        return 1
    return len({place[0] for place in places})


def per_device(
    mesh, q_latent, kv_latent, rope_key, w_query, w_keyval, w_out, query_gain, latent_gain, out_gain
):
    n, m = mesh.shape["sp"], mesh.shape["dp"]
    rows = q_latent.shape[1]
    length = n * rows
    rank = q_latent.shape[2]
    width = w_query.shape[1]
    local_heads = H // n
    k = local_heads * HEAD // width
    chunks = 16
    columns = x_size(mesh)
    groups = k if k == columns == 2 and width % HEAD == 0 else 1
    dim = w_out.shape[1]
    group = local_heads * VDIM
    if groups == columns and width == 2 * HEAD and H % m == 0 and n == 4 and m == n * columns:
        return paired(
            mesh, columns, q_latent, kv_latent, rope_key, w_query, w_keyval, w_out, query_gain,
            latent_gain, out_gain,
        )
    table = jnp.asarray(turn_table(length))
    geometry = (n, m, columns, k, chunks, local_heads, groups)
    any_spec = pl.BlockSpec(memory_space=pl.ANY)
    vmem_spec = pl.BlockSpec(memory_space=pltpu.VMEM)
    dma = pltpu.SemaphoreType.DMA
    return pl.pallas_call(
        functools.partial(kernel, geometry),
        out_shape=pltpu.VMEM((1, rows, dim), BF16),
        in_specs=[any_spec] * 7 + [vmem_spec] * 3,
        out_specs=vmem_spec,
        scratch_shapes=[
            pltpu.VMEM((n, rows, rank), BF16),
            pltpu.VMEM((n, rows, kv_latent.shape[2]), BF16),
            pltpu.VMEM((n, ROPE, rows), BF16),
            pltpu.VMEM((k, rank, width), BF16),
            pltpu.VMEM(w_keyval.shape, BF16),
            pltpu.VMEM(w_out.shape, BF16),
            pltpu.VMEM((length, 128), F32),
            pltpu.VMEM((local_heads // groups, width, 256), BF16),
            pltpu.VMEM((length, rank), BF16),
            pltpu.VMEM((local_heads, length, 256), BF16),
            pltpu.VMEM((local_heads, length, 256), BF16),
            pltpu.VMEM((local_heads, length, VDIM), BF16),
            pltpu.VMEM((n, groups, rows, group // groups), BF16),
            pltpu.VMEM((n, groups, rows, group // groups), BF16),
            pltpu.VMEM((rows, dim), F32),
            pltpu.VMEM((n, 1, group), F32),
            dma((7,)),
            dma((3, n // 2)),
            dma((3, n)),
            dma((3, n // 2)),
            dma((4, k, chunks)),
            dma((k, chunks)),
            dma((n, groups)),
            dma((n, groups)),
        ],
        compiler_params=pltpu.CompilerParams(
            collective_id=0, has_side_effects=True, vmem_limit_bytes=56 * 1024 * 1024
        ),
    )(
        q_latent, kv_latent, jnp.swapaxes(rope_key, 1, 2), w_query, w_keyval, w_out, table,
        query_gain, latent_gain, out_gain,
    )


def solution(mesh):
    in_specs = (
        P("dp", "sp", None),
        P("dp", "sp", None),
        P("dp", "sp", None),
        P(None, "dp"),
        P(None, "sp"),
        P(),
        P(),
        P(),
        P(),
    )
    return jax.shard_map(
        functools.partial(per_device, mesh), mesh=mesh, in_specs=in_specs,
        out_specs=P("dp", "sp", None), check_vma=False,
    )
```

```python
import functools

import jax
import jax.numpy as jnp
import numpy as np
from jax import lax
from jax.experimental import pallas as pl
from jax.experimental.pallas import tpu as pltpu
from jax.sharding import PartitionSpec as P

H = 16
NOPE = 128
ROPE = 64
VDIM = 128
HEAD = NOPE + ROPE
MESH = pl.DeviceIdType.MESH
F32 = jnp.float32
BF16 = jnp.bfloat16


def turn_table(length):
    half = ROPE // 2
    inverse = np.float32(10000.0) ** (-np.arange(half, dtype=np.float32) / np.float32(half))
    angles = np.arange(length, dtype=np.float32)[:, None] * inverse[None, :].astype(np.float32)
    angles = angles.astype(np.float64)
    cosine, sine = np.cos(angles), np.sin(angles)
    return np.concatenate([cosine, cosine, sine, sine], axis=1).astype(np.float32)


def spread_matrix(rows, row_start, head):
    g = lax.broadcasted_iota(jnp.int32, (rows, 256), 0) + row_start
    f = lax.broadcasted_iota(jnp.int32, (rows, 256), 1)
    source = jnp.where(f < HEAD, f, jnp.where(f < HEAD + 32, f - 32, f - 96)) + head * HEAD
    sign = jnp.where((f >= HEAD) & (f < HEAD + 32), -1.0, 1.0)
    return jnp.where(g == source, sign, 0.0).astype(BF16)


def rope_matrix():
    r = lax.broadcasted_iota(jnp.int32, (ROPE, 128), 0)
    f = lax.broadcasted_iota(jnp.int32, (ROPE, 128), 1)
    source = jnp.where(f < 64, f, jnp.where(f < 96, f - 32, f - 96))
    sign = jnp.where((f >= 64) & (f < 96), -1.0, 1.0)
    return jnp.where(r == source, sign, 0.0).astype(BF16)


def scaled_rows(values, gain):
    wide = values.astype(F32)
    mean = jnp.mean(wide * wide, axis=-1, keepdims=True)
    return (wide * lax.rsqrt(mean + 1e-05) * gain).astype(BF16)


def kernel(
    geometry,
    q_ref, kv_ref, rope_ref, wq_ref, wkv_ref, wout_ref, table_ref, qg_ref, lg_ref, og_ref,
    out_ref,
    qall, kvall, ropeall, wqall, wkv, wout, table, spread, qn, qs, ks, vs, att_out, att_in, acc,
    out_gain,
    local_sem, gat_send, gat_recv, fwd_send, w_send, w_recv, att_send, att_recv,
):
    n, m, X, k, chunks, local_heads, groups = geometry
    per_group = local_heads // groups
    width = wqall.shape[2]
    Z = m // X
    rows = q_ref.shape[1]
    n_chips = n // 2
    i = lax.axis_index("sp")
    j = lax.axis_index("dp")
    core = lax.rem(i, 2)
    chip = lax.div(i, 2)
    partner = i + 1 - 2 * core
    z = lax.div(j, X)
    x = lax.rem(j, X)
    first = i * k
    owns = (j >= first) & (j < first + k)

    gathered = ((kv_ref.at[0], kvall), (rope_ref.at[0], ropeall), (q_ref.at[0], qall))
    own_copies = [
        pltpu.make_async_copy(src, dst.at[i], local_sem.at[a]) for a, (src, dst) in enumerate(gathered)
    ]
    wq_copy = pltpu.make_async_copy(wq_ref, wqall.at[lax.rem(j, k)], local_sem.at[3])
    wkv_copy = pltpu.make_async_copy(wkv_ref, wkv, local_sem.at[4])
    table_copy = pltpu.make_async_copy(table_ref, table, local_sem.at[5])
    wout_copy = pltpu.make_async_copy(wout_ref, wout, local_sem.at[6])

    @pl.when(owns)
    def _():
        wq_copy.start()

    for copy in own_copies:
        copy.start()
    wkv_copy.start()
    table_copy.start()
    wout_copy.start()

    turner = rope_matrix()
    latent_gain = lg_ref[...].astype(F32).reshape(1, -1)
    query_gain = qg_ref[...].astype(F32).reshape(1, -1)
    group = local_heads * VDIM
    every_gain = og_ref[...].astype(F32).reshape(1, -1)
    for s in range(n):
        out_gain[s] = every_gain[:, s * group:(s + 1) * group]
    if groups > 1:
        for h in range(per_group):
            spread[h] = spread_matrix(width, 0, h)

    barrier = pltpu.get_barrier_semaphore()
    for d in range(1, n):
        pl.semaphore_signal(
            barrier, inc=1, device_id={"sp": lax.rem(i + d, n)}, device_id_type=MESH
        )
    sides = ((z < Z - 1, j + X), (z > 0, j - X), (x < X - 1, j + 1), (x > 0, j - 1))
    count = n - 1
    for present, target in sides:
        @pl.when(present)
        def _(target=target):
            pl.semaphore_signal(barrier, inc=1, device_id={"dp": target}, device_id_type=MESH)
        count = count + jnp.where(present, 1, 0)
    pl.semaphore_wait(barrier, count)

    step_rows = wqall.shape[1] // chunks

    def relay_parts(slot, c):
        owner = first + slot
        zo, xo = lax.div(owner, X), lax.rem(owner, X)
        part = wqall.at[slot, pl.ds(c * step_rows, step_rows)]
        in_column = x == xo
        conditions = (
            in_column & (z >= zo) & (z < Z - 1),
            in_column & (z <= zo) & (z > 0),
            (x >= xo) & (x < X - 1),
            (x <= xo) & (x > 0),
        )
        copies = [
            pltpu.make_async_remote_copy(
                src_ref=part, dst_ref=part,
                send_sem=w_send.at[side, slot, c], recv_sem=w_recv.at[slot, c],
                device_id={"dp": sides[side][1]}, device_id_type=MESH,
            )
            for side in range(4)
        ]
        return owner, conditions, copies

    def relay(slot, c):
        owner, conditions, copies = relay_parts(slot, c)

        @pl.when(owner != j)
        def _():
            copies[0].wait_recv()

        for condition, copy in zip(conditions, copies):
            @pl.when(condition)
            def _(copy=copy):
                copy.start()

    def relay_finish(slot, c):
        _, conditions, copies = relay_parts(slot, c)
        for condition, copy in zip(conditions, copies):
            @pl.when(condition)
            def _(copy=copy):
                copy.wait_send()

    if groups > 1:
        columns = [lax.rem(x + t, k) for t in range(k)]
        events = [[(column, c) for c in range(chunks)] for column in columns]
    else:
        columns = [0]
        events = [[(slot, c) for c in range(chunks) for slot in range(k)]]
    events_left = list(events[0])

    def relay_some(number):
        for _ in range(min(number, len(events_left))):
            relay(*events_left.pop(0))

    def gather_copy(a, slot, sem, target):
        dst = gathered[a][1]
        return pltpu.make_async_remote_copy(
            src_ref=dst.at[slot], dst_ref=dst.at[slot],
            send_sem=sem, recv_sem=gat_recv.at[a, slot],
            device_id={"sp": target}, device_id_type=MESH,
        )

    sends = []

    @pl.when(owns)
    def _():
        wq_copy.wait()

    for a in range(3):
        own_copies[a].wait()
        for d in range(1, n_chips):
            target = 2 * lax.rem(chip + d, n_chips) + core
            sends.append(gather_copy(a, i, gat_send.at[a, d], target))
            sends[-1].start()
    for a in range(3):
        sends.append(gather_copy(a, i, gat_send.at[a, 0], partner))
        sends[-1].start()

    def far_slot(d):
        return 2 * lax.rem(chip + n_chips - d, n_chips) + core

    def forward(a, d):
        slot = far_slot(d)
        copy = gather_copy(a, slot, fwd_send.at[a, d - 1], partner)
        copy.wait_recv()
        copy.start()
        sends.append(copy)

    def arrive(a, slot):
        gather_copy(a, slot, gat_send.at[a, 0], partner).wait_recv()

    lane = lax.broadcasted_iota(jnp.int32, (rows, 128), 1)

    def keyval(slot):
        at = pl.ds(pl.multiple_of(slot * rows, rows), rows)
        both = jnp.dot(
            scaled_rows(kvall[slot], latent_gain), wkv[...], preferred_element_type=F32
        ).astype(BF16)
        pair = lax.dot_general(
            ropeall[slot], turner, (((0,), (0,)), ((), ())), preferred_element_type=F32
        ) * table[at, :]
        pair = pair + pltpu.roll(pair, 64, 1)
        turned = jnp.where(lane < 64, pair, 0.0).astype(BF16)
        for h in range(local_heads):
            base = h * (NOPE + VDIM)
            ks[h, at, 0:NOPE] = both[:, base:base + NOPE]
            ks[h, at, NOPE:256] = turned
            vs[h, at, :] = both[:, base + NOPE:base + NOPE + VDIM]

    def query_rows(slot):
        at = pl.ds(pl.multiple_of(slot * rows, rows), rows)
        qn[at, :] = scaled_rows(qall[slot], query_gain)

    relay_some(k + 1)
    wkv_copy.wait()
    table_copy.wait()
    keyval(i)
    relay_some(1)
    query_rows(i)
    relay_some(1)
    arrive(0, partner)
    arrive(1, partner)
    keyval(partner)
    relay_some(1)
    for d in range(1, n_chips):
        forward(0, d)
        forward(1, d)
        keyval(far_slot(d))
        relay_some(1)
    arrive(2, partner)
    query_rows(partner)
    relay_some(2)
    for d in range(1, n_chips):
        other = far_slot(d) + 1 - 2 * core
        arrive(0, other)
        arrive(1, other)
        keyval(other)
        relay_some(2)
    for d in range(1, n_chips):
        forward(2, d)
        query_rows(far_slot(d))
        relay_some(2)
    for d in range(1, n_chips):
        other = far_slot(d) + 1 - 2 * core
        arrive(2, other)
        query_rows(other)
    relay_some(len(events_left))

    def raw_queries(slot, hh):
        if groups > 1:
            total = jnp.dot(wqall[slot], spread[hh], preferred_element_type=F32)
        else:
            total = None
            for s in range(k):
                if (s + 1) * width <= hh * HEAD or s * width >= (hh + 1) * HEAD:
                    continue
                term = jnp.dot(
                    wqall[s], spread_matrix(width, s * width, hh), preferred_element_type=F32
                )
                total = term if total is None else total + term
        return jnp.dot(qn[...], total.astype(BF16), preferred_element_type=F32)

    def queries(slot):
        for hh in range(per_group):
            h = slot * per_group + hh
            raw = raw_queries(slot, hh)
            qs[h, :, 0:NOPE] = raw[:, 0:NOPE].astype(BF16)
            pair = raw[:, NOPE:256] * table[...]
            qs[h, :, NOPE:256] = (pair + pltpu.roll(pair, 64, 1)).astype(BF16)

    power = HEAD ** (-0.5) * float(np.log2(np.e))
    causal = lax.broadcasted_iota(jnp.int32, (rows, rows), 1) <= lax.broadcasted_iota(
        jnp.int32, (rows, rows), 0
    )

    def attend(b, slot):
        stop = (b + 1) * rows
        for hh in range(per_group):
            h = slot * per_group + hh
            scores = lax.dot_general(
                qs[h, b * rows:stop, :], ks[h, 0:stop, :], (((1,), (1,)), ((), ())),
                preferred_element_type=F32,
            )
            last = jnp.where(causal, scores[:, b * rows:], -jnp.inf)
            if b:
                scores = jnp.concatenate([scores[:, :b * rows], last], axis=1)
            else:
                scores = last
            top = jnp.max(scores, axis=-1, keepdims=True)
            weights = jnp.exp2((scores - top) * power)
            row_total = jnp.sum(weights, axis=-1, keepdims=True)
            summed = jnp.dot(weights.astype(BF16), vs[h, 0:stop, :], preferred_element_type=F32)
            att_out[b, slot, :, hh * VDIM:(hh + 1) * VDIM] = (summed / row_total).astype(BF16)

    def att_copy(b, slot):
        return pltpu.make_async_remote_copy(
            src_ref=att_out.at[b, slot], dst_ref=att_in.at[i, slot],
            send_sem=att_send.at[b, slot], recv_sem=att_recv.at[i, slot],
            device_id={"sp": b}, device_id_type=MESH,
        )

    for t, slot in enumerate(columns):
        if t:
            for event in events[t]:
                relay(*event)
        queries(slot)
        for c in range(n_chips):
            @pl.when(chip != c)
            def _(c=c):
                for b in (2 * c, 2 * c + 1):
                    attend(b, slot)
                    att_copy(b, slot).start()
    for c in range(n_chips):
        @pl.when(chip == c)
        def _(c=c):
            for slot in columns:
                for b in (2 * c, 2 * c + 1):
                    attend(b, slot)
    for slot in columns:
        att_copy(partner, slot).start()

    wout_copy.wait()
    squares = None
    order = [partner]
    for d in range(1, n_chips):
        order += [far_slot(d), far_slot(d) + 1 - 2 * core]
    for t, s in enumerate([i] + order):
        source = att_out
        if t:
            source = att_in
            for slot in range(groups):
                pltpu.make_async_remote_copy(
                    src_ref=att_in.at[s, slot], dst_ref=att_in.at[s, slot],
                    send_sem=att_send.at[0, slot], recv_sem=att_recv.at[s, slot],
                    device_id={"sp": partner}, device_id_type=MESH,
                ).wait_recv()
        values = jnp.concatenate([source[s, slot] for slot in range(groups)], axis=1).astype(F32)
        at = pl.ds(pl.multiple_of(s * group, group), group)
        square = jnp.sum(values * values, axis=-1, keepdims=True)
        squares = square if squares is None else squares + square
        scaled = (values * out_gain[s]).astype(BF16)
        term = jnp.dot(scaled, wout[at, :], preferred_element_type=F32)
        if t == 0:
            acc[...] = term
        elif t < n - 1:
            acc[...] += term
        else:
            factor = lax.rsqrt(squares / (n * group) + 1e-05)
            out_ref[0] = ((acc[...] + term) * factor).astype(BF16)

    for copy in sends:
        copy.wait_send()
    for event in sum(events, []):
        relay_finish(*event)
    for b in range(n):
        @pl.when(i != b)
        def _(b=b):
            for slot in range(groups):
                att_copy(b, slot).wait_send()


def paired_table(length):
    half = ROPE // 2
    inverse = np.float32(10000.0) ** (-np.arange(half, dtype=np.float32) / np.float32(half))
    angles = np.arange(length, dtype=np.float32)[:, None] * inverse[None, :].astype(np.float32)
    angles = angles.astype(np.float64)
    cosine, sine = np.cos(angles), np.sin(angles)
    parts = [cosine] * 4 + [-sine, sine, -sine, sine]
    return np.concatenate(parts, axis=1).astype(np.float32)


def paired_kernel(
    geometry,
    q_ref, kv_ref, rope_ref, wq_ref, wkv_ref, wout_ref, table_ref, qg_ref, lg_ref, og_ref,
    out_ref,
    qall, kvall, ropeall, wqa, wqb, assist, wkv, wout, table, qgain, lgain, ogain, head_gain, qn, qs, ks, vs,
    att_out, att_in, acc,
    local_sem, gat_send, gat_recv, w_send, w_recv, x_recv, att_send, att_recv,
):
    n, X, Z, chunks, local_heads = geometry
    whead = (wqa, wqb)
    first_width = wqa.shape[2]
    rows = q_ref.shape[1]
    n_chips = n // 2
    i = lax.axis_index("sp")
    j = lax.axis_index("dp")
    core = lax.rem(i, 2)
    chip = lax.div(i, 2)
    partner = i + 1 - 2 * core
    z = lax.div(j, X)
    x = lax.rem(j, X)
    across = 1 - x
    zo = i
    owns = z == zo

    gathered = ((kv_ref.at[0], kvall), (rope_ref.at[0], ropeall), (q_ref.at[0], qall))
    own_copies = [
        pltpu.make_async_copy(src, dst.at[i], local_sem.at[a]) for a, (src, dst) in enumerate(gathered)
    ]
    wq_copies = [
        pltpu.make_async_copy(wq_ref.at[:, 0:first_width], wqa.at[x], local_sem.at[3]),
        pltpu.make_async_copy(
            wq_ref.at[:, first_width:first_width + wqb.shape[2]], wqb.at[x], local_sem.at[10]
        ),
    ]
    wkv_copy = pltpu.make_async_copy(wkv_ref, wkv, local_sem.at[4])
    table_copy = pltpu.make_async_copy(table_ref, table, local_sem.at[5])
    wout_copy = pltpu.make_async_copy(wout_ref, wout, local_sem.at[6])
    gain_copies = [
        pltpu.make_async_copy(src, dst, local_sem.at[7 + a])
        for a, (src, dst) in enumerate(((qg_ref, qgain), (lg_ref, lgain), (og_ref, ogain)))
    ]

    @pl.when(z == i)
    def _():
        for copy in wq_copies:
            copy.start()

    for copy in own_copies:
        copy.start()
    for copy in gain_copies:
        copy.start()

    assist_copy = pltpu.make_async_copy(
        wq_ref.at[:, first_width:first_width + wqb.shape[2]], assist, local_sem.at[11]
    )

    barrier = pltpu.get_barrier_semaphore()
    for d in range(1, n):
        pl.semaphore_signal(
            barrier, inc=1, device_id={"sp": lax.rem(i + d, n)}, device_id_type=MESH
        )
    def places(owner):
        low = owner * 2 < Z
        inner = owner == jnp.where(low, 1, Z - 2)
        last = jnp.where(low, Z - 1, 0)
        relayer = jnp.where(low, Z - 2, 1)
        return last, relayer, jnp.where(low, jnp.where(inner, 0, 1), jnp.where(inner, Z - 1, Z - 2))

    end, mid, other = places(zo)
    at_mid, at_end, at_other = z == mid, z == end, z == other
    twin = lax.rem(i + n // 2, n)
    twin_end = places(twin)[0]
    assists = z == twin

    def row(target, column=x):
        return target * X + column

    greet = (
        (at_other | at_mid, {"dp": row(zo)}), (at_end, {"dp": row(mid)}),
        (at_end, {"sp": twin, "dp": row(zo)}), (at_end, {"sp": twin, "dp": row(zo, across)}),
    )
    pl.semaphore_signal(barrier, inc=1, device_id={"dp": row(z, across)}, device_id_type=MESH)
    count = n + jnp.where(owns, 2, 0) + jnp.where(at_mid, 1, 0) + jnp.where(assists, 2, 0)
    for present, target in greet:
        @pl.when(present)
        def _(target=target):
            pl.semaphore_signal(barrier, inc=1, device_id=target, device_id_type=MESH)

    @pl.when(assists)
    def _():
        assist_copy.start()

    wkv_copy.start()
    table_copy.start()

    for h in range(local_heads):
        vs[h, :, VDIM:2 * VDIM] = jnp.ones((vs.shape[1], VDIM), BF16)
    r = lax.broadcasted_iota(jnp.int32, (ROPE, 128), 0)
    f = lax.broadcasted_iota(jnp.int32, (ROPE, 128), 1)
    turner = jnp.where(r == lax.rem(f, ROPE), 1.0, 0.0).astype(BF16)

    parts = [(part, c) for part in range(2) for c in range(chunks[part])]

    def w_part(index):
        part, c = parts[index]
        step = whead[part].shape[1] // chunks[part]
        return whead[part].at[x, pl.ds(c * step, step)]

    targets = (row(other), row(mid), row(end))

    def assist_send(column, sem):
        return pltpu.make_async_remote_copy(
            src_ref=assist, dst_ref=wqb.at[x], send_sem=w_send.at[4],
            recv_sem=x_recv.at[1 + sem],
            device_id={"sp": twin, "dp": row(twin_end, column)}, device_id_type=MESH,
        )

    def w_copy(side, c):
        part = w_part(c)
        return pltpu.make_async_remote_copy(
            src_ref=part, dst_ref=part, send_sem=w_send.at[parts[c][0]], recv_sem=w_recv.at[c],
            device_id={"dp": targets[side]}, device_id_type=MESH,
        )

    def x_copy(source, part):
        return pltpu.make_async_remote_copy(
            src_ref=source, dst_ref=source, send_sem=w_send.at[2 + part], recv_sem=x_recv.at[part],
            device_id={"dp": j + 1 - 2 * x}, device_id_type=MESH,
        )

    inner_owner = (zo != 0) & (zo != Z - 1)
    roles = (at_mid | (at_other & jnp.logical_not(inner_owner)), at_other & inner_owner, at_end)
    chunks_left = [list(range(len(parts))) for _ in roles]
    chunks_left[2] = chunks_left[2][:chunks[0]]

    def relay_one(index):
        w_copy(0, index).wait_recv()
        if parts[index][0] == 0:
            @pl.when(at_mid)
            def _():
                w_copy(2, index).start()
        x_copy(w_part(index), parts[index][0]).start()

    def relay(*numbers):
        for role, number, left in zip(roles, numbers, chunks_left):
            todo = [left.pop(0) for _ in range(min(number, len(left)))]
            if todo:
                @pl.when(role)
                def _(todo=todo):
                    for index in todo:
                        relay_one(index)

    def peer(slot, reader):
        return lax.rem(slot - reader + n, n) - 1

    def gather_copy(a, slot, target, reader=None):
        dst = gathered[a][1]
        return pltpu.make_async_remote_copy(
            src_ref=dst.at[slot], dst_ref=dst.at[slot], send_sem=gat_send.at[a],
            recv_sem=gat_recv.at[a, peer(slot, target if reader is None else reader)],
            device_id={"sp": target}, device_id_type=MESH,
        )

    def far_slot(d):
        return 2 * lax.rem(chip + n_chips - d, n_chips) + core

    def arrive(a, slot):
        gather_copy(a, slot, partner, i).wait_recv()

    def forward(a, d):
        arrive(a, far_slot(d))
        gather_copy(a, far_slot(d), partner).start()

    lane = lax.broadcasted_iota(jnp.int32, (rows, 128), 1)
    left = lane < 64

    def turned_pair(both_halves, at):
        swap_low = lax.rem(lax.broadcasted_iota(jnp.int32, both_halves.shape, 1), 64) < 32
        swapped = jnp.where(
            swap_low, pltpu.roll(both_halves, 96, 1), pltpu.roll(both_halves, 32, 1)
        )
        return both_halves * table[at, 0:128] + swapped * table[at, 128:256]

    def keyval(slot):
        at = pl.ds(pl.multiple_of(slot * rows, rows), rows)
        both = jnp.dot(
            scaled_rows(kvall[slot], lgain[...].astype(F32).reshape(1, -1)), wkv[...],
            preferred_element_type=F32,
        )
        twice = lax.dot_general(
            ropeall[slot], turner, (((0,), (0,)), ((), ())), preferred_element_type=F32
        )
        turned = turned_pair(twice, at)
        for h in range(local_heads):
            base = h * (NOPE + VDIM)
            key = both[:, base:base + NOPE]
            if h % 2 == 0:
                ks[h, at, 0:NOPE] = key.astype(BF16)
                ks[h, at, NOPE:256] = jnp.where(left, turned, 0.0).astype(BF16)
            else:
                key = pltpu.roll(key, 64, 1)
                ks[h, at, 0:NOPE] = jnp.where(left, 0.0, key).astype(BF16)
                ks[h, at, NOPE:256] = jnp.where(left, key, turned).astype(BF16)
            vs[h, at, 0:VDIM] = both[:, base + NOPE:base + NOPE + VDIM].astype(BF16)

    def query_rows(slot):
        at = pl.ds(pl.multiple_of(slot * rows, rows), rows)
        qn[at, :] = scaled_rows(qall[slot], qgain[...].astype(F32).reshape(1, -1))

    @pl.when(owns)
    def _():
        for copy in wq_copies:
            copy.wait()

    for copy in own_copies:
        copy.wait()

    pl.semaphore_wait(barrier, count)

    for a in range(3):
        for d in range(1, n_chips):
            gather_copy(a, i, 2 * lax.rem(chip + d, n_chips) + core).start()

    @pl.when(owns)
    def _():
        for part in range(2):
            x_copy(whead[part].at[x], part).start()
        for index in range(len(parts)):
            w_copy(1, index).start()
            w_copy(0, index).start()

    for a in range(3):
        gather_copy(a, i, partner).start()

    wout_copy.start()
    for copy in gain_copies:
        copy.wait()
    query_rows(i)
    every_gain = ogain[...].astype(F32).reshape(1, -1)
    for h in range(n * local_heads):
        head_gain[h] = every_gain[:, h * VDIM:(h + 1) * VDIM]

    wkv_copy.wait()
    table_copy.wait()
    keyval(i)
    arrive(0, partner)
    arrive(1, partner)
    keyval(partner)
    arrive(2, partner)
    query_rows(partner)
    relay(8, 12, 0)
    for d in range(1, n_chips):
        forward(0, d)
        forward(1, d)
        relay(1, 2, 0)
        keyval(far_slot(d))

    @pl.when(assists)
    def _():
        assist_copy.wait()
        assist_send(x, 1).start()

    relay(2, 2, 2)
    for d in range(1, n_chips):
        other = far_slot(d) + 1 - 2 * core
        arrive(0, other)
        arrive(1, other)
        keyval(other)

    @pl.when(assists)
    def _():
        assist_send(across, 0).start()

    relay(5, 1, 4)
    for d in range(1, n_chips):
        forward(2, d)
        query_rows(far_slot(d))
    relay(0, 1, 4)
    for d in range(1, n_chips):
        other = far_slot(d) + 1 - 2 * core
        arrive(2, other)
        query_rows(other)
    relay(1, 2, chunks[0])

    wide_left = lax.broadcasted_iota(jnp.int32, (2 * rows, 128), 1) < 64

    def queries(slot, part, c):
        at = pl.ds(c * 2 * rows, 2 * rows)
        raw = jnp.dot(qn[at, :], whead[part][slot], preferred_element_type=F32)
        last = raw[:, raw.shape[1] - 128:]
        turned = turned_pair(last, at)
        if part == 0:
            qs[slot, at, 0:128] = raw[:, 0:128].astype(BF16)
            qs[slot, at, 128:256] = jnp.where(wide_left, turned, last).astype(BF16)
        else:
            qs[slot, at, 256:384] = jnp.where(wide_left, last, turned).astype(BF16)

    power = HEAD ** (-0.5) * float(np.log2(np.e))
    block = 2 * rows
    causal = lax.broadcasted_iota(jnp.int32, (block, block), 1) <= lax.broadcasted_iota(
        jnp.int32, (block, block), 0
    )

    def attend(c, slot, heads):
        start, stop = c * block, (c + 1) * block
        scores = []
        for hh in heads:
            score = lax.dot_general(
                qs[slot, start:stop, hh * 128:hh * 128 + 256], ks[2 * slot + hh, 0:stop, :],
                (((1,), (1,)), ((), ())), preferred_element_type=F32,
            )
            last = jnp.where(causal, score[:, start:], -jnp.inf)
            scores.append(jnp.concatenate([score[:, :start], last], axis=1) if c else last)
        tops = [jnp.max(score, axis=-1, keepdims=True) for score in scores]
        weights = [
            jnp.exp2((score - top) * power).astype(BF16) for score, top in zip(scores, tops)
        ]
        for hh, weight in zip(heads, weights):
            summed = jnp.dot(weight, vs[2 * slot + hh, 0:stop, :], preferred_element_type=F32)
            result = (summed[:, 0:VDIM] / summed[:, VDIM:2 * VDIM]).astype(BF16)
            for e in range(2):
                att_out[2 * c + e, 2 * slot + hh] = result[e * rows:(e + 1) * rows]

    def att_copy(b, head):
        return pltpu.make_async_remote_copy(
            src_ref=att_out.at[b, head], dst_ref=att_in.at[i, head],
            send_sem=att_send.at[0], recv_sem=att_recv.at[peer(i, b), head],
            device_id={"sp": b}, device_id_type=MESH,
        )

    def far_head(slot, hh):
        for c in range(n_chips):
            @pl.when(chip != c)
            def _(c=c):
                queries(slot, hh, c)
                attend(c, slot, (hh,))
                for b in (2 * c, 2 * c + 1):
                    att_copy(b, 2 * slot + hh).start()

    def own_heads(slot):
        for c in range(n_chips):
            @pl.when(chip == c)
            def _(c=c):
                for hh in range(2):
                    queries(slot, hh, c)
                attend(c, slot, (0, 1))
        for hh in range(2):
            att_copy(partner, 2 * slot + hh).start()

    far_head(x, 0)
    relay(len(parts), len(parts), 0)

    @pl.when(at_end)
    def _():
        assist_send(x, 1).wait_recv()

    far_head(x, 1)
    own_heads(x)
    for part in range(2):
        x_copy(whead[part].at[across], part).wait_recv()
        far_head(across, part)
    own_heads(across)

    wout_copy.wait()
    squares = []
    group = local_heads * VDIM

    def product(pieces):
        sides = []
        for s, first, number in pieces:
            values = []
            for hh in range(number):
                if s is not i:
                    pltpu.make_async_remote_copy(
                        src_ref=att_in.at[s, first + hh], dst_ref=att_in.at[s, first + hh],
                        send_sem=att_send.at[0], recv_sem=att_recv.at[peer(s, i), first + hh],
                        device_id={"sp": partner}, device_id_type=MESH,
                    ).wait_recv()
                value = (att_out if s is i else att_in)[s, first + hh].astype(F32)
                squares.append(value * value)
                values.append((value * head_gain[s * local_heads + first + hh]).astype(BF16))
            at = pl.multiple_of(s * group + first * VDIM, VDIM)
            sides.append((values, wout[pl.ds(at, number * VDIM), :]))
        return jnp.dot(
            jnp.concatenate(sum((values for values, _ in sides), []), axis=1),
            jnp.concatenate([rows_of for _, rows_of in sides], axis=0),
            preferred_element_type=F32,
        )

    far = []
    for d in range(1, n_chips):
        far += [far_slot(d), far_slot(d) + 1 - 2 * core]
    acc[...] = product([(i, 0, local_heads), (partner, 0, local_heads)])
    acc[...] += product([(s, 2 * x, 2) for s in far])
    acc[...] += product([(s, 2 * across, 1) for s in far])
    term = product([(s, 2 * across + 1, 1) for s in far])
    squared = jnp.sum(sum(squares[1:], squares[0]), axis=-1, keepdims=True)
    factor = lax.rsqrt(squared / (n * group) + 1e-05)
    out_ref[0] = ((acc[...] + term) * factor).astype(BF16)

    for a in range(3):
        every = gathered[a][1].at[pl.ds(0, n - 1)]
        pltpu.make_async_remote_copy(
            src_ref=every, dst_ref=every, send_sem=gat_send.at[a], recv_sem=gat_recv.at[a, 0],
            device_id={"sp": partner}, device_id_type=MESH,
        ).wait_send()
    def all_sent(every, sem):
        pltpu.make_async_remote_copy(
            src_ref=every, dst_ref=every, send_sem=w_send.at[sem], recv_sem=w_recv.at[0],
            device_id={"dp": targets[0]}, device_id_type=MESH,
        ).wait_send()

    @pl.when(owns)
    def _():
        all_sent(wqa, 0)
        all_sent(wqb, 1)

    @pl.when(at_mid)
    def _():
        all_sent(wqa.at[x], 0)

    @pl.when(assists)
    def _():
        all_sent(wqb, 4)

    x_copy(wqa.at[x], 0).wait_send()

    @pl.when(jnp.logical_not(at_end))
    def _():
        x_copy(wqb.at[x], 1).wait_send()

    every = att_out.at[pl.ds(0, n - 1)]
    pltpu.make_async_remote_copy(
        src_ref=every, dst_ref=every, send_sem=att_send.at[0], recv_sem=att_recv.at[0, 0],
        device_id={"sp": partner}, device_id_type=MESH,
    ).wait_send()


def paired(
    mesh, columns, q_latent, kv_latent, rope_key, w_query, w_keyval, w_out, query_gain, latent_gain,
    out_gain,
):
    n, m = mesh.shape["sp"], mesh.shape["dp"]
    rows = q_latent.shape[1]
    length = n * rows
    rank = q_latent.shape[2]
    width = w_query.shape[1]
    local_heads = H // n
    chunks = (16, 4)
    dim = w_out.shape[1]
    geometry = (n, columns, m // columns, chunks, local_heads)
    any_spec = pl.BlockSpec(memory_space=pl.ANY)
    vmem_spec = pl.BlockSpec(memory_space=pltpu.VMEM)
    dma = pltpu.SemaphoreType.DMA
    return pl.pallas_call(
        functools.partial(paired_kernel, geometry),
        out_shape=pltpu.VMEM((1, rows, dim), BF16),
        in_specs=[any_spec] * 10,
        out_specs=vmem_spec,
        scratch_shapes=[
            pltpu.VMEM((n, rows, rank), BF16),
            pltpu.VMEM((n, rows, kv_latent.shape[2]), BF16),
            pltpu.VMEM((n, ROPE, rows), BF16),
            pltpu.VMEM((columns, rank, 2 * NOPE), BF16),
            pltpu.VMEM((columns, rank, width - 2 * NOPE), BF16),
            pltpu.VMEM((rank, width - 2 * NOPE), BF16),
            pltpu.VMEM(w_keyval.shape, BF16),
            pltpu.VMEM(w_out.shape, BF16),
            pltpu.VMEM((length, 256), F32),
            pltpu.VMEM(query_gain.shape, BF16),
            pltpu.VMEM(latent_gain.shape, BF16),
            pltpu.VMEM(out_gain.shape, BF16),
            pltpu.VMEM((n * local_heads, 1, VDIM), F32),
            pltpu.VMEM((length, rank), BF16),
            pltpu.VMEM((columns, length, width), BF16),
            pltpu.VMEM((local_heads, length, 256), BF16),
            pltpu.VMEM((local_heads, length, 2 * VDIM), BF16),
            pltpu.VMEM((n, local_heads, rows, VDIM), BF16),
            pltpu.VMEM((n, local_heads, rows, VDIM), BF16),
            pltpu.VMEM((rows, dim), F32),
            dma((12,)),
            dma((3,)),
            dma((3, n - 1)),
            dma((5,)),
            dma((sum(chunks),)),
            dma((3,)),
            dma((1,)),
            dma((n - 1, local_heads)),
        ],
        compiler_params=pltpu.CompilerParams(
            collective_id=0, has_side_effects=True, vmem_limit_bytes=56 * 1024 * 1024
        ),
    )(
        q_latent, kv_latent, jnp.swapaxes(rope_key, 1, 2), w_query, w_keyval, w_out,
        jnp.asarray(paired_table(length)), query_gain, latent_gain, out_gain,
    )


def x_size(mesh):
    row = mesh.devices[0]
    places = [getattr(device, "coords", None) for device in row]
    if any(place is None for place in places):
        return 1
    return len({place[0] for place in places})


def per_device(
    mesh, q_latent, kv_latent, rope_key, w_query, w_keyval, w_out, query_gain, latent_gain, out_gain
):
    n, m = mesh.shape["sp"], mesh.shape["dp"]
    rows = q_latent.shape[1]
    length = n * rows
    rank = q_latent.shape[2]
    width = w_query.shape[1]
    local_heads = H // n
    k = local_heads * HEAD // width
    chunks = 16
    columns = x_size(mesh)
    groups = k if k == columns == 2 and width % HEAD == 0 else 1
    dim = w_out.shape[1]
    group = local_heads * VDIM
    if groups == columns and width == 2 * HEAD and H % m == 0 and n == 4 and m == n * columns:
        return paired(
            mesh, columns, q_latent, kv_latent, rope_key, w_query, w_keyval, w_out, query_gain,
            latent_gain, out_gain,
        )
    table = jnp.asarray(turn_table(length))
    geometry = (n, m, columns, k, chunks, local_heads, groups)
    any_spec = pl.BlockSpec(memory_space=pl.ANY)
    vmem_spec = pl.BlockSpec(memory_space=pltpu.VMEM)
    dma = pltpu.SemaphoreType.DMA
    return pl.pallas_call(
        functools.partial(kernel, geometry),
        out_shape=pltpu.VMEM((1, rows, dim), BF16),
        in_specs=[any_spec] * 7 + [vmem_spec] * 3,
        out_specs=vmem_spec,
        scratch_shapes=[
            pltpu.VMEM((n, rows, rank), BF16),
            pltpu.VMEM((n, rows, kv_latent.shape[2]), BF16),
            pltpu.VMEM((n, ROPE, rows), BF16),
            pltpu.VMEM((k, rank, width), BF16),
            pltpu.VMEM(w_keyval.shape, BF16),
            pltpu.VMEM(w_out.shape, BF16),
            pltpu.VMEM((length, 128), F32),
            pltpu.VMEM((local_heads // groups, width, 256), BF16),
            pltpu.VMEM((length, rank), BF16),
            pltpu.VMEM((local_heads, length, 256), BF16),
            pltpu.VMEM((local_heads, length, 256), BF16),
            pltpu.VMEM((local_heads, length, VDIM), BF16),
            pltpu.VMEM((n, groups, rows, group // groups), BF16),
            pltpu.VMEM((n, groups, rows, group // groups), BF16),
            pltpu.VMEM((rows, dim), F32),
            pltpu.VMEM((n, 1, group), F32),
            dma((7,)),
            dma((3, n // 2)),
            dma((3, n)),
            dma((3, n // 2)),
            dma((4, k, chunks)),
            dma((k, chunks)),
            dma((n, groups)),
            dma((n, groups)),
        ],
        compiler_params=pltpu.CompilerParams(
            collective_id=0, has_side_effects=True, vmem_limit_bytes=56 * 1024 * 1024
        ),
    )(
        q_latent, kv_latent, jnp.swapaxes(rope_key, 1, 2), w_query, w_keyval, w_out, table,
        query_gain, latent_gain, out_gain,
    )


def solution(mesh):
    in_specs = (
        P("dp", "sp", None),
        P("dp", "sp", None),
        P("dp", "sp", None),
        P(None, "dp"),
        P(None, "sp"),
        P(),
        P(),
        P(),
        P(),
    )
    return jax.shard_map(
        functools.partial(per_device, mesh), mesh=mesh, in_specs=in_specs,
        out_specs=P("dp", "sp", None), check_vma=False,
    )
```

```python
import functools

import jax
import jax.numpy as jnp
import numpy as np
from jax import lax
from jax.experimental import pallas as pl
from jax.experimental.pallas import tpu as pltpu
from jax.sharding import PartitionSpec as P

H = 16
NOPE = 128
ROPE = 64
VDIM = 128
HEAD = NOPE + ROPE
MESH = pl.DeviceIdType.MESH
F32 = jnp.float32
BF16 = jnp.bfloat16


def turn_table(length):
    half = ROPE // 2
    inverse = np.float32(10000.0) ** (-np.arange(half, dtype=np.float32) / np.float32(half))
    angles = np.arange(length, dtype=np.float32)[:, None] * inverse[None, :].astype(np.float32)
    angles = angles.astype(np.float64)
    cosine, sine = np.cos(angles), np.sin(angles)
    return np.concatenate([cosine, cosine, sine, sine], axis=1).astype(np.float32)


def spread_matrix(rows, row_start, head):
    g = lax.broadcasted_iota(jnp.int32, (rows, 256), 0) + row_start
    f = lax.broadcasted_iota(jnp.int32, (rows, 256), 1)
    source = jnp.where(f < HEAD, f, jnp.where(f < HEAD + 32, f - 32, f - 96)) + head * HEAD
    sign = jnp.where((f >= HEAD) & (f < HEAD + 32), -1.0, 1.0)
    return jnp.where(g == source, sign, 0.0).astype(BF16)


def rope_matrix():
    r = lax.broadcasted_iota(jnp.int32, (ROPE, 128), 0)
    f = lax.broadcasted_iota(jnp.int32, (ROPE, 128), 1)
    source = jnp.where(f < 64, f, jnp.where(f < 96, f - 32, f - 96))
    sign = jnp.where((f >= 64) & (f < 96), -1.0, 1.0)
    return jnp.where(r == source, sign, 0.0).astype(BF16)


def scaled_rows(values, gain):
    wide = values.astype(F32)
    mean = jnp.mean(wide * wide, axis=-1, keepdims=True)
    return (wide * lax.rsqrt(mean + 1e-05) * gain).astype(BF16)


def kernel(
    geometry,
    q_ref, kv_ref, rope_ref, wq_ref, wkv_ref, wout_ref, table_ref, qg_ref, lg_ref, og_ref,
    out_ref,
    qall, kvall, ropeall, wqall, wkv, wout, table, spread, qn, qs, ks, vs, att_out, att_in, acc,
    out_gain,
    local_sem, gat_send, gat_recv, fwd_send, w_send, w_recv, att_send, att_recv,
):
    n, m, X, k, chunks, local_heads, groups = geometry
    per_group = local_heads // groups
    width = wqall.shape[2]
    Z = m // X
    rows = q_ref.shape[1]
    n_chips = n // 2
    i = lax.axis_index("sp")
    j = lax.axis_index("dp")
    core = lax.rem(i, 2)
    chip = lax.div(i, 2)
    partner = i + 1 - 2 * core
    z = lax.div(j, X)
    x = lax.rem(j, X)
    first = i * k
    owns = (j >= first) & (j < first + k)

    gathered = ((kv_ref.at[0], kvall), (rope_ref.at[0], ropeall), (q_ref.at[0], qall))
    own_copies = [
        pltpu.make_async_copy(src, dst.at[i], local_sem.at[a]) for a, (src, dst) in enumerate(gathered)
    ]
    wq_copy = pltpu.make_async_copy(wq_ref, wqall.at[lax.rem(j, k)], local_sem.at[3])
    wkv_copy = pltpu.make_async_copy(wkv_ref, wkv, local_sem.at[4])
    table_copy = pltpu.make_async_copy(table_ref, table, local_sem.at[5])
    wout_copy = pltpu.make_async_copy(wout_ref, wout, local_sem.at[6])

    @pl.when(owns)
    def _():
        wq_copy.start()

    for copy in own_copies:
        copy.start()
    wkv_copy.start()
    table_copy.start()
    wout_copy.start()

    turner = rope_matrix()
    latent_gain = lg_ref[...].astype(F32).reshape(1, -1)
    query_gain = qg_ref[...].astype(F32).reshape(1, -1)
    group = local_heads * VDIM
    every_gain = og_ref[...].astype(F32).reshape(1, -1)
    for s in range(n):
        out_gain[s] = every_gain[:, s * group:(s + 1) * group]
    if groups > 1:
        for h in range(per_group):
            spread[h] = spread_matrix(width, 0, h)

    barrier = pltpu.get_barrier_semaphore()
    for d in range(1, n):
        pl.semaphore_signal(
            barrier, inc=1, device_id={"sp": lax.rem(i + d, n)}, device_id_type=MESH
        )
    sides = ((z < Z - 1, j + X), (z > 0, j - X), (x < X - 1, j + 1), (x > 0, j - 1))
    count = n - 1
    for present, target in sides:
        @pl.when(present)
        def _(target=target):
            pl.semaphore_signal(barrier, inc=1, device_id={"dp": target}, device_id_type=MESH)
        count = count + jnp.where(present, 1, 0)
    pl.semaphore_wait(barrier, count)

    step_rows = wqall.shape[1] // chunks

    def relay_parts(slot, c):
        owner = first + slot
        zo, xo = lax.div(owner, X), lax.rem(owner, X)
        part = wqall.at[slot, pl.ds(c * step_rows, step_rows)]
        in_column = x == xo
        conditions = (
            in_column & (z >= zo) & (z < Z - 1),
            in_column & (z <= zo) & (z > 0),
            (x >= xo) & (x < X - 1),
            (x <= xo) & (x > 0),
        )
        copies = [
            pltpu.make_async_remote_copy(
                src_ref=part, dst_ref=part,
                send_sem=w_send.at[side, slot, c], recv_sem=w_recv.at[slot, c],
                device_id={"dp": sides[side][1]}, device_id_type=MESH,
            )
            for side in range(4)
        ]
        return owner, conditions, copies

    def relay(slot, c):
        owner, conditions, copies = relay_parts(slot, c)

        @pl.when(owner != j)
        def _():
            copies[0].wait_recv()

        for condition, copy in zip(conditions, copies):
            @pl.when(condition)
            def _(copy=copy):
                copy.start()

    def relay_finish(slot, c):
        _, conditions, copies = relay_parts(slot, c)
        for condition, copy in zip(conditions, copies):
            @pl.when(condition)
            def _(copy=copy):
                copy.wait_send()

    if groups > 1:
        columns = [lax.rem(x + t, k) for t in range(k)]
        events = [[(column, c) for c in range(chunks)] for column in columns]
    else:
        columns = [0]
        events = [[(slot, c) for c in range(chunks) for slot in range(k)]]
    events_left = list(events[0])

    def relay_some(number):
        for _ in range(min(number, len(events_left))):
            relay(*events_left.pop(0))

    def gather_copy(a, slot, sem, target):
        dst = gathered[a][1]
        return pltpu.make_async_remote_copy(
            src_ref=dst.at[slot], dst_ref=dst.at[slot],
            send_sem=sem, recv_sem=gat_recv.at[a, slot],
            device_id={"sp": target}, device_id_type=MESH,
        )

    sends = []

    @pl.when(owns)
    def _():
        wq_copy.wait()

    for a in range(3):
        own_copies[a].wait()
        for d in range(1, n_chips):
            target = 2 * lax.rem(chip + d, n_chips) + core
            sends.append(gather_copy(a, i, gat_send.at[a, d], target))
            sends[-1].start()
    for a in range(3):
        sends.append(gather_copy(a, i, gat_send.at[a, 0], partner))
        sends[-1].start()

    def far_slot(d):
        return 2 * lax.rem(chip + n_chips - d, n_chips) + core

    def forward(a, d):
        slot = far_slot(d)
        copy = gather_copy(a, slot, fwd_send.at[a, d - 1], partner)
        copy.wait_recv()
        copy.start()
        sends.append(copy)

    def arrive(a, slot):
        gather_copy(a, slot, gat_send.at[a, 0], partner).wait_recv()

    lane = lax.broadcasted_iota(jnp.int32, (rows, 128), 1)

    def keyval(slot):
        at = pl.ds(pl.multiple_of(slot * rows, rows), rows)
        both = jnp.dot(
            scaled_rows(kvall[slot], latent_gain), wkv[...], preferred_element_type=F32
        ).astype(BF16)
        pair = lax.dot_general(
            ropeall[slot], turner, (((0,), (0,)), ((), ())), preferred_element_type=F32
        ) * table[at, :]
        pair = pair + pltpu.roll(pair, 64, 1)
        turned = jnp.where(lane < 64, pair, 0.0).astype(BF16)
        for h in range(local_heads):
            base = h * (NOPE + VDIM)
            ks[h, at, 0:NOPE] = both[:, base:base + NOPE]
            ks[h, at, NOPE:256] = turned
            vs[h, at, :] = both[:, base + NOPE:base + NOPE + VDIM]

    def query_rows(slot):
        at = pl.ds(pl.multiple_of(slot * rows, rows), rows)
        qn[at, :] = scaled_rows(qall[slot], query_gain)

    relay_some(k + 1)
    wkv_copy.wait()
    table_copy.wait()
    keyval(i)
    relay_some(1)
    query_rows(i)
    relay_some(1)
    arrive(0, partner)
    arrive(1, partner)
    keyval(partner)
    relay_some(1)
    for d in range(1, n_chips):
        forward(0, d)
        forward(1, d)
        keyval(far_slot(d))
        relay_some(1)
    arrive(2, partner)
    query_rows(partner)
    relay_some(2)
    for d in range(1, n_chips):
        other = far_slot(d) + 1 - 2 * core
        arrive(0, other)
        arrive(1, other)
        keyval(other)
        relay_some(2)
    for d in range(1, n_chips):
        forward(2, d)
        query_rows(far_slot(d))
        relay_some(2)
    for d in range(1, n_chips):
        other = far_slot(d) + 1 - 2 * core
        arrive(2, other)
        query_rows(other)
    relay_some(len(events_left))

    def raw_queries(slot, hh):
        if groups > 1:
            total = jnp.dot(wqall[slot], spread[hh], preferred_element_type=F32)
        else:
            total = None
            for s in range(k):
                if (s + 1) * width <= hh * HEAD or s * width >= (hh + 1) * HEAD:
                    continue
                term = jnp.dot(
                    wqall[s], spread_matrix(width, s * width, hh), preferred_element_type=F32
                )
                total = term if total is None else total + term
        return jnp.dot(qn[...], total.astype(BF16), preferred_element_type=F32)

    def queries(slot):
        for hh in range(per_group):
            h = slot * per_group + hh
            raw = raw_queries(slot, hh)
            qs[h, :, 0:NOPE] = raw[:, 0:NOPE].astype(BF16)
            pair = raw[:, NOPE:256] * table[...]
            qs[h, :, NOPE:256] = (pair + pltpu.roll(pair, 64, 1)).astype(BF16)

    power = HEAD ** (-0.5) * float(np.log2(np.e))
    causal = lax.broadcasted_iota(jnp.int32, (rows, rows), 1) <= lax.broadcasted_iota(
        jnp.int32, (rows, rows), 0
    )

    def attend(b, slot):
        stop = (b + 1) * rows
        for hh in range(per_group):
            h = slot * per_group + hh
            scores = lax.dot_general(
                qs[h, b * rows:stop, :], ks[h, 0:stop, :], (((1,), (1,)), ((), ())),
                preferred_element_type=F32,
            )
            last = jnp.where(causal, scores[:, b * rows:], -jnp.inf)
            if b:
                scores = jnp.concatenate([scores[:, :b * rows], last], axis=1)
            else:
                scores = last
            top = jnp.max(scores, axis=-1, keepdims=True)
            weights = jnp.exp2((scores - top) * power)
            row_total = jnp.sum(weights, axis=-1, keepdims=True)
            summed = jnp.dot(weights.astype(BF16), vs[h, 0:stop, :], preferred_element_type=F32)
            att_out[b, slot, :, hh * VDIM:(hh + 1) * VDIM] = (summed / row_total).astype(BF16)

    def att_copy(b, slot):
        return pltpu.make_async_remote_copy(
            src_ref=att_out.at[b, slot], dst_ref=att_in.at[i, slot],
            send_sem=att_send.at[b, slot], recv_sem=att_recv.at[i, slot],
            device_id={"sp": b}, device_id_type=MESH,
        )

    for t, slot in enumerate(columns):
        if t:
            for event in events[t]:
                relay(*event)
        queries(slot)
        for c in range(n_chips):
            @pl.when(chip != c)
            def _(c=c):
                for b in (2 * c, 2 * c + 1):
                    attend(b, slot)
                    att_copy(b, slot).start()
    for c in range(n_chips):
        @pl.when(chip == c)
        def _(c=c):
            for slot in columns:
                for b in (2 * c, 2 * c + 1):
                    attend(b, slot)
    for slot in columns:
        att_copy(partner, slot).start()

    wout_copy.wait()
    squares = None
    order = [partner]
    for d in range(1, n_chips):
        order += [far_slot(d), far_slot(d) + 1 - 2 * core]
    for t, s in enumerate([i] + order):
        source = att_out
        if t:
            source = att_in
            for slot in range(groups):
                pltpu.make_async_remote_copy(
                    src_ref=att_in.at[s, slot], dst_ref=att_in.at[s, slot],
                    send_sem=att_send.at[0, slot], recv_sem=att_recv.at[s, slot],
                    device_id={"sp": partner}, device_id_type=MESH,
                ).wait_recv()
        values = jnp.concatenate([source[s, slot] for slot in range(groups)], axis=1).astype(F32)
        at = pl.ds(pl.multiple_of(s * group, group), group)
        square = jnp.sum(values * values, axis=-1, keepdims=True)
        squares = square if squares is None else squares + square
        scaled = (values * out_gain[s]).astype(BF16)
        term = jnp.dot(scaled, wout[at, :], preferred_element_type=F32)
        if t == 0:
            acc[...] = term
        elif t < n - 1:
            acc[...] += term
        else:
            factor = lax.rsqrt(squares / (n * group) + 1e-05)
            out_ref[0] = ((acc[...] + term) * factor).astype(BF16)

    for copy in sends:
        copy.wait_send()
    for event in sum(events, []):
        relay_finish(*event)
    for b in range(n):
        @pl.when(i != b)
        def _(b=b):
            for slot in range(groups):
                att_copy(b, slot).wait_send()


def paired_table(length):
    half = ROPE // 2
    inverse = np.float32(10000.0) ** (-np.arange(half, dtype=np.float32) / np.float32(half))
    angles = np.arange(length, dtype=np.float32)[:, None] * inverse[None, :].astype(np.float32)
    angles = angles.astype(np.float64)
    cosine, sine = np.cos(angles), np.sin(angles)
    parts = [cosine] * 4 + [-sine, sine, -sine, sine]
    return np.concatenate(parts, axis=1).astype(np.float32)


def paired_kernel(
    geometry,
    q_ref, kv_ref, rope_ref, wq_ref, wkv_ref, wout_ref, table_ref, qg_ref, lg_ref, og_ref,
    out_ref,
    qall, kvall, ropeall, wqa, wqb, assist, wkv, wout, table, qgain, lgain, ogain, head_gain, qn, qs, ks, vs,
    att_out, att_in, acc,
    local_sem, gat_send, gat_recv, w_send, w_recv, x_recv, att_send, att_recv,
):
    n, X, Z, chunks, local_heads = geometry
    whead = (wqa, wqb)
    first_width = wqa.shape[2]
    rows = q_ref.shape[1]
    n_chips = n // 2
    i = lax.axis_index("sp")
    j = lax.axis_index("dp")
    core = lax.rem(i, 2)
    chip = lax.div(i, 2)
    partner = i + 1 - 2 * core
    z = lax.div(j, X)
    x = lax.rem(j, X)
    across = 1 - x
    zo = i
    owns = z == zo

    gathered = ((kv_ref.at[0], kvall), (rope_ref.at[0], ropeall), (q_ref.at[0], qall))
    own_copies = [
        pltpu.make_async_copy(src, dst.at[i], local_sem.at[a]) for a, (src, dst) in enumerate(gathered)
    ]
    wq_copies = [
        pltpu.make_async_copy(wq_ref.at[:, 0:first_width], wqa.at[x], local_sem.at[3]),
        pltpu.make_async_copy(
            wq_ref.at[:, first_width:first_width + wqb.shape[2]], wqb.at[x], local_sem.at[10]
        ),
    ]
    wkv_copy = pltpu.make_async_copy(wkv_ref, wkv, local_sem.at[4])
    table_copy = pltpu.make_async_copy(table_ref, table, local_sem.at[5])
    wout_copy = pltpu.make_async_copy(wout_ref, wout, local_sem.at[6])
    gain_copies = [
        pltpu.make_async_copy(src, dst, local_sem.at[7 + a])
        for a, (src, dst) in enumerate(((qg_ref, qgain), (lg_ref, lgain), (og_ref, ogain)))
    ]

    assist_copy = pltpu.make_async_copy(
        wq_ref.at[:, first_width:first_width + wqb.shape[2]], assist, local_sem.at[11]
    )

    barrier = pltpu.get_barrier_semaphore()
    for d in range(1, n):
        pl.semaphore_signal(
            barrier, inc=1, device_id={"sp": lax.rem(i + d, n)}, device_id_type=MESH
        )
    def places(owner):
        low = owner * 2 < Z
        inner = owner == jnp.where(low, 1, Z - 2)
        last = jnp.where(low, Z - 1, 0)
        relayer = jnp.where(low, Z - 2, 1)
        return last, relayer, jnp.where(low, jnp.where(inner, 0, 1), jnp.where(inner, Z - 1, Z - 2))

    end, mid, other = places(zo)
    at_mid, at_end, at_other = z == mid, z == end, z == other
    twin = lax.rem(i + n // 2, n)
    twin_end = places(twin)[0]
    assists = z == twin

    def row(target, column=x):
        return target * X + column

    greet = (
        (at_other | at_mid, {"dp": row(zo)}), (at_end, {"dp": row(mid)}),
        (at_end, {"sp": twin, "dp": row(zo)}), (at_end, {"sp": twin, "dp": row(zo, across)}),
    )
    pl.semaphore_signal(barrier, inc=1, device_id={"dp": row(z, across)}, device_id_type=MESH)
    count = n + jnp.where(owns, 2, 0) + jnp.where(at_mid, 1, 0) + jnp.where(assists, 2, 0)
    for present, target in greet:
        @pl.when(present)
        def _(target=target):
            pl.semaphore_signal(barrier, inc=1, device_id=target, device_id_type=MESH)

    @pl.when(z == i)
    def _():
        for copy in wq_copies:
            copy.start()

    for copy in own_copies:
        copy.start()
    for copy in gain_copies:
        copy.start()

    @pl.when(assists)
    def _():
        assist_copy.start()

    wkv_copy.start()
    table_copy.start()

    for h in range(local_heads):
        vs[h, :, VDIM:2 * VDIM] = jnp.ones((vs.shape[1], VDIM), BF16)
    r = lax.broadcasted_iota(jnp.int32, (ROPE, 128), 0)
    f = lax.broadcasted_iota(jnp.int32, (ROPE, 128), 1)
    turner = jnp.where(r == lax.rem(f, ROPE), 1.0, 0.0).astype(BF16)

    parts = [(part, c) for part in range(2) for c in range(chunks[part])]

    def w_part(index):
        part, c = parts[index]
        step = whead[part].shape[1] // chunks[part]
        return whead[part].at[x, pl.ds(c * step, step)]

    targets = (row(other), row(mid), row(end))

    def assist_send(column, sem):
        return pltpu.make_async_remote_copy(
            src_ref=assist, dst_ref=wqb.at[x], send_sem=w_send.at[4],
            recv_sem=x_recv.at[1 + sem],
            device_id={"sp": twin, "dp": row(twin_end, column)}, device_id_type=MESH,
        )

    def w_copy(side, c):
        part = w_part(c)
        return pltpu.make_async_remote_copy(
            src_ref=part, dst_ref=part, send_sem=w_send.at[parts[c][0]], recv_sem=w_recv.at[c],
            device_id={"dp": targets[side]}, device_id_type=MESH,
        )

    def x_copy(source, part):
        return pltpu.make_async_remote_copy(
            src_ref=source, dst_ref=source, send_sem=w_send.at[2 + part], recv_sem=x_recv.at[part],
            device_id={"dp": j + 1 - 2 * x}, device_id_type=MESH,
        )

    inner_owner = (zo != 0) & (zo != Z - 1)
    roles = (at_mid | (at_other & jnp.logical_not(inner_owner)), at_other & inner_owner, at_end)
    chunks_left = [list(range(len(parts))) for _ in roles]
    chunks_left[2] = chunks_left[2][:chunks[0]]

    def relay_one(index):
        w_copy(0, index).wait_recv()
        if parts[index][0] == 0:
            @pl.when(at_mid)
            def _():
                w_copy(2, index).start()
        x_copy(w_part(index), parts[index][0]).start()

    def relay(*numbers):
        for role, number, left in zip(roles, numbers, chunks_left):
            todo = [left.pop(0) for _ in range(min(number, len(left)))]
            if todo:
                @pl.when(role)
                def _(todo=todo):
                    for index in todo:
                        relay_one(index)

    def peer(slot, reader):
        return lax.rem(slot - reader + n, n) - 1

    def gather_copy(a, slot, target, reader=None):
        dst = gathered[a][1]
        return pltpu.make_async_remote_copy(
            src_ref=dst.at[slot], dst_ref=dst.at[slot], send_sem=gat_send.at[a],
            recv_sem=gat_recv.at[a, peer(slot, target if reader is None else reader)],
            device_id={"sp": target}, device_id_type=MESH,
        )

    def far_slot(d):
        return 2 * lax.rem(chip + n_chips - d, n_chips) + core

    def arrive(a, slot):
        gather_copy(a, slot, partner, i).wait_recv()

    def forward(a, d):
        arrive(a, far_slot(d))
        gather_copy(a, far_slot(d), partner).start()

    lane = lax.broadcasted_iota(jnp.int32, (rows, 128), 1)
    left = lane < 64

    def turned_pair(both_halves, at):
        swap_low = lax.rem(lax.broadcasted_iota(jnp.int32, both_halves.shape, 1), 64) < 32
        swapped = jnp.where(
            swap_low, pltpu.roll(both_halves, 96, 1), pltpu.roll(both_halves, 32, 1)
        )
        return both_halves * table[at, 0:128] + swapped * table[at, 128:256]

    def keyval(slot):
        at = pl.ds(pl.multiple_of(slot * rows, rows), rows)
        both = jnp.dot(
            scaled_rows(kvall[slot], lgain[...].astype(F32).reshape(1, -1)), wkv[...],
            preferred_element_type=F32,
        )
        twice = lax.dot_general(
            ropeall[slot], turner, (((0,), (0,)), ((), ())), preferred_element_type=F32
        )
        turned = turned_pair(twice, at)
        for h in range(local_heads):
            base = h * (NOPE + VDIM)
            key = both[:, base:base + NOPE]
            if h % 2 == 0:
                ks[h, at, 0:NOPE] = key.astype(BF16)
                ks[h, at, NOPE:256] = jnp.where(left, turned, 0.0).astype(BF16)
            else:
                key = pltpu.roll(key, 64, 1)
                ks[h, at, 0:NOPE] = jnp.where(left, 0.0, key).astype(BF16)
                ks[h, at, NOPE:256] = jnp.where(left, key, turned).astype(BF16)
            vs[h, at, 0:VDIM] = both[:, base + NOPE:base + NOPE + VDIM].astype(BF16)

    def query_rows(slot):
        at = pl.ds(pl.multiple_of(slot * rows, rows), rows)
        qn[at, :] = scaled_rows(qall[slot], qgain[...].astype(F32).reshape(1, -1))

    @pl.when(owns)
    def _():
        for copy in wq_copies:
            copy.wait()

    for copy in own_copies:
        copy.wait()

    pl.semaphore_wait(barrier, count)

    for a in range(3):
        for d in range(1, n_chips):
            gather_copy(a, i, 2 * lax.rem(chip + d, n_chips) + core).start()

    @pl.when(owns)
    def _():
        for part in range(2):
            x_copy(whead[part].at[x], part).start()
        for index in range(len(parts)):
            w_copy(1, index).start()
            w_copy(0, index).start()

    for a in range(3):
        gather_copy(a, i, partner).start()

    wout_copy.start()
    for copy in gain_copies:
        copy.wait()
    query_rows(i)
    every_gain = ogain[...].astype(F32).reshape(1, -1)
    for h in range(n * local_heads):
        head_gain[h] = every_gain[:, h * VDIM:(h + 1) * VDIM]

    wkv_copy.wait()
    table_copy.wait()
    keyval(i)
    arrive(0, partner)
    arrive(1, partner)
    keyval(partner)
    arrive(2, partner)
    query_rows(partner)
    relay(8, 12, 0)
    for d in range(1, n_chips):
        forward(0, d)
        forward(1, d)
        relay(1, 2, 0)
        keyval(far_slot(d))

    @pl.when(assists)
    def _():
        assist_copy.wait()
        assist_send(x, 1).start()

    relay(2, 2, 2)
    for d in range(1, n_chips):
        other = far_slot(d) + 1 - 2 * core
        arrive(0, other)
        arrive(1, other)
        keyval(other)

    @pl.when(assists)
    def _():
        assist_send(across, 0).start()

    relay(5, 1, 4)
    for d in range(1, n_chips):
        forward(2, d)
        query_rows(far_slot(d))
    relay(0, 1, 6)
    for d in range(1, n_chips):
        other = far_slot(d) + 1 - 2 * core
        arrive(2, other)
        query_rows(other)
    relay(1, 2, 16)

    wide_left = lax.broadcasted_iota(jnp.int32, (2 * rows, 128), 1) < 64

    def queries(slot, part, c):
        at = pl.ds(c * 2 * rows, 2 * rows)
        raw = jnp.dot(qn[at, :], whead[part][slot], preferred_element_type=F32)
        last = raw[:, raw.shape[1] - 128:]
        turned = turned_pair(last, at)
        if part == 0:
            qs[slot, at, 0:128] = raw[:, 0:128].astype(BF16)
            qs[slot, at, 128:256] = jnp.where(wide_left, turned, last).astype(BF16)
        else:
            qs[slot, at, 256:384] = jnp.where(wide_left, last, turned).astype(BF16)

    power = HEAD ** (-0.5) * float(np.log2(np.e))
    block = 2 * rows
    causal = lax.broadcasted_iota(jnp.int32, (block, block), 1) <= lax.broadcasted_iota(
        jnp.int32, (block, block), 0
    )

    def attend(c, slot, heads):
        start, stop = c * block, (c + 1) * block
        scores = []
        for hh in heads:
            score = lax.dot_general(
                qs[slot, start:stop, hh * 128:hh * 128 + 256], ks[2 * slot + hh, 0:stop, :],
                (((1,), (1,)), ((), ())), preferred_element_type=F32,
            )
            last = jnp.where(causal, score[:, start:], -jnp.inf)
            scores.append(jnp.concatenate([score[:, :start], last], axis=1) if c else last)
        tops = [jnp.max(score, axis=-1, keepdims=True) for score in scores]
        weights = [
            jnp.exp2((score - top) * power).astype(BF16) for score, top in zip(scores, tops)
        ]
        for hh, weight in zip(heads, weights):
            summed = jnp.dot(weight, vs[2 * slot + hh, 0:stop, :], preferred_element_type=F32)
            result = (summed[:, 0:VDIM] / summed[:, VDIM:2 * VDIM]).astype(BF16)
            for e in range(2):
                att_out[2 * c + e, 2 * slot + hh] = result[e * rows:(e + 1) * rows]

    def att_copy(b, head):
        return pltpu.make_async_remote_copy(
            src_ref=att_out.at[b, head], dst_ref=att_in.at[i, head],
            send_sem=att_send.at[0], recv_sem=att_recv.at[peer(i, b), head],
            device_id={"sp": b}, device_id_type=MESH,
        )

    def far_head(slot, hh):
        for c in range(n_chips):
            @pl.when(chip != c)
            def _(c=c):
                queries(slot, hh, c)
                attend(c, slot, (hh,))
                for b in (2 * c, 2 * c + 1):
                    att_copy(b, 2 * slot + hh).start()

    def own_heads(slot):
        for c in range(n_chips):
            @pl.when(chip == c)
            def _(c=c):
                for hh in range(2):
                    queries(slot, hh, c)
                attend(c, slot, (0, 1))
        for hh in range(2):
            att_copy(partner, 2 * slot + hh).start()

    far_head(x, 0)
    relay(len(parts), len(parts), 0)

    @pl.when(at_end)
    def _():
        assist_send(x, 1).wait_recv()

    far_head(x, 1)
    own_heads(x)
    for part in range(2):
        x_copy(whead[part].at[across], part).wait_recv()
        far_head(across, part)
    own_heads(across)

    wout_copy.wait()
    squares = []
    group = local_heads * VDIM

    def product(pieces):
        sides = []
        for s, first, number in pieces:
            values = []
            for hh in range(number):
                if s is not i:
                    pltpu.make_async_remote_copy(
                        src_ref=att_in.at[s, first + hh], dst_ref=att_in.at[s, first + hh],
                        send_sem=att_send.at[0], recv_sem=att_recv.at[peer(s, i), first + hh],
                        device_id={"sp": partner}, device_id_type=MESH,
                    ).wait_recv()
                value = (att_out if s is i else att_in)[s, first + hh].astype(F32)
                squares.append(value * value)
                values.append((value * head_gain[s * local_heads + first + hh]).astype(BF16))
            at = pl.multiple_of(s * group + first * VDIM, VDIM)
            sides.append((values, wout[pl.ds(at, number * VDIM), :]))
        return jnp.dot(
            jnp.concatenate(sum((values for values, _ in sides), []), axis=1),
            jnp.concatenate([rows_of for _, rows_of in sides], axis=0),
            preferred_element_type=F32,
        )

    far = []
    for d in range(1, n_chips):
        far += [far_slot(d), far_slot(d) + 1 - 2 * core]
    acc[...] = product([(i, 0, local_heads)])
    acc[...] += product([(s, 2 * x, 2) for s in far])
    acc[...] += product([(partner, 0, local_heads)])
    acc[...] += product([(s, 2 * across, 1) for s in far])
    term = product([(s, 2 * across + 1, 1) for s in far])
    squared = jnp.sum(sum(squares[1:], squares[0]), axis=-1, keepdims=True)
    factor = lax.rsqrt(squared / (n * group) + 1e-05)
    out_ref[0] = ((acc[...] + term) * factor).astype(BF16)

    for a in range(3):
        every = gathered[a][1].at[pl.ds(0, n - 1)]
        pltpu.make_async_remote_copy(
            src_ref=every, dst_ref=every, send_sem=gat_send.at[a], recv_sem=gat_recv.at[a, 0],
            device_id={"sp": partner}, device_id_type=MESH,
        ).wait_send()
    def all_sent(every, sem):
        pltpu.make_async_remote_copy(
            src_ref=every, dst_ref=every, send_sem=w_send.at[sem], recv_sem=w_recv.at[0],
            device_id={"dp": targets[0]}, device_id_type=MESH,
        ).wait_send()

    @pl.when(owns)
    def _():
        all_sent(wqa, 0)
        all_sent(wqb, 1)

    @pl.when(at_mid)
    def _():
        all_sent(wqa.at[x], 0)

    @pl.when(assists)
    def _():
        all_sent(wqb, 4)

    x_copy(wqa.at[x], 0).wait_send()

    @pl.when(jnp.logical_not(at_end))
    def _():
        x_copy(wqb.at[x], 1).wait_send()

    every = att_out.at[pl.ds(0, n - 1)]
    pltpu.make_async_remote_copy(
        src_ref=every, dst_ref=every, send_sem=att_send.at[0], recv_sem=att_recv.at[0, 0],
        device_id={"sp": partner}, device_id_type=MESH,
    ).wait_send()


def paired(
    mesh, columns, q_latent, kv_latent, rope_key, w_query, w_keyval, w_out, query_gain, latent_gain,
    out_gain,
):
    n, m = mesh.shape["sp"], mesh.shape["dp"]
    rows = q_latent.shape[1]
    length = n * rows
    rank = q_latent.shape[2]
    width = w_query.shape[1]
    local_heads = H // n
    chunks = (16, 4)
    dim = w_out.shape[1]
    geometry = (n, columns, m // columns, chunks, local_heads)
    any_spec = pl.BlockSpec(memory_space=pl.ANY)
    vmem_spec = pl.BlockSpec(memory_space=pltpu.VMEM)
    dma = pltpu.SemaphoreType.DMA
    return pl.pallas_call(
        functools.partial(paired_kernel, geometry),
        out_shape=pltpu.VMEM((1, rows, dim), BF16),
        in_specs=[any_spec] * 10,
        out_specs=vmem_spec,
        scratch_shapes=[
            pltpu.VMEM((n, rows, rank), BF16),
            pltpu.VMEM((n, rows, kv_latent.shape[2]), BF16),
            pltpu.VMEM((n, ROPE, rows), BF16),
            pltpu.VMEM((columns, rank, 2 * NOPE), BF16),
            pltpu.VMEM((columns, rank, width - 2 * NOPE), BF16),
            pltpu.VMEM((rank, width - 2 * NOPE), BF16),
            pltpu.VMEM(w_keyval.shape, BF16),
            pltpu.VMEM(w_out.shape, BF16),
            pltpu.VMEM((length, 256), F32),
            pltpu.VMEM(query_gain.shape, BF16),
            pltpu.VMEM(latent_gain.shape, BF16),
            pltpu.VMEM(out_gain.shape, BF16),
            pltpu.VMEM((n * local_heads, 1, VDIM), F32),
            pltpu.VMEM((length, rank), BF16),
            pltpu.VMEM((columns, length, width), BF16),
            pltpu.VMEM((local_heads, length, 256), BF16),
            pltpu.VMEM((local_heads, length, 2 * VDIM), BF16),
            pltpu.VMEM((n, local_heads, rows, VDIM), BF16),
            pltpu.VMEM((n, local_heads, rows, VDIM), BF16),
            pltpu.VMEM((rows, dim), F32),
            dma((12,)),
            dma((3,)),
            dma((3, n - 1)),
            dma((5,)),
            dma((sum(chunks),)),
            dma((3,)),
            dma((1,)),
            dma((n - 1, local_heads)),
        ],
        compiler_params=pltpu.CompilerParams(
            collective_id=0, has_side_effects=True, vmem_limit_bytes=56 * 1024 * 1024,
        ),
    )(
        q_latent, kv_latent, jnp.swapaxes(rope_key, 1, 2), w_query, w_keyval, w_out,
        jnp.asarray(paired_table(length)), query_gain, latent_gain, out_gain,
    )


def x_size(mesh):
    row = mesh.devices[0]
    places = [getattr(device, "coords", None) for device in row]
    if any(place is None for place in places):
        return 1
    return len({place[0] for place in places})


def per_device(
    mesh, q_latent, kv_latent, rope_key, w_query, w_keyval, w_out, query_gain, latent_gain, out_gain
):
    n, m = mesh.shape["sp"], mesh.shape["dp"]
    rows = q_latent.shape[1]
    length = n * rows
    rank = q_latent.shape[2]
    width = w_query.shape[1]
    local_heads = H // n
    k = local_heads * HEAD // width
    chunks = 16
    columns = x_size(mesh)
    groups = k if k == columns == 2 and width % HEAD == 0 else 1
    dim = w_out.shape[1]
    group = local_heads * VDIM
    if groups == columns and width == 2 * HEAD and H % m == 0 and n == 4 and m == n * columns:
        return paired(
            mesh, columns, q_latent, kv_latent, rope_key, w_query, w_keyval, w_out, query_gain,
            latent_gain, out_gain,
        )
    table = jnp.asarray(turn_table(length))
    geometry = (n, m, columns, k, chunks, local_heads, groups)
    any_spec = pl.BlockSpec(memory_space=pl.ANY)
    vmem_spec = pl.BlockSpec(memory_space=pltpu.VMEM)
    dma = pltpu.SemaphoreType.DMA
    return pl.pallas_call(
        functools.partial(kernel, geometry),
        out_shape=pltpu.VMEM((1, rows, dim), BF16),
        in_specs=[any_spec] * 7 + [vmem_spec] * 3,
        out_specs=vmem_spec,
        scratch_shapes=[
            pltpu.VMEM((n, rows, rank), BF16),
            pltpu.VMEM((n, rows, kv_latent.shape[2]), BF16),
            pltpu.VMEM((n, ROPE, rows), BF16),
            pltpu.VMEM((k, rank, width), BF16),
            pltpu.VMEM(w_keyval.shape, BF16),
            pltpu.VMEM(w_out.shape, BF16),
            pltpu.VMEM((length, 128), F32),
            pltpu.VMEM((local_heads // groups, width, 256), BF16),
            pltpu.VMEM((length, rank), BF16),
            pltpu.VMEM((local_heads, length, 256), BF16),
            pltpu.VMEM((local_heads, length, 256), BF16),
            pltpu.VMEM((local_heads, length, VDIM), BF16),
            pltpu.VMEM((n, groups, rows, group // groups), BF16),
            pltpu.VMEM((n, groups, rows, group // groups), BF16),
            pltpu.VMEM((rows, dim), F32),
            pltpu.VMEM((n, 1, group), F32),
            dma((7,)),
            dma((3, n // 2)),
            dma((3, n)),
            dma((3, n // 2)),
            dma((4, k, chunks)),
            dma((k, chunks)),
            dma((n, groups)),
            dma((n, groups)),
        ],
        compiler_params=pltpu.CompilerParams(
            collective_id=0, has_side_effects=True, vmem_limit_bytes=56 * 1024 * 1024
        ),
    )(
        q_latent, kv_latent, jnp.swapaxes(rope_key, 1, 2), w_query, w_keyval, w_out, table,
        query_gain, latent_gain, out_gain,
    )


def solution(mesh):
    in_specs = (
        P("dp", "sp", None),
        P("dp", "sp", None),
        P("dp", "sp", None),
        P(None, "dp"),
        P(None, "sp"),
        P(),
        P(),
        P(),
        P(),
    )
    return jax.shard_map(
        functools.partial(per_device, mesh), mesh=mesh, in_specs=in_specs,
        out_specs=P("dp", "sp", None), check_vma=False,
    )
```

```python
import functools

import jax
import jax.numpy as jnp
import numpy as np
from jax import lax
from jax.experimental import pallas as pl
from jax.experimental.pallas import tpu as pltpu
from jax.sharding import PartitionSpec as P

H = 16
NOPE = 128
ROPE = 64
VDIM = 128
HEAD = NOPE + ROPE
MESH = pl.DeviceIdType.MESH
F32 = jnp.float32
BF16 = jnp.bfloat16


def turn_table(length):
    half = ROPE // 2
    inverse = np.float32(10000.0) ** (-np.arange(half, dtype=np.float32) / np.float32(half))
    angles = np.arange(length, dtype=np.float32)[:, None] * inverse[None, :].astype(np.float32)
    angles = angles.astype(np.float64)
    cosine, sine = np.cos(angles), np.sin(angles)
    return np.concatenate([cosine, cosine, sine, sine], axis=1).astype(np.float32)


def spread_matrix(rows, row_start, head):
    g = lax.broadcasted_iota(jnp.int32, (rows, 256), 0) + row_start
    f = lax.broadcasted_iota(jnp.int32, (rows, 256), 1)
    source = jnp.where(f < HEAD, f, jnp.where(f < HEAD + 32, f - 32, f - 96)) + head * HEAD
    sign = jnp.where((f >= HEAD) & (f < HEAD + 32), -1.0, 1.0)
    return jnp.where(g == source, sign, 0.0).astype(BF16)


def rope_matrix():
    r = lax.broadcasted_iota(jnp.int32, (ROPE, 128), 0)
    f = lax.broadcasted_iota(jnp.int32, (ROPE, 128), 1)
    source = jnp.where(f < 64, f, jnp.where(f < 96, f - 32, f - 96))
    sign = jnp.where((f >= 64) & (f < 96), -1.0, 1.0)
    return jnp.where(r == source, sign, 0.0).astype(BF16)


def scaled_rows(values, gain):
    wide = values.astype(F32)
    mean = jnp.mean(wide * wide, axis=-1, keepdims=True)
    return (wide * lax.rsqrt(mean + 1e-05) * gain).astype(BF16)


def kernel(
    geometry,
    q_ref, kv_ref, rope_ref, wq_ref, wkv_ref, wout_ref, table_ref, qg_ref, lg_ref, og_ref,
    out_ref,
    qall, kvall, ropeall, wqall, wkv, wout, table, spread, qn, qs, ks, vs, att_out, att_in, acc,
    out_gain,
    local_sem, gat_send, gat_recv, fwd_send, w_send, w_recv, att_send, att_recv,
):
    n, m, X, k, chunks, local_heads, groups = geometry
    per_group = local_heads // groups
    width = wqall.shape[2]
    Z = m // X
    rows = q_ref.shape[1]
    n_chips = n // 2
    i = lax.axis_index("sp")
    j = lax.axis_index("dp")
    core = lax.rem(i, 2)
    chip = lax.div(i, 2)
    partner = i + 1 - 2 * core
    z = lax.div(j, X)
    x = lax.rem(j, X)
    first = i * k
    owns = (j >= first) & (j < first + k)

    gathered = ((kv_ref.at[0], kvall), (rope_ref.at[0], ropeall), (q_ref.at[0], qall))
    own_copies = [
        pltpu.make_async_copy(src, dst.at[i], local_sem.at[a]) for a, (src, dst) in enumerate(gathered)
    ]
    wq_copy = pltpu.make_async_copy(wq_ref, wqall.at[lax.rem(j, k)], local_sem.at[3])
    wkv_copy = pltpu.make_async_copy(wkv_ref, wkv, local_sem.at[4])
    table_copy = pltpu.make_async_copy(table_ref, table, local_sem.at[5])
    wout_copy = pltpu.make_async_copy(wout_ref, wout, local_sem.at[6])

    @pl.when(owns)
    def _():
        wq_copy.start()

    for copy in own_copies:
        copy.start()
    wkv_copy.start()
    table_copy.start()
    wout_copy.start()

    turner = rope_matrix()
    latent_gain = lg_ref[...].astype(F32).reshape(1, -1)
    query_gain = qg_ref[...].astype(F32).reshape(1, -1)
    group = local_heads * VDIM
    every_gain = og_ref[...].astype(F32).reshape(1, -1)
    for s in range(n):
        out_gain[s] = every_gain[:, s * group:(s + 1) * group]
    if groups > 1:
        for h in range(per_group):
            spread[h] = spread_matrix(width, 0, h)

    barrier = pltpu.get_barrier_semaphore()
    for d in range(1, n):
        pl.semaphore_signal(
            barrier, inc=1, device_id={"sp": lax.rem(i + d, n)}, device_id_type=MESH
        )
    sides = ((z < Z - 1, j + X), (z > 0, j - X), (x < X - 1, j + 1), (x > 0, j - 1))
    count = n - 1
    for present, target in sides:
        @pl.when(present)
        def _(target=target):
            pl.semaphore_signal(barrier, inc=1, device_id={"dp": target}, device_id_type=MESH)
        count = count + jnp.where(present, 1, 0)
    pl.semaphore_wait(barrier, count)

    step_rows = wqall.shape[1] // chunks

    def relay_parts(slot, c):
        owner = first + slot
        zo, xo = lax.div(owner, X), lax.rem(owner, X)
        part = wqall.at[slot, pl.ds(c * step_rows, step_rows)]
        in_column = x == xo
        conditions = (
            in_column & (z >= zo) & (z < Z - 1),
            in_column & (z <= zo) & (z > 0),
            (x >= xo) & (x < X - 1),
            (x <= xo) & (x > 0),
        )
        copies = [
            pltpu.make_async_remote_copy(
                src_ref=part, dst_ref=part,
                send_sem=w_send.at[side, slot, c], recv_sem=w_recv.at[slot, c],
                device_id={"dp": sides[side][1]}, device_id_type=MESH,
            )
            for side in range(4)
        ]
        return owner, conditions, copies

    def relay(slot, c):
        owner, conditions, copies = relay_parts(slot, c)

        @pl.when(owner != j)
        def _():
            copies[0].wait_recv()

        for condition, copy in zip(conditions, copies):
            @pl.when(condition)
            def _(copy=copy):
                copy.start()

    def relay_finish(slot, c):
        _, conditions, copies = relay_parts(slot, c)
        for condition, copy in zip(conditions, copies):
            @pl.when(condition)
            def _(copy=copy):
                copy.wait_send()

    if groups > 1:
        columns = [lax.rem(x + t, k) for t in range(k)]
        events = [[(column, c) for c in range(chunks)] for column in columns]
    else:
        columns = [0]
        events = [[(slot, c) for c in range(chunks) for slot in range(k)]]
    events_left = list(events[0])

    def relay_some(number):
        for _ in range(min(number, len(events_left))):
            relay(*events_left.pop(0))

    def gather_copy(a, slot, sem, target):
        dst = gathered[a][1]
        return pltpu.make_async_remote_copy(
            src_ref=dst.at[slot], dst_ref=dst.at[slot],
            send_sem=sem, recv_sem=gat_recv.at[a, slot],
            device_id={"sp": target}, device_id_type=MESH,
        )

    sends = []

    @pl.when(owns)
    def _():
        wq_copy.wait()

    for a in range(3):
        own_copies[a].wait()
        for d in range(1, n_chips):
            target = 2 * lax.rem(chip + d, n_chips) + core
            sends.append(gather_copy(a, i, gat_send.at[a, d], target))
            sends[-1].start()
    for a in range(3):
        sends.append(gather_copy(a, i, gat_send.at[a, 0], partner))
        sends[-1].start()

    def far_slot(d):
        return 2 * lax.rem(chip + n_chips - d, n_chips) + core

    def forward(a, d):
        slot = far_slot(d)
        copy = gather_copy(a, slot, fwd_send.at[a, d - 1], partner)
        copy.wait_recv()
        copy.start()
        sends.append(copy)

    def arrive(a, slot):
        gather_copy(a, slot, gat_send.at[a, 0], partner).wait_recv()

    lane = lax.broadcasted_iota(jnp.int32, (rows, 128), 1)

    def keyval(slot):
        at = pl.ds(pl.multiple_of(slot * rows, rows), rows)
        both = jnp.dot(
            scaled_rows(kvall[slot], latent_gain), wkv[...], preferred_element_type=F32
        ).astype(BF16)
        pair = lax.dot_general(
            ropeall[slot], turner, (((0,), (0,)), ((), ())), preferred_element_type=F32
        ) * table[at, :]
        pair = pair + pltpu.roll(pair, 64, 1)
        turned = jnp.where(lane < 64, pair, 0.0).astype(BF16)
        for h in range(local_heads):
            base = h * (NOPE + VDIM)
            ks[h, at, 0:NOPE] = both[:, base:base + NOPE]
            ks[h, at, NOPE:256] = turned
            vs[h, at, :] = both[:, base + NOPE:base + NOPE + VDIM]

    def query_rows(slot):
        at = pl.ds(pl.multiple_of(slot * rows, rows), rows)
        qn[at, :] = scaled_rows(qall[slot], query_gain)

    relay_some(k + 1)
    wkv_copy.wait()
    table_copy.wait()
    keyval(i)
    relay_some(1)
    query_rows(i)
    relay_some(1)
    arrive(0, partner)
    arrive(1, partner)
    keyval(partner)
    relay_some(1)
    for d in range(1, n_chips):
        forward(0, d)
        forward(1, d)
        keyval(far_slot(d))
        relay_some(1)
    arrive(2, partner)
    query_rows(partner)
    relay_some(2)
    for d in range(1, n_chips):
        other = far_slot(d) + 1 - 2 * core
        arrive(0, other)
        arrive(1, other)
        keyval(other)
        relay_some(2)
    for d in range(1, n_chips):
        forward(2, d)
        query_rows(far_slot(d))
        relay_some(2)
    for d in range(1, n_chips):
        other = far_slot(d) + 1 - 2 * core
        arrive(2, other)
        query_rows(other)
    relay_some(len(events_left))

    def raw_queries(slot, hh):
        if groups > 1:
            total = jnp.dot(wqall[slot], spread[hh], preferred_element_type=F32)
        else:
            total = None
            for s in range(k):
                if (s + 1) * width <= hh * HEAD or s * width >= (hh + 1) * HEAD:
                    continue
                term = jnp.dot(
                    wqall[s], spread_matrix(width, s * width, hh), preferred_element_type=F32
                )
                total = term if total is None else total + term
        return jnp.dot(qn[...], total.astype(BF16), preferred_element_type=F32)

    def queries(slot):
        for hh in range(per_group):
            h = slot * per_group + hh
            raw = raw_queries(slot, hh)
            qs[h, :, 0:NOPE] = raw[:, 0:NOPE].astype(BF16)
            pair = raw[:, NOPE:256] * table[...]
            qs[h, :, NOPE:256] = (pair + pltpu.roll(pair, 64, 1)).astype(BF16)

    power = HEAD ** (-0.5) * float(np.log2(np.e))
    causal = lax.broadcasted_iota(jnp.int32, (rows, rows), 1) <= lax.broadcasted_iota(
        jnp.int32, (rows, rows), 0
    )

    def attend(b, slot):
        stop = (b + 1) * rows
        for hh in range(per_group):
            h = slot * per_group + hh
            scores = lax.dot_general(
                qs[h, b * rows:stop, :], ks[h, 0:stop, :], (((1,), (1,)), ((), ())),
                preferred_element_type=F32,
            )
            last = jnp.where(causal, scores[:, b * rows:], -jnp.inf)
            if b:
                scores = jnp.concatenate([scores[:, :b * rows], last], axis=1)
            else:
                scores = last
            top = jnp.max(scores, axis=-1, keepdims=True)
            weights = jnp.exp2((scores - top) * power)
            row_total = jnp.sum(weights, axis=-1, keepdims=True)
            summed = jnp.dot(weights.astype(BF16), vs[h, 0:stop, :], preferred_element_type=F32)
            att_out[b, slot, :, hh * VDIM:(hh + 1) * VDIM] = (summed / row_total).astype(BF16)

    def att_copy(b, slot):
        return pltpu.make_async_remote_copy(
            src_ref=att_out.at[b, slot], dst_ref=att_in.at[i, slot],
            send_sem=att_send.at[b, slot], recv_sem=att_recv.at[i, slot],
            device_id={"sp": b}, device_id_type=MESH,
        )

    for t, slot in enumerate(columns):
        if t:
            for event in events[t]:
                relay(*event)
        queries(slot)
        for c in range(n_chips):
            @pl.when(chip != c)
            def _(c=c):
                for b in (2 * c, 2 * c + 1):
                    attend(b, slot)
                    att_copy(b, slot).start()
    for c in range(n_chips):
        @pl.when(chip == c)
        def _(c=c):
            for slot in columns:
                for b in (2 * c, 2 * c + 1):
                    attend(b, slot)
    for slot in columns:
        att_copy(partner, slot).start()

    wout_copy.wait()
    squares = None
    order = [partner]
    for d in range(1, n_chips):
        order += [far_slot(d), far_slot(d) + 1 - 2 * core]
    for t, s in enumerate([i] + order):
        source = att_out
        if t:
            source = att_in
            for slot in range(groups):
                pltpu.make_async_remote_copy(
                    src_ref=att_in.at[s, slot], dst_ref=att_in.at[s, slot],
                    send_sem=att_send.at[0, slot], recv_sem=att_recv.at[s, slot],
                    device_id={"sp": partner}, device_id_type=MESH,
                ).wait_recv()
        values = jnp.concatenate([source[s, slot] for slot in range(groups)], axis=1).astype(F32)
        at = pl.ds(pl.multiple_of(s * group, group), group)
        square = jnp.sum(values * values, axis=-1, keepdims=True)
        squares = square if squares is None else squares + square
        scaled = (values * out_gain[s]).astype(BF16)
        term = jnp.dot(scaled, wout[at, :], preferred_element_type=F32)
        if t == 0:
            acc[...] = term
        elif t < n - 1:
            acc[...] += term
        else:
            factor = lax.rsqrt(squares / (n * group) + 1e-05)
            out_ref[0] = ((acc[...] + term) * factor).astype(BF16)

    for copy in sends:
        copy.wait_send()
    for event in sum(events, []):
        relay_finish(*event)
    for b in range(n):
        @pl.when(i != b)
        def _(b=b):
            for slot in range(groups):
                att_copy(b, slot).wait_send()


def paired_table(length):
    half = ROPE // 2
    inverse = np.float32(10000.0) ** (-np.arange(half, dtype=np.float32) / np.float32(half))
    angles = np.arange(length, dtype=np.float32)[:, None] * inverse[None, :].astype(np.float32)
    angles = angles.astype(np.float64)
    cosine, sine = np.cos(angles), np.sin(angles)
    parts = [cosine] * 4 + [-sine, sine, -sine, sine]
    return np.concatenate(parts, axis=1).astype(np.float32)


def paired_kernel(
    geometry,
    q_ref, kv_ref, rope_ref, wq_ref, wkv_ref, wout_ref, table_ref, qg_ref, lg_ref, og_ref,
    out_ref,
    qall, kvall, ropeall, wqa, wqb, assist, wkv, wout, table, qgain, lgain, ogain, head_gain, qn, qs, ks, vs,
    att_out, att_in, acc,
    local_sem, gat_send, gat_recv, w_send, w_recv, x_recv, att_send, att_recv,
):
    n, X, Z, chunks, local_heads = geometry
    whead = (wqa, wqb)
    first_width = wqa.shape[2]
    rows = q_ref.shape[1]
    n_chips = n // 2
    i = lax.axis_index("sp")
    j = lax.axis_index("dp")
    core = lax.rem(i, 2)
    chip = lax.div(i, 2)
    partner = i + 1 - 2 * core
    z = lax.div(j, X)
    x = lax.rem(j, X)
    across = 1 - x
    zo = i
    owns = z == zo

    gathered = ((kv_ref.at[0], kvall), (rope_ref.at[0], ropeall), (q_ref.at[0], qall))
    own_copies = [
        pltpu.make_async_copy(src, dst.at[i], local_sem.at[a]) for a, (src, dst) in enumerate(gathered)
    ]
    wq_copies = [
        pltpu.make_async_copy(wq_ref.at[:, 0:first_width], wqa.at[x], local_sem.at[3]),
        pltpu.make_async_copy(
            wq_ref.at[:, first_width:first_width + wqb.shape[2]], wqb.at[x], local_sem.at[10]
        ),
    ]
    wkv_copy = pltpu.make_async_copy(wkv_ref, wkv, local_sem.at[4])
    table_copy = pltpu.make_async_copy(table_ref, table, local_sem.at[5])
    wout_copy = pltpu.make_async_copy(wout_ref, wout, local_sem.at[6])
    gain_copies = [
        pltpu.make_async_copy(src, dst, local_sem.at[7 + a])
        for a, (src, dst) in enumerate(((qg_ref, qgain), (lg_ref, lgain), (og_ref, ogain)))
    ]

    assist_copy = pltpu.make_async_copy(
        wq_ref.at[:, first_width:first_width + wqb.shape[2]], assist, local_sem.at[10]
    )

    barrier = pltpu.get_barrier_semaphore()
    for d in range(1, n):
        pl.semaphore_signal(
            barrier, inc=1, device_id={"sp": lax.rem(i + d, n)}, device_id_type=MESH
        )
    def places(owner):
        low = owner * 2 < Z
        inner = owner == jnp.where(low, 1, Z - 2)
        last = jnp.where(low, Z - 1, 0)
        relayer = jnp.where(low, Z - 2, 1)
        return last, relayer, jnp.where(low, jnp.where(inner, 0, 1), jnp.where(inner, Z - 1, Z - 2))

    end, mid, other = places(zo)
    at_mid, at_end, at_other = z == mid, z == end, z == other
    twin = lax.rem(i + n // 2, n)
    twin_end = places(twin)[0]
    assists = z == twin

    def row(target, column=x):
        return target * X + column

    greet = (
        (at_other | at_mid, {"dp": row(zo)}), (at_end, {"dp": row(mid)}),
        (at_end, {"sp": twin, "dp": row(zo)}), (at_end, {"sp": twin, "dp": row(zo, across)}),
    )
    pl.semaphore_signal(barrier, inc=1, device_id={"dp": row(z, across)}, device_id_type=MESH)
    count = n + jnp.where(owns, 2, 0) + jnp.where(at_mid, 1, 0) + jnp.where(assists, 2, 0)
    for present, target in greet:
        @pl.when(present)
        def _(target=target):
            pl.semaphore_signal(barrier, inc=1, device_id=target, device_id_type=MESH)

    @pl.when(z == i)
    def _():
        for copy in wq_copies:
            copy.start()

    for copy in own_copies:
        copy.start()
    for copy in gain_copies:
        copy.start()

    @pl.when(assists)
    def _():
        assist_copy.start()

    wkv_copy.start()
    table_copy.start()

    for h in range(local_heads):
        vs[h, :, VDIM:2 * VDIM] = jnp.ones((vs.shape[1], VDIM), BF16)
    r = lax.broadcasted_iota(jnp.int32, (ROPE, 128), 0)
    f = lax.broadcasted_iota(jnp.int32, (ROPE, 128), 1)
    turner = jnp.where(r == lax.rem(f, ROPE), 1.0, 0.0).astype(BF16)

    parts = [(part, c) for part in range(2) for c in range(chunks[part])]

    def w_part(index):
        part, c = parts[index]
        step = whead[part].shape[1] // chunks[part]
        return whead[part].at[x, pl.ds(c * step, step)]

    targets = (row(other), row(mid), row(end))

    def assist_send(column, sem):
        return pltpu.make_async_remote_copy(
            src_ref=assist, dst_ref=wqb.at[x], send_sem=w_send.at[1],
            recv_sem=x_recv.at[1 + sem],
            device_id={"sp": twin, "dp": row(twin_end, column)}, device_id_type=MESH,
        )

    def w_copy(side, c):
        part = w_part(c)
        return pltpu.make_async_remote_copy(
            src_ref=part, dst_ref=part, send_sem=w_send.at[parts[c][0]], recv_sem=w_recv.at[c],
            device_id={"dp": targets[side]}, device_id_type=MESH,
        )

    def x_copy(source, part):
        return pltpu.make_async_remote_copy(
            src_ref=source, dst_ref=source, send_sem=w_send.at[2 + part], recv_sem=x_recv.at[part],
            device_id={"dp": j + 1 - 2 * x}, device_id_type=MESH,
        )

    inner_owner = (zo != 0) & (zo != Z - 1)
    roles = (at_mid | (at_other & jnp.logical_not(inner_owner)), at_other & inner_owner, at_end)
    chunks_left = [list(range(len(parts))) for _ in roles]
    chunks_left[2] = chunks_left[2][:chunks[0]]

    def relay_one(index):
        w_copy(0, index).wait_recv()
        if parts[index][0] == 0:
            @pl.when(at_mid)
            def _():
                w_copy(2, index).start()
        x_copy(w_part(index), parts[index][0]).start()

    def relay(*numbers):
        for role, number, left in zip(roles, numbers, chunks_left):
            todo = [left.pop(0) for _ in range(min(number, len(left)))]
            if todo:
                @pl.when(role)
                def _(todo=todo):
                    for index in todo:
                        relay_one(index)

    def peer(slot, reader):
        return lax.rem(slot - reader + n, n) - 1

    def gather_copy(a, slot, target, reader=None):
        dst = gathered[a][1]
        return pltpu.make_async_remote_copy(
            src_ref=dst.at[slot], dst_ref=dst.at[slot], send_sem=gat_send.at[a],
            recv_sem=gat_recv.at[a, peer(slot, target if reader is None else reader)],
            device_id={"sp": target}, device_id_type=MESH,
        )

    def far_slot(d):
        return 2 * lax.rem(chip + n_chips - d, n_chips) + core

    def arrive(a, slot):
        gather_copy(a, slot, partner, i).wait_recv()

    def forward(a, d):
        arrive(a, far_slot(d))
        gather_copy(a, far_slot(d), partner).start()

    lane = lax.broadcasted_iota(jnp.int32, (rows, 128), 1)
    left = lane < 64

    def turned_pair(both_halves, at):
        swap_low = lax.rem(lax.broadcasted_iota(jnp.int32, both_halves.shape, 1), 64) < 32
        swapped = jnp.where(
            swap_low, pltpu.roll(both_halves, 96, 1), pltpu.roll(both_halves, 32, 1)
        )
        return both_halves * table[at, 0:128] + swapped * table[at, 128:256]

    def keyval(slot):
        at = pl.ds(pl.multiple_of(slot * rows, rows), rows)
        both = jnp.dot(
            scaled_rows(kvall[slot], lgain[...].astype(F32).reshape(1, -1)), wkv[...],
            preferred_element_type=F32,
        )
        twice = lax.dot_general(
            ropeall[slot], turner, (((0,), (0,)), ((), ())), preferred_element_type=F32
        )
        turned = turned_pair(twice, at)
        for h in range(local_heads):
            base = h * (NOPE + VDIM)
            key = both[:, base:base + NOPE]
            if h % 2 == 0:
                ks[h, at, 0:NOPE] = key.astype(BF16)
                ks[h, at, NOPE:256] = jnp.where(left, turned, 0.0).astype(BF16)
            else:
                key = pltpu.roll(key, 64, 1)
                ks[h, at, 0:NOPE] = jnp.where(left, 0.0, key).astype(BF16)
                ks[h, at, NOPE:256] = jnp.where(left, key, turned).astype(BF16)
            vs[h, at, 0:VDIM] = both[:, base + NOPE:base + NOPE + VDIM].astype(BF16)

    def query_rows(slot):
        at = pl.ds(pl.multiple_of(slot * rows, rows), rows)
        qn[at, :] = scaled_rows(qall[slot], qgain[...].astype(F32).reshape(1, -1))

    @pl.when(owns)
    def _():
        for copy in wq_copies:
            copy.wait()

    for copy in own_copies:
        copy.wait()

    pl.semaphore_wait(barrier, count)

    for a in range(3):
        for d in range(1, n_chips):
            gather_copy(a, i, 2 * lax.rem(chip + d, n_chips) + core).start()

    @pl.when(owns)
    def _():
        for part in range(2):
            x_copy(whead[part].at[x], part).start()
        for index in range(len(parts)):
            w_copy(1, index).start()
            w_copy(0, index).start()

    for a in range(3):
        gather_copy(a, i, partner).start()

    wout_copy.start()
    for copy in gain_copies:
        copy.wait()
    query_rows(i)
    every_gain = ogain[...].astype(F32).reshape(1, -1)
    for h in range(n * local_heads):
        head_gain[h] = every_gain[:, h * VDIM:(h + 1) * VDIM]

    wkv_copy.wait()
    table_copy.wait()
    keyval(i)
    arrive(0, partner)
    arrive(1, partner)
    keyval(partner)
    arrive(2, partner)
    query_rows(partner)
    relay(8, 12, 0)
    for d in range(1, n_chips):
        forward(0, d)
        forward(1, d)
        relay(1, 2, 0)
        keyval(far_slot(d))

    @pl.when(assists)
    def _():
        assist_copy.wait()
        assist_send(x, 1).start()

    relay(2, 2, 2)
    for d in range(1, n_chips):
        other = far_slot(d) + 1 - 2 * core
        arrive(0, other)
        arrive(1, other)
        keyval(other)

    @pl.when(assists)
    def _():
        assist_send(across, 0).start()

    relay(5, 1, 4)
    for d in range(1, n_chips):
        forward(2, d)
        query_rows(far_slot(d))
    relay(0, 1, 6)
    for d in range(1, n_chips):
        other = far_slot(d) + 1 - 2 * core
        arrive(2, other)
        query_rows(other)
    relay(1, 2, 16)

    wide_left = lax.broadcasted_iota(jnp.int32, (2 * rows, 128), 1) < 64

    def queries(slot, part, c):
        at = pl.ds(c * 2 * rows, 2 * rows)
        raw = jnp.dot(qn[at, :], whead[part][slot], preferred_element_type=F32)
        last = raw[:, raw.shape[1] - 128:]
        turned = turned_pair(last, at)
        if part == 0:
            qs[slot, at, 0:128] = raw[:, 0:128].astype(BF16)
            qs[slot, at, 128:256] = jnp.where(wide_left, turned, last).astype(BF16)
        else:
            qs[slot, at, 256:384] = jnp.where(wide_left, last, turned).astype(BF16)

    power = HEAD ** (-0.5) * float(np.log2(np.e))
    block = 2 * rows
    causal = lax.broadcasted_iota(jnp.int32, (block, block), 1) <= lax.broadcasted_iota(
        jnp.int32, (block, block), 0
    )

    def attend(c, slot, heads):
        start, stop = c * block, (c + 1) * block
        scores = []
        for hh in heads:
            score = lax.dot_general(
                qs[slot, start:stop, hh * 128:hh * 128 + 256], ks[2 * slot + hh, 0:stop, :],
                (((1,), (1,)), ((), ())), preferred_element_type=F32,
            )
            last = jnp.where(causal, score[:, start:], -jnp.inf)
            scores.append(jnp.concatenate([score[:, :start], last], axis=1) if c else last)
        tops = [jnp.max(score, axis=-1, keepdims=True) for score in scores]
        weights = [
            jnp.exp2((score - top) * power).astype(BF16) for score, top in zip(scores, tops)
        ]
        for hh, weight in zip(heads, weights):
            summed = jnp.dot(weight, vs[2 * slot + hh, 0:stop, :], preferred_element_type=F32)
            result = (summed[:, 0:VDIM] / summed[:, VDIM:2 * VDIM]).astype(BF16)
            for e in range(2):
                att_out[2 * c + e, 2 * slot + hh] = result[e * rows:(e + 1) * rows]

    def batch(head, sender_x):
        own = lax.div(head, 2) == sender_x
        return jnp.where(own, 0, 1 + lax.rem(head, 2))

    def att_copy(b, head):
        return pltpu.make_async_remote_copy(
            src_ref=att_out.at[b, head], dst_ref=att_in.at[i, head],
            send_sem=att_send.at[0], recv_sem=att_recv.at[peer(i, b), batch(head, x)],
            device_id={"sp": b}, device_id_type=MESH,
        )

    def far_head(slot, hh):
        for c in range(n_chips):
            @pl.when(chip != c)
            def _(c=c):
                queries(slot, hh, c)
                attend(c, slot, (hh,))
                for b in (2 * c, 2 * c + 1):
                    att_copy(b, 2 * slot + hh).start()

    def own_heads(slot):
        for c in range(n_chips):
            @pl.when(chip == c)
            def _(c=c):
                for hh in range(2):
                    queries(slot, hh, c)
                attend(c, slot, (0, 1))
        for hh in range(2):
            att_copy(partner, 2 * slot + hh).start()

    far_head(x, 0)
    relay(len(parts), len(parts), 0)

    @pl.when(at_end)
    def _():
        assist_send(x, 1).wait_recv()

    far_head(x, 1)
    own_heads(x)
    for part in range(2):
        x_copy(whead[part].at[across], part).wait_recv()
        far_head(across, part)
    own_heads(across)

    wout_copy.wait()
    squares = []
    group = local_heads * VDIM

    def product(pieces):
        sides = []
        for s, first, number in pieces:
            values = []
            if s is not i:
                heads = [(first, number)]
                if number > 2:
                    heads = [(2 * x, 2), (2 * across, 1), (2 * across + 1, 1)]
                for head, together in heads:
                    landed = att_in.at[s, pl.ds(head, together)]
                    pltpu.make_async_remote_copy(
                        src_ref=landed, dst_ref=landed, send_sem=att_send.at[0],
                        recv_sem=att_recv.at[peer(s, i), batch(head, x)],
                        device_id={"sp": partner}, device_id_type=MESH,
                    ).wait_recv()
            for hh in range(number):
                value = (att_out if s is i else att_in)[s, first + hh].astype(F32)
                squares.append(value * value)
                values.append((value * head_gain[s * local_heads + first + hh]).astype(BF16))
            at = pl.multiple_of(s * group + first * VDIM, VDIM)
            sides.append((values, wout[pl.ds(at, number * VDIM), :]))
        return jnp.dot(
            jnp.concatenate(sum((values for values, _ in sides), []), axis=1),
            jnp.concatenate([rows_of for _, rows_of in sides], axis=0),
            preferred_element_type=F32,
        )

    far = []
    for d in range(1, n_chips):
        far += [far_slot(d), far_slot(d) + 1 - 2 * core]
    acc[...] = product([(i, 0, local_heads)])
    acc[...] += product([(s, 2 * x, 2) for s in far])
    acc[...] += product([(partner, 0, local_heads)])
    acc[...] += product([(s, 2 * across, 1) for s in far])
    term = product([(s, 2 * across + 1, 1) for s in far])
    squared = jnp.sum(sum(squares[1:], squares[0]), axis=-1, keepdims=True)
    factor = lax.rsqrt(squared / (n * group) + 1e-05)
    out_ref[0] = ((acc[...] + term) * factor).astype(BF16)

    for a in range(3):
        every = gathered[a][1].at[pl.ds(0, n - 1)]
        pltpu.make_async_remote_copy(
            src_ref=every, dst_ref=every, send_sem=gat_send.at[a], recv_sem=gat_recv.at[a, 0],
            device_id={"sp": partner}, device_id_type=MESH,
        ).wait_send()
    def all_sent(every, sem):
        pltpu.make_async_remote_copy(
            src_ref=every, dst_ref=every, send_sem=w_send.at[sem], recv_sem=w_recv.at[0],
            device_id={"dp": targets[0]}, device_id_type=MESH,
        ).wait_send()

    @pl.when(owns)
    def _():
        all_sent(wqa, 0)
        all_sent(wqb, 1)

    @pl.when(at_mid)
    def _():
        all_sent(wqa.at[x], 0)

    @pl.when(assists)
    def _():
        all_sent(wqb, 1)

    x_copy(wqa.at[x], 0).wait_send()

    @pl.when(jnp.logical_not(at_end))
    def _():
        x_copy(wqb.at[x], 1).wait_send()

    every = att_out.at[pl.ds(0, n - 1)]
    pltpu.make_async_remote_copy(
        src_ref=every, dst_ref=every, send_sem=att_send.at[0], recv_sem=att_recv.at[0, 0],
        device_id={"sp": partner}, device_id_type=MESH,
    ).wait_send()


def paired(
    mesh, columns, q_latent, kv_latent, rope_key, w_query, w_keyval, w_out, query_gain, latent_gain,
    out_gain,
):
    n, m = mesh.shape["sp"], mesh.shape["dp"]
    rows = q_latent.shape[1]
    length = n * rows
    rank = q_latent.shape[2]
    width = w_query.shape[1]
    local_heads = H // n
    chunks = (16, 4)
    dim = w_out.shape[1]
    geometry = (n, columns, m // columns, chunks, local_heads)
    any_spec = pl.BlockSpec(memory_space=pl.ANY)
    vmem_spec = pl.BlockSpec(memory_space=pltpu.VMEM)
    dma = pltpu.SemaphoreType.DMA
    return pl.pallas_call(
        functools.partial(paired_kernel, geometry),
        out_shape=pltpu.VMEM((1, rows, dim), BF16),
        in_specs=[any_spec] * 10,
        out_specs=vmem_spec,
        scratch_shapes=[
            pltpu.VMEM((n, rows, rank), BF16),
            pltpu.VMEM((n, rows, kv_latent.shape[2]), BF16),
            pltpu.VMEM((n, ROPE, rows), BF16),
            pltpu.VMEM((columns, rank, 2 * NOPE), BF16),
            pltpu.VMEM((columns, rank, width - 2 * NOPE), BF16),
            pltpu.VMEM((rank, width - 2 * NOPE), BF16),
            pltpu.VMEM(w_keyval.shape, BF16),
            pltpu.VMEM(w_out.shape, BF16),
            pltpu.VMEM((length, 256), F32),
            pltpu.VMEM(query_gain.shape, BF16),
            pltpu.VMEM(latent_gain.shape, BF16),
            pltpu.VMEM(out_gain.shape, BF16),
            pltpu.VMEM((n * local_heads, 1, VDIM), F32),
            pltpu.VMEM((length, rank), BF16),
            pltpu.VMEM((columns, length, width), BF16),
            pltpu.VMEM((local_heads, length, 256), BF16),
            pltpu.VMEM((local_heads, length, 2 * VDIM), BF16),
            pltpu.VMEM((n, local_heads, rows, VDIM), BF16),
            pltpu.VMEM((n, local_heads, rows, VDIM), BF16),
            pltpu.VMEM((rows, dim), F32),
            dma((11,)),
            dma((3,)),
            dma((3, n - 1)),
            dma((4,)),
            dma((sum(chunks),)),
            dma((3,)),
            dma((1,)),
            dma((n - 1, 3)),
        ],
        compiler_params=pltpu.CompilerParams(
            collective_id=0, has_side_effects=True, vmem_limit_bytes=56 * 1024 * 1024,
        ),
    )(
        q_latent, kv_latent, jnp.swapaxes(rope_key, 1, 2), w_query, w_keyval, w_out,
        jnp.asarray(paired_table(length)), query_gain, latent_gain, out_gain,
    )


def x_size(mesh):
    row = mesh.devices[0]
    places = [getattr(device, "coords", None) for device in row]
    if any(place is None for place in places):
        return 1
    return len({place[0] for place in places})


def per_device(
    mesh, q_latent, kv_latent, rope_key, w_query, w_keyval, w_out, query_gain, latent_gain, out_gain
):
    n, m = mesh.shape["sp"], mesh.shape["dp"]
    rows = q_latent.shape[1]
    length = n * rows
    rank = q_latent.shape[2]
    width = w_query.shape[1]
    local_heads = H // n
    k = local_heads * HEAD // width
    chunks = 16
    columns = x_size(mesh)
    groups = k if k == columns == 2 and width % HEAD == 0 else 1
    dim = w_out.shape[1]
    group = local_heads * VDIM
    if groups == columns and width == 2 * HEAD and H % m == 0 and n == 4 and m == n * columns:
        return paired(
            mesh, columns, q_latent, kv_latent, rope_key, w_query, w_keyval, w_out, query_gain,
            latent_gain, out_gain,
        )
    table = jnp.asarray(turn_table(length))
    geometry = (n, m, columns, k, chunks, local_heads, groups)
    any_spec = pl.BlockSpec(memory_space=pl.ANY)
    vmem_spec = pl.BlockSpec(memory_space=pltpu.VMEM)
    dma = pltpu.SemaphoreType.DMA
    return pl.pallas_call(
        functools.partial(kernel, geometry),
        out_shape=pltpu.VMEM((1, rows, dim), BF16),
        in_specs=[any_spec] * 7 + [vmem_spec] * 3,
        out_specs=vmem_spec,
        scratch_shapes=[
            pltpu.VMEM((n, rows, rank), BF16),
            pltpu.VMEM((n, rows, kv_latent.shape[2]), BF16),
            pltpu.VMEM((n, ROPE, rows), BF16),
            pltpu.VMEM((k, rank, width), BF16),
            pltpu.VMEM(w_keyval.shape, BF16),
            pltpu.VMEM(w_out.shape, BF16),
            pltpu.VMEM((length, 128), F32),
            pltpu.VMEM((local_heads // groups, width, 256), BF16),
            pltpu.VMEM((length, rank), BF16),
            pltpu.VMEM((local_heads, length, 256), BF16),
            pltpu.VMEM((local_heads, length, 256), BF16),
            pltpu.VMEM((local_heads, length, VDIM), BF16),
            pltpu.VMEM((n, groups, rows, group // groups), BF16),
            pltpu.VMEM((n, groups, rows, group // groups), BF16),
            pltpu.VMEM((rows, dim), F32),
            pltpu.VMEM((n, 1, group), F32),
            dma((7,)),
            dma((3, n // 2)),
            dma((3, n)),
            dma((3, n // 2)),
            dma((4, k, chunks)),
            dma((k, chunks)),
            dma((n, groups)),
            dma((n, groups)),
        ],
        compiler_params=pltpu.CompilerParams(
            collective_id=0, has_side_effects=True, vmem_limit_bytes=56 * 1024 * 1024
        ),
    )(
        q_latent, kv_latent, jnp.swapaxes(rope_key, 1, 2), w_query, w_keyval, w_out, table,
        query_gain, latent_gain, out_gain,
    )


def solution(mesh):
    in_specs = (
        P("dp", "sp", None),
        P("dp", "sp", None),
        P("dp", "sp", None),
        P(None, "dp"),
        P(None, "sp"),
        P(),
        P(),
        P(),
        P(),
    )
    return jax.shard_map(
        functools.partial(per_device, mesh), mesh=mesh, in_specs=in_specs,
        out_specs=P("dp", "sp", None), check_vma=False,
    )
```
